32 devices in a mesh: sp: 4 (over z), tp: 4 (over y, x), dp: 2 (over core).
Axes of the slice: x: 2, y: 2, z: 4, core: 2. Of those that a mesh axis runs over, the one named last changes fastest.
Arguments:
- latents: bfloat16 [1024, 2048], P(('dp', 'sp', 'tp')), parts along dimension 0, may hold values from -6 to 6
- sample_vector: float32 [2, 2048], P('dp'), parts along dimension 0, may hold values from -6 to 6
- context: bfloat16 [512, 2048], P(('dp', 'sp')), parts along dimension 0, may hold values from -6 to 6
- context_vector: float32 [1, 2048], replicated, may hold values from -6 to 6
- norm_gain: float32 [2048], replicated, may hold values from 0.1 to 1.9
- modulator: bfloat16 [2048, 6144], P(None, ('sp', 'tp')), may hold values from -0.25 to 0.25
- query_weight: bfloat16 [2048, 1024], P('sp', 'tp'), may hold values from -0.125 to 0.125
- key_weight: bfloat16 [2048, 1024], P('sp', 'tp'), may hold values from -0.125 to 0.125
- value_weight: bfloat16 [2048, 2048], P('sp', 'tp'), may hold values from -0.125 to 0.125
- decay_down: bfloat16 [2048, 64], replicated, may hold values from -0.125 to 0.125
- decay_up: bfloat16 [2, 32, 1024], P(None, None, 'tp'), may hold values from -1 to 1
- decay_bias: float32 [2, 1024], P(None, 'tp'), as said below
- decay_extra: float32 [2, 1024, 8], P(None, ('dp', 'sp'), 'tp'), parts along dimension 1, may hold values from -2 to 0
- head_gain: float32 [256], replicated, may hold values from 0.1 to 1.9
- out_weight: bfloat16 [2048, 2048], P('tp'), may hold values from -0.125 to 0.125
Outputs:
- updated: bfloat16 [1024, 2048], P(('dp', 'sp', 'tp')), parts along dimension 0
The draws below stay inside these ranges and needn't reach their ends.
There are 2 independent parts, one for each index of `dp`. The reference program is written for one: setup_inputs(seed, part) draws one part's arguments, and reference() takes and returns one part's arrays. A program takes and returns all parts, laid end to end along the dimension named above; an argument that names none is the same for every part. Nothing has to cross between parts.
Inputs may be any that keep to these rules, and one draw needn't show every extreme that they name: `decay_bias`: offsets of the decay gates,.
All inputs are finite; a program needn't handle non-finite values.
Results may differ from the reference program's by a relative error of at most 0.012.
Values may be sent and summed in bfloat16 or wider, within the bound.
A program may use at most 64 MiB of HBM per device.

```python
import jax
import jax.numpy as jnp
from jax import lax

D = 2048
HEADS = 8
DK = 128
DV = 256
RANK = 32
BLOCK = 64
CTX_LIFT = 4
CTX = 256
TOK_DEV = 128
TOKENS = 512
N_TP = 4


def draw_decay_bias(key, part):
    pick_key, slow_key, fast_key = jax.random.split(jax.random.fold_in(key, 11), 3)
    fast_limit = 5
    is_fast = jax.random.randint(pick_key, (2, HEADS, 1), 0, 10) < fast_limit
    slow_level = jnp.log(1.65 * TOKENS / 4.8)
    slow = slow_level + jax.random.uniform(slow_key, (2, HEADS, DK), jnp.float32, -0.5, 0.5)
    fast = jax.random.uniform(fast_key, (2, HEADS, DK), jnp.float32, -0.5, 1.5)
    return jnp.where(is_fast, fast, slow).reshape(2, HEADS * DK).astype(jnp.float32)


def draw_decay_extra(key, part):
    base_key, place_key, size_key = jax.random.split(jax.random.fold_in(key, 23), 3)
    block_count = TOKENS // TOK_DEV
    rates = jnp.exp(jax.random.uniform(base_key, (2, block_count, HEADS), jnp.float32, jnp.log(0.4), jnp.log(2.5)))
    baseline_magnitude = -(0.8 / TOKENS) * jnp.repeat(rates, TOK_DEV, axis=1)
    places = jax.random.randint(place_key, (2, 2, HEADS), 0, TOKENS)
    objective_totals = jnp.log(1.0 - jax.random.uniform(size_key, (2, 2, HEADS), jnp.float32, 0.2, 0.5))
    positions = jnp.arange(TOKENS, dtype=jnp.int32)
    agreement_tally = positions[None, None, :, None] == places[:, :, None, :]
    cluster_batches = jnp.sum(jnp.where(agreement_tally, objective_totals[:, :, None, :], 0.0), axis=1)
    return (baseline_magnitude + cluster_batches).astype(jnp.float32)


def level_of(stream_key, extent, cuts, smallest, top_value):
    def one(dim, shards_of):
        draws = jax.random.uniform(jax.random.fold_in(jax.random.fold_in(stream_key, 6), dim), (shards_of,), jnp.float32, smallest / len(cuts), top_value / len(cuts))
        return jnp.repeat(jnp.exp(draws), extent[dim] // shards_of).reshape((-1,) + (1,) * (len(extent) - dim - 1))

    factor_of = one(*cuts[0])
    for cut in cuts[1:]:
        factor_of = factor_of * one(*cut)
    return factor_of


def centred(key, dims, width, limit, cuts=(), held_as=jnp.bfloat16):
    drawn = jax.random.normal(key, dims, jnp.float32) * width
    if len(cuts) > 0:
        drawn = level_of(key, dims, cuts, -0.22, 0.18) * drawn
    return jnp.clip(drawn, min=-limit, max=limit).astype(held_as)


def setup_inputs(seed: int = 0, part: int = 0) -> dict:
    splits = jax.random.split(jax.random.key(seed), 16)
    part_keys = jax.random.split(jax.random.fold_in(splits[15], part), 16)
    latents = centred(part_keys[0], (TOKENS, D), 1.0, 6.0, ((0, 16),))
    sample_vector = centred(part_keys[1], (1, D), 1.0, 6.0, (), jnp.float32)
    context = centred(part_keys[2], (CTX, D), 1.0, 6.0, ((0, 4),))
    context_vector = centred(splits[3], (1, D), 1.0, 6.0, (), jnp.float32)
    norm_gain = jnp.clip(1.0 + 0.18 * jax.random.normal(splits[4], (D,), jnp.float32), 0.1, 1.9)
    modulator = centred(splits[5], (D, 3 * D), (D // 4) ** -0.5, 0.25, ((1, 16),))
    query_weight = centred(splits[6], (D, HEADS * DK), D ** -0.5, 0.125, ((0, 4), (1, 4)))
    key_weight = centred(splits[7], (D, HEADS * DK), D ** -0.5, 0.125, ((0, 4), (1, 4)))
    value_weight = centred(splits[8], (D, HEADS * DV), D ** -0.5, 0.125, ((0, 4), (1, 4)))
    decay_down = centred(splits[9], (D, 2 * RANK), D ** -0.5, 0.125)
    decay_up = centred(splits[10], (2, RANK, HEADS * DK), RANK ** -0.5, 1.0, ((2, 4),))
    decay_bias = draw_decay_bias(jax.random.fold_in(splits[15], 71), part)
    decay_extra = draw_decay_extra(jax.random.fold_in(jax.random.fold_in(splits[15], part), 71), part)
    head_gain = jnp.clip(1.0 + 0.18 * jax.random.normal(splits[13], (DV,), jnp.float32), 0.1, 1.9)
    out_weight = centred(splits[14], (HEADS * DV, D), (HEADS * DV) ** -0.5, 0.125, ((0, 4),))
    return dict(latents=latents, sample_vector=sample_vector, context=context, context_vector=context_vector, norm_gain=norm_gain, modulator=modulator, query_weight=query_weight, key_weight=key_weight, value_weight=value_weight, decay_down=decay_down, decay_up=decay_up, decay_bias=decay_bias, decay_extra=decay_extra, head_gain=head_gain, out_weight=out_weight)


epsilon = 1e-06
exponential_sharpness = 16.0
precise = lax.Precision.HIGHEST

def rms_rows(values, gains):
    values = values.astype(jnp.float32)
    return values * lax.rsqrt(lax.optimization_barrier(jnp.mean(values * values, axis=-1, keepdims=True)) + epsilon) * gains

def modulated(tokens, gains, modulation, model_width):
    shift_vector = modulation[:model_width]
    scale_vector = modulation[model_width:2 * model_width]
    return (rms_rows(tokens, gains) * (1.0 + scale_vector) + shift_vector).astype(jnp.bfloat16)

def log_decays(low_rank, decay_up, decay_bias):
    fragment_sequence = []
    for direction in range(2):
        low_piece = lax.optimization_barrier(low_rank[:, direction * RANK:(direction + 1) * RANK]).astype(jnp.float32)
        unnormalized_ratings = jnp.dot(low_piece, decay_up[direction].astype(jnp.float32), precision=precise) + decay_bias[direction]
        fragment_sequence.append(jax.nn.log_sigmoid(unnormalized_ratings) / exponential_sharpness)
    return jnp.stack(fragment_sequence)

def sweep(queries, key_rows, value_rows, decays, carried):
    block_count = queries.shape[0] // BLOCK
    lower_mask = jnp.tril(jnp.ones((BLOCK, BLOCK), dtype=bool))

    def to_blocks(values):
        return values.reshape((block_count, BLOCK) + values.shape[1:])

    def advance(carried, inputs):
        query_block, key_block, value_block, decay_block = inputs
        within = jnp.cumsum(decay_block, axis=0)
        block_total = within[-1]
        query_dec = query_block * jnp.exp(within)
        scores = jnp.einsum('chd,shd->hcs', query_dec, key_block * jnp.exp(-within), precision=precise)
        scores = jnp.where(lower_mask[None], scores, 0.0)
        output = jnp.einsum('hcs,she->che', scores, value_block, precision=precise)
        output = output + jnp.einsum('chd,hde->che', query_dec, carried, precision=precise)
        update = jnp.einsum('shd,she->hde', key_block * jnp.exp(block_total - within), value_block, precision=precise)
        return (jnp.exp(block_total)[:, :, None] * carried + update, output)
    carried, outputs = lax.scan(advance, carried, (to_blocks(queries), to_blocks(key_rows), to_blocks(value_rows), to_blocks(decays)))
    return (carried, outputs.reshape(queries.shape[0], queries.shape[1], value_rows.shape[2]))

def reference(latents, sample_vector, context, context_vector, norm_gain, modulator, query_weight, key_weight, value_weight, decay_down, decay_up, decay_bias, decay_extra, head_gain, out_weight):
    model_width = latents.shape[1]
    conditions = jax.nn.silu(jnp.concatenate([sample_vector, context_vector], 0)).astype(jnp.bfloat16)
    modulation = jnp.dot(conditions, modulator, preferred_element_type=jnp.float32)
    hidden = modulated(latents, norm_gain, modulation[0], model_width)
    context_hidden = modulated(context, norm_gain, modulation[1], model_width)

    def project(token_rows, weight):
        return jnp.dot(token_rows, weight, preferred_element_type=jnp.float32).astype(jnp.bfloat16)

    def by_head(values, size):
        return lax.optimization_barrier(values).astype(jnp.float32).reshape(values.shape[0], HEADS, size)
    queries = by_head(project(hidden, query_weight), DK)
    key_rows = by_head(project(hidden, key_weight), DK)
    value_rows = by_head(project(hidden, value_weight), DV)
    context_keys = by_head(project(context_hidden, key_weight), DK)
    context_values = by_head(project(context_hidden, value_weight), DV)
    decays = log_decays(project(hidden, decay_down), decay_up, decay_bias).reshape(2, TOKENS, HEADS, DK) + decay_extra[:, :, :, None]
    context_decays = log_decays(project(context_hidden, decay_down), decay_up, decay_bias).reshape(2, CTX, HEADS, DK)
    zero_state = jnp.zeros((HEADS, DK, DV), jnp.float32)
    start_forward, _ = sweep(context_keys, context_keys, context_values, context_decays[0], zero_state)
    start_backward, _ = sweep(context_keys[::-1], context_keys[::-1], context_values[::-1], context_decays[1][::-1], zero_state)
    _, forward = sweep(queries, key_rows, value_rows, decays[0], CTX_LIFT * start_forward)
    _, backward = sweep(queries[::-1], key_rows[::-1], value_rows[::-1], decays[1][::-1], CTX_LIFT * start_backward)
    mixed = forward + backward[::-1]
    normed = rms_rows(mixed, head_gain).astype(jnp.bfloat16).reshape(TOKENS, HEADS * DV)
    group_width = HEADS * DV // N_TP
    summed = jnp.zeros((TOKENS, model_width), jnp.float32)
    for group_index in range(N_TP):
        lower_edge = group_index * group_width
        partial_value = jnp.dot(normed[:, lower_edge:lower_edge + group_width], out_weight[lower_edge:lower_edge + group_width], preferred_element_type=jnp.float32).astype(jnp.bfloat16)
        summed = summed + lax.optimization_barrier(partial_value).astype(jnp.float32)
    projected = lax.optimization_barrier(summed.astype(jnp.bfloat16)).astype(jnp.float32)
    gate_vector = modulation[0, 2 * model_width:]
    return (latents.astype(jnp.float32) + gate_vector * projected).astype(jnp.bfloat16)
```

```python
import functools

import jax
import jax.numpy as jnp
from jax import lax
from jax.experimental import pallas as pl
from jax.experimental.pallas import tpu as pltpu
from jax.sharding import PartitionSpec as P

DK = 128
BLOCK = 64
CTX_LIFT = 4
EPS = 1e-06
SHARP = 16.0
F32 = jnp.float32
BF16 = jnp.bfloat16
MESH = pl.DeviceIdType.MESH


def dot(a, b):
    return jnp.dot(a, b, preferred_element_type=F32)


def dot_nt(a, b):
    return lax.dot_general(a, b, (((1,), (1,)), ((), ())), preferred_element_type=F32)


def dot_tn(a, b):
    return lax.dot_general(a, b, (((0,), (0,)), ((), ())), preferred_element_type=F32)


def sums(mask, values):
    high = values.astype(BF16)
    low = (values - high.astype(F32)).astype(BF16)
    width = values.shape[1]
    both = dot(mask.astype(F32).astype(BF16), jnp.concatenate([high, low], axis=1))
    return both[:, :width] + both[:, width:]


def log_sigmoid(x):
    return jnp.minimum(x, 0.0) - jnp.log1p(jnp.exp(-jnp.abs(x)))


def kernel(
    n_sp,
    n_tp,
    latents_in,
    sample_vector_in,
    context_in,
    context_vector_in,
    norm_gain_in,
    modulator,
    query_weight,
    key_weight,
    value_weight,
    decay_down_in,
    decay_up_in,
    decay_bias_in,
    decay_extra_in,
    head_gain_in,
    out_weight,
    out,
    latents,
    sample_vector,
    context,
    context_vector,
    norm_gain,
    decay_down,
    decay_up,
    decay_bias,
    decay_extra,
    head_gain,
    mod_w,
    mods,
    lat,
    outer_context,
    extras,
    hid,
    wk,
    wv,
    wq,
    wo,
    acc_k,
    acc_v,
    acc_q,
    tots,
    key_rows,
    c_state,
    l_state,
    f_out,
    f_in,
    g_out,
    g_in,
    state,
    normed,
    part,
    rs,
    loc_sem,
    mt_s,
    mt_r,
    ms_s,
    ms_r,
    lat_s,
    lat_r,
    lo_s,
    lo_r,
    cx_s,
    cx_r,
    up_s,
    up_r,
    w_s,
    w_r,
    p_s,
    p_r,
    tt_s,
    tt_r,
    f_s,
    f_r,
    g_s,
    g_r,
    o_s,
    o_r,
    rs_s,
    rs_r,
):
    s = lax.axis_index("sp")
    t = lax.axis_index("tp")
    d = lax.axis_index("dp")
    h = lax.rem(d, 2)
    mate = d + 1 - 2 * h
    n_dev = n_sp * n_tp
    me = s * n_tp + t
    n_pairs = n_sp // 2
    pair = s // 2
    pos = lax.rem(s, 2)
    partner = s + 1 - 2 * pos
    is_worker = pos == 1 - s // n_pairs
    is_outer = pos == s // n_pairs
    rows, width = latents.shape
    ctx_rows = context.shape[0]
    length = rows * n_tp
    lat_all = 2 * length
    total = hid.shape[1]
    depth = hid.shape[2]
    half = depth // 2
    heads = decay_bias.shape[1] // DK
    dv = head_gain.shape[1]
    rank = decay_up.shape[1]
    span_t = width // n_tp

    def remote(src, dst, send, recv, device):
        return pltpu.make_async_remote_copy(
            src_ref=src,
            dst_ref=dst,
            send_sem=send,
            recv_sem=recv,
            device_id=device,
            device_id_type=MESH,
        )

    def worker_of(p):
        return 2 * p + 1 - p // (n_pairs // 2)

    def tp_peer(k):
        return lax.rem(t + k, n_tp)

    def tp_from(k):
        return lax.rem(t - k + n_tp, n_tp)

    def sp_peer(k):
        return lax.rem(s + k, n_sp)

    def sp_from(k):
        return lax.rem(s - k + n_sp, n_sp)

    weights = ((key_weight, wk), (value_weight, wv), (query_weight, wq))
    local = [pltpu.make_async_copy(modulator, mod_w, loc_sem.at[0])]
    for m, (source, slots) in enumerate(weights):
        for i in range(2):
            local.append(
                pltpu.make_async_copy(
                    source.at[pl.ds(i * half, half)], slots.at[s, i], loc_sem.at[1 + 2 * m + i]
                )
            )
    local.append(pltpu.make_async_copy(out_weight, wo, loc_sem.at[7]))
    barrier = pltpu.get_barrier_semaphore()
    for k in range(1, n_tp):
        pl.semaphore_signal(barrier, inc=1, device_id={"tp": tp_peer(k)}, device_id_type=MESH)
    for k in range(1, n_sp):
        pl.semaphore_signal(barrier, inc=1, device_id={"sp": sp_peer(k)}, device_id_type=MESH)
    pl.semaphore_signal(barrier, inc=1, device_id={"dp": mate}, device_id_type=MESH)
    small = [
        pltpu.make_async_copy(source, target, loc_sem.at[8 + i])
        for i, (source, target) in enumerate(
            (
                (sample_vector_in, sample_vector),
                (context_vector_in, context_vector),
                (latents_in, latents),
                (context_in, context),
                (decay_extra_in, decay_extra),
                (norm_gain_in, norm_gain),
                (decay_down_in, decay_down),
                (decay_up_in, decay_up),
                (decay_bias_in, decay_bias),
                (head_gain_in, head_gain),
            )
        )
    ]
    for copy in small[:5] + local[:1] + small[5:] + local[1:]:
        copy.start()
    small[2].wait()
    small[3].wait()
    small[4].wait()
    pl.semaphore_wait(barrier, n_tp + n_sp - 1)

    def inner():
        return jnp.logical_and(s >= 1, s <= n_sp - 2)

    def onward(r):
        return s + 1 <= n_sp - 2 if r == 0 else s - 1 >= 1

    def exists(r, j):
        return jnp.logical_and(inner(), s - j >= 0 if r == 0 else s + j < n_sp)

    def origin_of(r, j):
        return s - j if r == 0 else s + j

    def ring_copy(m, r, j, first=False):
        source, slots = weights[m]
        origin = origin_of(r, j)
        src = source.at[pl.ds(h * half, half)] if first else slots.at[origin, h]
        target = s + 1 if r == 0 else s - 1
        return remote(src, slots.at[origin, h], w_s.at[m, r, j], w_r.at[m, r, j], {"sp": target})

    def ring_arrival(m, r, j):
        view = weights[m][1].at[origin_of(r, j), h]
        return remote(view, view, w_s.at[m, r, j - 1], w_r.at[m, r, j - 1], {"sp": s})

    def mate_copy(m, r, j, side):
        view = weights[m][1].at[origin_of(r, j), side]
        return remote(view, view, p_s.at[m, r, j - 1], p_r.at[m, r, j - 1], {"dp": mate})

    def send_own(m):
        for r in range(2):

            @pl.when(onward(r))
            def _():
                ring_copy(m, r, 0, True).start()

    def relay(m, j, share):
        for r in range(2):

            @pl.when(exists(r, j))
            def _():
                ring_arrival(m, r, j).wait_recv()

                @pl.when(onward(r))
                def _():
                    ring_copy(m, r, j).start()

                if share:
                    mate_copy(m, r, j, h).start()

    def whole(slots, o):
        return slots[o].reshape(depth, slots.shape[3])

    def multiply(m, j, acc, count):
        slots = weights[m][1]
        for r in range(2):

            @pl.when(exists(r, j))
            def _():
                origin = origin_of(r, j)
                mate_copy(m, r, j, 1 - h).wait_recv()
                acc[...] += dot(hid[origin, 0:count], whole(slots, origin))

    def lat_copy(k):
        return remote(latents, lat.at[pos, t], lat_s.at[0, k], lat_r.at[0, k], {"tp": tp_peer(k)})

    def lat_arrival(k):
        view = lat.at[pos, tp_from(k)]
        return remote(view, view, lat_s.at[0, k], lat_r.at[0, k], {"tp": t})

    def outer_lat():
        return remote(latents, lat.at[pos, t], lo_s, lo_r, {"sp": partner})

    def outer_lat_arrival():
        view = lat.at[1 - pos, t]
        return remote(view, view, lo_s, lo_r, {"sp": s})

    def lat_relay(k, owner, to):
        view = lat.at[1 - pos, owner]
        return remote(view, view, lat_s.at[1, k], lat_r.at[1, k], {"tp": to})

    def ctx_cols(owner):
        return pl.ds(pl.multiple_of(owner * span_t, span_t), span_t)

    def ctx_copy():
        return remote(
            context.at[:, ctx_cols(t)],
            outer_context.at[:, ctx_cols(t)],
            cx_s.at[0],
            cx_r.at[0],
            {"sp": partner},
        )

    def ctx_relay(k, owner, to):
        view = outer_context.at[:, ctx_cols(owner)]
        return remote(view, view, cx_s.at[k], cx_r.at[k], {"tp": to})

    def extra_copy():
        return remote(decay_extra, extras.at[pos], up_s, up_r, {"sp": partner})

    def extra_arrival():
        view = extras.at[1 - pos]
        return remote(view, view, up_s, up_r, {"sp": s})

    @pl.when(is_outer)
    def _():
        outer_lat().start()
        extra_copy().start()
        ctx_copy().start()
        for m in range(3):
            send_own(m)

    @pl.when(is_worker)
    def _():
        for k in range(1, n_tp):
            lat_copy(k).start()
        send_own(0)
        send_own(1)

    small[0].wait()
    small[1].wait()
    is_first = lax.broadcasted_iota(jnp.int32, (16, width), 0) == 0
    vectors = jnp.where(is_first, sample_vector[...], context_vector[...])
    conditions = (vectors / (1.0 + jnp.exp(-vectors))).astype(BF16)
    local[0].wait()
    mods[me] = dot(conditions, mod_w[...])[0:2]

    def mod_tp(k, owner, to):
        view = mods.at[s * n_tp + owner]
        return remote(view, view, mt_s.at[k], mt_r.at[k], {"tp": to})

    def mod_sp(k, owner, to):
        view = mods.at[pl.ds(owner * n_tp, n_tp)]
        return remote(view, view, ms_s.at[k], ms_r.at[k], {"sp": to})

    for k in range(1, n_tp):
        mod_tp(k, t, tp_peer(k)).start()
    for k in range(1, n_tp):
        mod_tp(k, tp_from(k), t).wait_recv()
    for k in range(1, n_sp):
        mod_sp(k, s, sp_peer(k)).start()
    for copy in small[5:]:
        copy.wait()

    def modulation_now():
        for k in range(1, n_sp):
            mod_sp(k, sp_from(k), s).wait_recv()

    def mod_part(i):
        return jnp.concatenate([mods[j] for j in range(n_dev)], axis=1)[
            :, i * width : (i + 1) * width
        ]

    def tot_copy(k, owner, to):
        view = tots.at[owner]
        return remote(view, view, tt_s.at[k], tt_r.at[k], {"sp": to})

    def has_pred(z):
        return pair > 0 if z == 0 else pair < n_pairs - 1

    def has_succ(z):
        return pair < n_pairs - 1 if z == 0 else pair > 0

    def lone(a, b):
        return jnp.logical_and(a, jnp.logical_not(b))

    def f_copy(z, g):
        to = worker_of(pair + 1) if z == 0 else worker_of(pair - 1)
        return remote(f_out.at[z, g], f_in.at[z, g], f_s.at[z, g], f_r.at[z, g], {"sp": to})

    def g_copy(z, g):
        to = worker_of(pair - 1) if z == 0 else worker_of(pair + 1)
        return remote(g_out.at[z, g], g_in.at[z, g], g_s.at[z, g], g_r.at[z, g], {"sp": to})

    def o_copy(g, where, to):
        view = normed.at[where, g]
        return remote(view, view, o_s.at[g], o_r.at[g], {"sp": to})

    def work():
        outer_lat_arrival().wait_recv()
        for k in range(1, n_tp):
            lat_relay(k, t, tp_peer(k)).start()
        remote(
            outer_context.at[:, ctx_cols(t)],
            outer_context.at[:, ctx_cols(t)],
            cx_s.at[0],
            cx_r.at[0],
            {"sp": s},
        ).wait_recv()
        for k in range(1, n_tp):
            ctx_relay(k, t, tp_peer(k)).start()
        relay(0, 1, True)
        send_own(2)

        lat[pos, t] = latents[...]
        for k in range(1, n_tp):
            lat_arrival(k).wait_recv()
        modulation_now()
        shift = mod_part(0)
        scale = mod_part(1)

        def modulated(x, row):
            x = x.astype(F32)
            x = x * lax.rsqrt(jnp.mean(x * x, axis=-1, keepdims=True) + EPS) * norm_gain[...]
            return (x * (1.0 + scale[row : row + 1]) + shift[row : row + 1]).astype(BF16)

        piece = min(32, ctx_rows)

        def put(x, at):
            count = x.shape[0]
            at = pl.multiple_of(at, piece)
            for o in range(n_sp):
                hid[o, pl.ds(at, count)] = x[:, o * depth : (o + 1) * depth]

        for i in range(n_tp):
            put(modulated(lat[pos, i], 0), pos * length + i * rows)
        for i in range(ctx_rows // piece):
            put(
                modulated(context[i * piece : (i + 1) * piece], 1),
                lat_all + pos * ctx_rows + i * piece,
            )
        for k in range(1, n_tp):
            lat_relay(k, tp_from(k), t).wait_recv()
        for i in range(n_tp):
            put(modulated(lat[1 - pos, i], 0), (1 - pos) * length + i * rows)
        for k in range(1, n_tp):
            ctx_relay(k, tp_from(k), t).wait_recv()
        for i in range(ctx_rows // piece):
            put(
                modulated(outer_context[i * piece : (i + 1) * piece], 1),
                lat_all + (1 - pos) * ctx_rows + i * piece,
            )

        low = dot_nt(hid[0], decay_down[:, 0:depth])
        for o in range(1, n_sp):
            low = low + dot_nt(hid[o], decay_down[:, o * depth : (o + 1) * depth])
        low = low.astype(BF16)
        relay(1, 1, True)

        def log_decays(z):
            x = dot(low[:, z * rank : (z + 1) * rank], decay_up[z]) + decay_bias[z : z + 1]
            return log_sigmoid(x) / SHARP

        row_id = lax.broadcasted_iota(jnp.int32, (lat_all, lat_all), 0)
        col_id = lax.broadcasted_iota(jnp.int32, (lat_all, lat_all), 1)
        same = row_id // BLOCK == col_id // BLOCK
        within_mask = [same & (col_id <= row_id), same & (col_id >= row_id)]
        extras[pos] = decay_extra[...]
        extra_arrival().wait_recv()

        def extra_sums(z):
            columns = []
            for g in range(heads):
                line = jnp.concatenate([extras[i, z, g : g + 1, :] for i in range(2)], axis=1)
                columns.append(
                    jnp.sum(jnp.where(within_mask[z], line, 0.0), axis=1, keepdims=True)
                )
            return jnp.concatenate([jnp.broadcast_to(c, (lat_all, DK)) for c in columns], axis=1)

        decays = [log_decays(z) for z in range(2)]
        within = [sums(within_mask[z], decays[z][:lat_all]) + extra_sums(z) for z in range(2)]
        blocks = lat_all // BLOCK
        totals = [
            [within[0][(b + 1) * BLOCK - 1 : (b + 1) * BLOCK] for b in range(blocks)],
            [within[1][b * BLOCK : b * BLOCK + 1] for b in range(blocks)],
        ]
        none = jnp.zeros_like(totals[0][0])

        def between(z, lo, hi):
            value = none
            for b in range(lo, hi):
                value = value + totals[z][b]
            return value

        crow = lax.broadcasted_iota(jnp.int32, (total - lat_all, total - lat_all), 0)
        ccol = lax.broadcasted_iota(jnp.int32, (total - lat_all, total - lat_all), 1)
        after = [
            sums(ccol > crow, decays[0][lat_all:]),
            sums(ccol < crow, decays[1][lat_all:]),
        ]
        lat_total = [between(z, 0, blocks) for z in range(2)]
        ctx_total = [
            after[0][0:1] + decays[0][lat_all : lat_all + 1],
            after[1][total - lat_all - 1 :] + decays[1][total - 1 :],
        ]
        tots[pair] = jnp.concatenate(lat_total + ctx_total, axis=0)
        for k in range(1, n_pairs):
            to = lax.rem(pair + k, n_pairs)
            tot_copy(k, pair, worker_of(to)).start()

        for copy in local[1:5]:
            copy.wait()
        acc_k[...] = dot(hid[s], whole(wk, s))
        acc_v[...] = dot(hid[s], whole(wv, s))
        multiply(0, 1, acc_k, total)
        multiply(1, 1, acc_v, total)
        for k in range(1, n_pairs):
            tot_copy(k, lax.rem(pair - k + n_pairs, n_pairs), s).wait_recv()
        before = [none, none]
        suffix = [none, none]
        for u in range(n_pairs):
            line = tots[u]
            below = jnp.where(u < pair, 1.0, 0.0)
            above = jnp.where(u > pair, 1.0, 0.0)
            before[0] = before[0] + below * line[0:1]
            before[1] = before[1] + above * line[1:2]
            suffix[0] = suffix[0] + above * line[2:3]
            suffix[1] = suffix[1] + below * line[3:4]
        ctx_weight = [jnp.exp(after[z] + suffix[z]) for z in range(2)]

        def per_block(f):
            return jnp.concatenate([f(b) for b in range(blocks)], axis=0)

        def rows_of(x, b):
            return x[b * BLOCK : (b + 1) * BLOCK]

        ending = [
            jnp.exp(
                per_block(
                    lambda b: totals[0][b] - rows_of(within[0], b) + between(0, b + 1, blocks)
                )
            ),
            jnp.exp(per_block(lambda b: totals[1][b] - rows_of(within[1], b) + between(1, 0, b))),
        ]
        for j in range(2, max(n_sp - 1, 2)):
            relay(0, j, True)
            multiply(0, j, acc_k, total)
            if j == 2:
                relay(2, 1, True)
            relay(1, j, True)
            multiply(1, j, acc_v, total)
        keys = acc_k[...].astype(BF16)
        values = acc_v[...].astype(BF16)
        ckeys = keys[lat_all:].astype(F32)
        cvals = values[lat_all:]
        keys = keys[:lat_all].astype(F32)
        values = values[:lat_all]

        def columns(g, n):
            return slice(g * n, (g + 1) * n)

        for z in range(2):
            ended = (keys * ending[z]).astype(BF16)
            cended = (ckeys * ctx_weight[z]).astype(BF16)
            lift = CTX_LIFT * jnp.exp(before[z])
            lift_on = CTX_LIFT * jnp.exp(before[z] + lat_total[z])
            for g in range(heads):
                c = dot_tn(cvals[:, columns(g, dv)], cended[:, columns(g, DK)])
                g_out[z, g] = c.astype(BF16)
                own = dot_tn(values[:, columns(g, dv)], ended[:, columns(g, DK)])
                f_out[z, g] = (own + lift_on[:, columns(g, DK)] * c).astype(BF16)
                if n_pairs > 2:
                    c_state[z, g] = c
                    l_state[z, g] = own + lift_on[:, columns(g, DK)] * c
                state[z, g] = lift[:, columns(g, DK)] * c

                @pl.when(lone(has_succ(z), has_pred(z)))
                def _():
                    f_copy(z, g).start()

                @pl.when(lone(has_pred(z), has_succ(z)))
                def _():
                    g_copy(z, g).start()

        if n_pairs > 2:
            for z in range(2):

                @pl.when(jnp.logical_and(has_pred(z), has_succ(z)))
                def _():
                    for g in range(heads):
                        f_copy(z, g).wait_recv()
                        on = jnp.exp(lat_total[z])[:, columns(g, DK)]
                        f_out[z, g] = (l_state[z, g] + on * f_in[z, g].astype(F32)).astype(BF16)
                        f_copy(z, g).start()

                @pl.when(jnp.logical_and(has_pred(z), has_succ(z)))
                def _():
                    for g in range(heads):
                        g_copy(z, g).wait_recv()
                        g_out[z, g] = (c_state[z, g] + g_in[z, g].astype(F32)).astype(BF16)
                        g_copy(z, g).start()

        for z in range(2):
            close = (keys * jnp.exp(-within[z])).astype(BF16)
            near = keys * jnp.exp(per_block(lambda b: totals[z][b] - rows_of(within[z], b)))
            for i in range(blocks):
                for j in range(blocks):
                    if i == j:
                        block = rows_of(close, j)
                    elif (j < i) == (z == 0):
                        gap = between(z, min(i, j) + 1, max(i, j))
                        block = (rows_of(near, j) * jnp.exp(gap)).astype(BF16)
                    else:
                        block = jnp.zeros((BLOCK, heads * DK), BF16)
                    key_rows[z, i, j * BLOCK : (j + 1) * BLOCK] = block
        reach = [jnp.exp(within[z]) for z in range(2)]
        lifted_by = [
            jnp.exp(per_block(lambda b: rows_of(within[0], b) + between(0, 0, b))),
            jnp.exp(per_block(lambda b: rows_of(within[1], b) + between(1, b + 1, blocks))),
        ]

        for copy in local[5:7]:
            copy.wait()
        acc_q[...] = dot(hid[s, 0:lat_all], whole(wq, s))
        for j in range(1, max(n_sp - 1, 2)):
            if j > 1:
                relay(2, j, True)
            multiply(2, j, acc_q, lat_all)
        queries = acc_q[...].astype(BF16).astype(F32)

        query_dec = [(queries * reach[z]).astype(BF16) for z in range(2)]
        lifted = [(queries * lifted_by[z]).astype(BF16) for z in range(2)]
        masks = [col_id <= row_id, col_id >= row_id]
        for z in range(2):
            lift = CTX_LIFT * jnp.exp(before[z])

            @pl.when(has_pred(z))
            def _():
                for g in range(heads):
                    if n_pairs == 2:
                        f_copy(z, g).wait_recv()
                    else:

                        @pl.when(jnp.logical_not(has_succ(z)))
                        def _():
                            f_copy(z, g).wait_recv()

                    state[z, g] += f_in[z, g].astype(F32)

            @pl.when(has_succ(z))
            def _():
                for g in range(heads):
                    if n_pairs == 2:
                        g_copy(z, g).wait_recv()
                    else:

                        @pl.when(jnp.logical_not(has_pred(z)))
                        def _():
                            g_copy(z, g).wait_recv()

                    state[z, g] += lift[:, columns(g, DK)] * g_in[z, g].astype(F32)

        for g in range(heads):
            cs = columns(g, DK)
            lines = []
            for i in range(blocks):
                line = 0.0
                for z in range(2):
                    score = dot_nt(rows_of(query_dec[z], i)[:, cs], key_rows[z, i, :, cs])
                    line = line + jnp.where(rows_of(masks[z], i), score, 0.0)
                lines.append(line.astype(BF16))
            mixed = dot(jnp.concatenate(lines, axis=0), values[:, columns(g, dv)])
            for z in range(2):
                mixed = mixed + dot_nt(lifted[z][:, cs], state[z, g].astype(BF16))
            by = lax.rsqrt(jnp.mean(mixed * mixed, axis=-1, keepdims=True) + EPS)
            result = (mixed * by * head_gain[...]).astype(BF16)
            for i in range(2):
                normed[i, g] = result[i * length : (i + 1) * length]
            o_copy(g, 1 - pos, partner).start()

    pl.when(is_worker)(work)

    @pl.when(is_outer)
    def _():
        for copy in local[1:7]:
            copy.wait()
        for m in (0, 1):
            relay(m, 1, False)
        for j in range(2, n_sp - 1):
            relay(0, j, False)
            if j == 2:
                relay(2, 1, False)
            relay(1, j, False)
        for j in range(2, n_sp - 1):
            relay(2, j, False)
        modulation_now()
        for g in range(heads):
            o_copy(g, pos, s).wait_recv()

    gate = mod_part(2)[0:1]
    local[7].wait()
    chunks = rs_s.shape[1]
    span = width // chunks
    rs_copies = []
    for c in range(chunks):
        cols = slice(c * span, (c + 1) * span)
        product = dot(normed[pos, 0], wo[0:dv, cols])
        for g in range(1, heads):
            product = product + dot(normed[pos, g], wo[g * dv : (g + 1) * dv, cols])
        product = product.astype(BF16)
        for i in range(n_tp):
            part[i, :, cols] = product[i * rows : (i + 1) * rows]
        for k in range(1, n_tp):
            to = tp_peer(k)
            copy = remote(
                part.at[to, :, pl.ds(c * span, span)],
                rs.at[k, :, pl.ds(c * span, span)],
                rs_s.at[k, c],
                rs_r.at[k, c],
                {"tp": to},
            )
            copy.start()
            rs_copies.append(copy)
    for c in range(chunks):
        cols = slice(c * span, (c + 1) * span)
        summed = part[t, :, cols].astype(F32)
        for k in range(1, n_tp):
            rs_copies[c * (n_tp - 1) + k - 1].wait_recv()
            summed = summed + rs[k, :, cols].astype(F32)
        projected = summed.astype(BF16).astype(F32)
        out[:, cols] = (latents[:, cols].astype(F32) + gate[:, cols] * projected).astype(BF16)

    for copy in rs_copies:
        copy.wait_send()
    for k in range(1, n_tp):
        mod_tp(k, t, tp_peer(k)).wait_send()
    for k in range(1, n_sp):
        mod_sp(k, s, sp_peer(k)).wait_send()

    @pl.when(is_outer)
    def _():
        outer_lat().wait_send()
        extra_copy().wait_send()
        ctx_copy().wait_send()

    @pl.when(is_worker)
    def _():
        for k in range(1, n_tp):
            lat_copy(k).wait_send()
            lat_relay(k, t, tp_peer(k)).wait_send()
            ctx_relay(k, t, tp_peer(k)).wait_send()
        for k in range(1, n_pairs):
            tot_copy(k, pair, s).wait_send()
        for g in range(heads):
            o_copy(g, 1 - pos, partner).wait_send()
            for z in range(2):

                @pl.when(has_succ(z))
                def _():
                    f_copy(z, g).wait_send()

                @pl.when(has_pred(z))
                def _():
                    g_copy(z, g).wait_send()

    for m in range(3):
        for r in range(2):

            @pl.when(onward(r))
            def _():
                ring_copy(m, r, 0, True).wait_send()

            for j in range(1, n_sp - 1):

                @pl.when(exists(r, j))
                def _():
                    @pl.when(onward(r))
                    def _():
                        ring_copy(m, r, j).wait_send()

                    @pl.when(is_worker)
                    def _():
                        mate_copy(m, r, j, h).wait_send()


def per_device(n_sp, n_tp, *args):
    (latents, sv, context, cv, gain, modulator, wq, wk, wv, down, up, bias, extra, hg, wo) = args
    rows, width = latents.shape
    ctx_rows = context.shape[0]
    n_dev = n_sp * n_tp
    n_pairs = n_sp // 2
    length = rows * n_tp
    total = 2 * (length + ctx_rows)
    depth = wq.shape[0]
    kw, vw = wk.shape[1], wv.shape[1]
    heads = bias.shape[1] // DK
    dv = hg.shape[0]
    chunks = 4
    vmem = pl.BlockSpec(memory_space=pltpu.VMEM)
    hbm = pl.BlockSpec(memory_space=pl.ANY)
    dma = pltpu.SemaphoreType.DMA
    states = (2, heads, dv, DK)
    chained = states if n_pairs > 2 else (2, heads, 8, DK)
    scratch = [
        pltpu.VMEM(latents.shape, BF16),
        pltpu.VMEM(sv.shape, F32),
        pltpu.VMEM(context.shape, BF16),
        pltpu.VMEM(cv.shape, F32),
        pltpu.VMEM((1, width), F32),
        pltpu.VMEM(down.shape[::-1], BF16),
        pltpu.VMEM(up.shape, BF16),
        pltpu.VMEM(bias.shape, F32),
        pltpu.VMEM((2, heads, length), F32),
        pltpu.VMEM((1, dv), F32),
        pltpu.VMEM(modulator.shape, BF16),
        pltpu.VMEM((n_dev, 2, modulator.shape[1]), F32),
        pltpu.VMEM((2, n_tp, rows, width), BF16),
        pltpu.VMEM((ctx_rows, width), BF16),
        pltpu.VMEM((2, 2, heads, length), F32),
        pltpu.VMEM((n_sp, total, depth), BF16),
        pltpu.VMEM((n_sp, 2, depth // 2, kw), BF16),
        pltpu.VMEM((n_sp, 2, depth // 2, vw), BF16),
        pltpu.VMEM((n_sp, 2, depth // 2, kw), BF16),
        pltpu.VMEM(wo.shape, BF16),
        pltpu.VMEM((total, kw), F32),
        pltpu.VMEM((total, vw), F32),
        pltpu.VMEM((2 * length, kw), F32),
        pltpu.VMEM((n_pairs, 4, kw), F32),
        pltpu.VMEM((2, 2 * length // BLOCK, 2 * length, kw), BF16),
        pltpu.VMEM(chained, F32),
        pltpu.VMEM(chained, F32),
        pltpu.VMEM(states, BF16),
        pltpu.VMEM(states, BF16),
        pltpu.VMEM(states, BF16),
        pltpu.VMEM(states, BF16),
        pltpu.VMEM(states, F32),
        pltpu.VMEM((2, heads, length, dv), BF16),
        pltpu.VMEM((n_tp, rows, width), BF16),
        pltpu.VMEM((n_tp, rows, width), BF16),
        dma((18,)),
        dma((n_tp,)),
        dma((n_tp,)),
        dma((n_sp,)),
        dma((n_sp,)),
        dma((2, n_tp)),
        dma((2, n_tp)),
        dma,
        dma,
        dma((n_tp,)),
        dma((n_tp,)),
        dma,
        dma,
        dma((3, 2, n_sp)),
        dma((3, 2, n_sp)),
        dma((3, 2, n_sp)),
        dma((3, 2, n_sp)),
        dma((n_pairs,)),
        dma((n_pairs,)),
        dma((2, heads)),
        dma((2, heads)),
        dma((2, heads)),
        dma((2, heads)),
        dma((heads,)),
        dma((heads,)),
        dma((n_tp, chunks)),
        dma((n_tp, chunks)),
    ]
    return pl.pallas_call(
        functools.partial(kernel, n_sp, n_tp),
        out_shape=jax.ShapeDtypeStruct(latents.shape, BF16),
        in_specs=[hbm] * 15,
        out_specs=vmem,
        scratch_shapes=scratch,
        compiler_params=pltpu.CompilerParams(
            collective_id=0, has_side_effects=True, vmem_limit_bytes=56 * 1024 * 1024
        ),
    )(
        latents,
        sv,
        context,
        cv,
        gain.reshape(1, -1),
        modulator,
        wq,
        wk,
        wv,
        down.T,
        up,
        bias,
        extra.transpose(0, 2, 1),
        hg.reshape(1, -1),
        wo,
    )


def solution(mesh):
    placed = (
        P(("dp", "sp", "tp"), None),
        P("dp", None),
        P(("dp", "sp"), None),
        P(),
        P(),
        P(None, ("sp", "tp")),
        P("sp", "tp"),
        P("sp", "tp"),
        P("sp", "tp"),
        P(),
        P(None, None, "tp"),
        P(None, "tp"),
        P(None, ("dp", "sp"), "tp"),
        P(),
        P("tp", None),
    )
    return jax.shard_map(
        functools.partial(per_device, mesh.shape["sp"], mesh.shape["tp"]),
        mesh=mesh,
        in_specs=placed,
        out_specs=P(("dp", "sp", "tp"), None),
        check_vma=False,
    )
```

```python
import functools

import jax
import jax.numpy as jnp
from jax import lax
from jax.experimental import pallas as pl
from jax.experimental.pallas import tpu as pltpu
from jax.sharding import PartitionSpec as P

DK = 128
BLOCK = 64
CTX_LIFT = 4
EPS = 1e-06
SHARP = 16.0
F32 = jnp.float32
BF16 = jnp.bfloat16
MESH = pl.DeviceIdType.MESH


def dot(a, b):
    return jnp.dot(a, b, preferred_element_type=F32)


def dot_nt(a, b):
    return lax.dot_general(a, b, (((1,), (1,)), ((), ())), preferred_element_type=F32)


def dot_tn(a, b):
    return lax.dot_general(a, b, (((0,), (0,)), ((), ())), preferred_element_type=F32)


def sums(mask, values):
    high = values.astype(BF16)
    low = (values - high.astype(F32)).astype(BF16)
    width = values.shape[1]
    both = dot(mask.astype(F32).astype(BF16), jnp.concatenate([high, low], axis=1))
    return both[:, :width] + both[:, width:]


def log_sigmoid(x):
    return jnp.minimum(x, 0.0) - jnp.log1p(jnp.exp(-jnp.abs(x)))


def chain_kernel(
    n_sp,
    n_tp,
    latents_in,
    sample_vector_in,
    context_in,
    context_vector_in,
    norm_gain_in,
    modulator,
    query_weight,
    key_weight,
    value_weight,
    decay_down_in,
    decay_up_in,
    decay_bias_in,
    decay_extra_in,
    head_gain_in,
    out_weight,
    out,
    latents,
    sample_vector,
    context,
    context_vector,
    norm_gain,
    decay_down,
    decay_up,
    decay_bias,
    decay_extra,
    head_gain,
    mod_w,
    mods,
    lat,
    outer_context,
    extras,
    hid,
    wk,
    wv,
    wq,
    wo,
    acc_k,
    acc_v,
    acc_q,
    tots,
    key_rows,
    query_rows,
    c_state,
    l_state,
    f_out,
    f_in,
    g_out,
    g_in,
    state,
    normed,
    part,
    rs,
    loc_sem,
    mt_s,
    mt_r,
    ms_s,
    ms_r,
    lat_s,
    lat_r,
    lo_s,
    lo_r,
    cx_s,
    cx_r,
    up_s,
    up_r,
    w_s,
    w_r,
    p_s,
    p_r,
    tt_s,
    tt_r,
    f_s,
    f_r,
    g_s,
    g_r,
    o_s,
    o_r,
    rs_s,
    rs_r,
):
    s = lax.axis_index("sp")
    t = lax.axis_index("tp")
    d = lax.axis_index("dp")
    h = lax.rem(d, 2)
    mate = d + 1 - 2 * h
    n_dev = n_sp * n_tp
    me = s * n_tp + t
    n_pairs = n_sp // 2
    pair = s // 2
    pos = lax.rem(s, 2)
    partner = s + 1 - 2 * pos
    is_worker = pos == 1 - s // n_pairs
    is_outer = pos == s // n_pairs
    rows, width = latents.shape
    ctx_rows = context.shape[0]
    length = rows * n_tp
    lat_all = 2 * length
    total = hid.shape[1]
    depth = hid.shape[2]
    half = depth // 2
    heads = decay_bias.shape[1] // DK
    dv = head_gain.shape[1]
    rank = decay_up.shape[1]
    span_t = width // n_tp

    def remote(src, dst, send, recv, device):
        return pltpu.make_async_remote_copy(
            src_ref=src,
            dst_ref=dst,
            send_sem=send,
            recv_sem=recv,
            device_id=device,
            device_id_type=MESH,
        )

    def worker_of(p):
        return 2 * p + 1 - p // (n_pairs // 2)

    def tp_peer(k):
        return lax.rem(t + k, n_tp)

    def tp_from(k):
        return lax.rem(t - k + n_tp, n_tp)

    def sp_peer(k):
        return lax.rem(s + k, n_sp)

    def sp_from(k):
        return lax.rem(s - k + n_sp, n_sp)

    weights = ((key_weight, wk), (value_weight, wv), (query_weight, wq))
    local = [pltpu.make_async_copy(modulator, mod_w, loc_sem.at[0])]
    for m, (source, slots) in enumerate(weights):
        for i in range(2):
            local.append(
                pltpu.make_async_copy(
                    source.at[pl.ds(i * half, half)], slots.at[s, i], loc_sem.at[1 + 2 * m + i]
                )
            )
    local.append(pltpu.make_async_copy(out_weight, wo, loc_sem.at[7]))
    barrier = pltpu.get_barrier_semaphore()
    for k in range(1, n_tp):
        pl.semaphore_signal(barrier, inc=1, device_id={"tp": tp_peer(k)}, device_id_type=MESH)
    for k in range(1, n_sp):
        pl.semaphore_signal(barrier, inc=1, device_id={"sp": sp_peer(k)}, device_id_type=MESH)
    pl.semaphore_signal(barrier, inc=1, device_id={"dp": mate}, device_id_type=MESH)
    small = [
        pltpu.make_async_copy(source, target, loc_sem.at[8 + i])
        for i, (source, target) in enumerate(
            (
                (sample_vector_in, sample_vector),
                (context_vector_in, context_vector),
                (latents_in, latents),
                (context_in, context),
                (decay_extra_in, decay_extra),
                (norm_gain_in, norm_gain),
                (decay_down_in, decay_down),
                (decay_up_in, decay_up),
                (decay_bias_in, decay_bias),
                (head_gain_in, head_gain),
            )
        )
    ]
    for copy in small[:5] + local[:1] + small[5:] + local[1:]:
        copy.start()
    small[2].wait()
    small[3].wait()
    small[4].wait()
    pl.semaphore_wait(barrier, n_tp + n_sp - 1)

    def inner():
        return jnp.logical_and(s >= 1, s <= n_sp - 2)

    def onward(r):
        return s + 1 <= n_sp - 2 if r == 0 else s - 1 >= 1

    def exists(r, j):
        return jnp.logical_and(inner(), s - j >= 0 if r == 0 else s + j < n_sp)

    def origin_of(r, j):
        return s - j if r == 0 else s + j

    def ring_copy(m, r, j, first=False):
        source, slots = weights[m]
        origin = origin_of(r, j)
        src = source.at[pl.ds(h * half, half)] if first else slots.at[origin, h]
        target = s + 1 if r == 0 else s - 1
        return remote(src, slots.at[origin, h], w_s.at[m, r, j], w_r.at[m, r, j], {"sp": target})

    def ring_arrival(m, r, j):
        view = weights[m][1].at[origin_of(r, j), h]
        return remote(view, view, w_s.at[m, r, j - 1], w_r.at[m, r, j - 1], {"sp": s})

    def mate_copy(m, r, j, side):
        view = weights[m][1].at[origin_of(r, j), side]
        return remote(view, view, p_s.at[m, r, j - 1], p_r.at[m, r, j - 1], {"dp": mate})

    def send_own(m):
        for r in range(2):

            @pl.when(onward(r))
            def _():
                ring_copy(m, r, 0, True).start()

    def relay(m, j, share):
        for r in range(2):

            @pl.when(exists(r, j))
            def _():
                ring_arrival(m, r, j).wait_recv()

                @pl.when(onward(r))
                def _():
                    ring_copy(m, r, j).start()

                if share:
                    mate_copy(m, r, j, h).start()

    def whole(slots, o):
        return slots[o].reshape(depth, slots.shape[3])

    def multiply(m, j, acc, count):
        slots = weights[m][1]
        for r in range(2):

            @pl.when(exists(r, j))
            def _():
                origin = origin_of(r, j)
                mate_copy(m, r, j, 1 - h).wait_recv()
                acc[...] += dot(hid[origin, 0:count], whole(slots, origin))

    def lat_copy(k):
        return remote(latents, lat.at[pos, t], lat_s.at[0, k], lat_r.at[0, k], {"tp": tp_peer(k)})

    def lat_arrival(k):
        view = lat.at[pos, tp_from(k)]
        return remote(view, view, lat_s.at[0, k], lat_r.at[0, k], {"tp": t})

    def outer_lat():
        return remote(latents, lat.at[pos, t], lo_s, lo_r, {"sp": partner})

    def outer_lat_arrival():
        view = lat.at[1 - pos, t]
        return remote(view, view, lo_s, lo_r, {"sp": s})

    def lat_relay(k, owner, to):
        view = lat.at[1 - pos, owner]
        return remote(view, view, lat_s.at[1, k], lat_r.at[1, k], {"tp": to})

    def ctx_cols(owner):
        return pl.ds(pl.multiple_of(owner * span_t, span_t), span_t)

    def ctx_copy():
        return remote(
            context.at[:, ctx_cols(t)],
            outer_context.at[:, ctx_cols(t)],
            cx_s.at[0],
            cx_r.at[0],
            {"sp": partner},
        )

    def ctx_relay(k, owner, to):
        view = outer_context.at[:, ctx_cols(owner)]
        return remote(view, view, cx_s.at[k], cx_r.at[k], {"tp": to})

    def extra_copy():
        return remote(decay_extra, extras.at[pos], up_s, up_r, {"sp": partner})

    def extra_arrival():
        view = extras.at[1 - pos]
        return remote(view, view, up_s, up_r, {"sp": s})

    @pl.when(is_outer)
    def _():
        outer_lat().start()
        extra_copy().start()
        ctx_copy().start()
        for m in range(3):
            send_own(m)

    @pl.when(is_worker)
    def _():
        for k in range(1, n_tp):
            lat_copy(k).start()
        send_own(0)
        send_own(1)

    small[0].wait()
    small[1].wait()
    is_first = lax.broadcasted_iota(jnp.int32, (16, width), 0) == 0
    vectors = jnp.where(is_first, sample_vector[...], context_vector[...])
    conditions = (vectors / (1.0 + jnp.exp(-vectors))).astype(BF16)
    local[0].wait()
    mods[me] = dot(conditions, mod_w[...])[0:2]

    def mod_tp(k, owner, to):
        view = mods.at[s * n_tp + owner]
        return remote(view, view, mt_s.at[k], mt_r.at[k], {"tp": to})

    def mod_sp(k, owner, to):
        view = mods.at[pl.ds(owner * n_tp, n_tp)]
        return remote(view, view, ms_s.at[k], ms_r.at[k], {"sp": to})

    for k in range(1, n_tp):
        mod_tp(k, t, tp_peer(k)).start()
    for k in range(1, n_tp):
        mod_tp(k, tp_from(k), t).wait_recv()
    for k in range(1, n_sp):
        mod_sp(k, s, sp_peer(k)).start()
    for copy in small[5:]:
        copy.wait()

    def modulation_now():
        for k in range(1, n_sp):
            mod_sp(k, sp_from(k), s).wait_recv()

    def mod_part(i):
        return jnp.concatenate([mods[j] for j in range(n_dev)], axis=1)[
            :, i * width : (i + 1) * width
        ]

    def tot_copy(k, owner, to):
        view = tots.at[owner]
        return remote(view, view, tt_s.at[k], tt_r.at[k], {"sp": to})

    def has_pred(z):
        return pair > 0 if z == 0 else pair < n_pairs - 1

    def has_succ(z):
        return pair < n_pairs - 1 if z == 0 else pair > 0

    def lone(a, b):
        return jnp.logical_and(a, jnp.logical_not(b))

    def f_copy(z, g):
        to = worker_of(pair + 1) if z == 0 else worker_of(pair - 1)
        return remote(f_out.at[z, g], f_in.at[z, g], f_s.at[z, g], f_r.at[z, g], {"sp": to})

    def g_copy(z, g):
        to = worker_of(pair - 1) if z == 0 else worker_of(pair + 1)
        return remote(g_out.at[z, g], g_in.at[z, g], g_s.at[z, g], g_r.at[z, g], {"sp": to})

    def o_copy(g, where, to):
        view = normed.at[where, g]
        return remote(view, view, o_s.at[g], o_r.at[g], {"sp": to})

    def work():
        outer_lat_arrival().wait_recv()
        for k in range(1, n_tp):
            lat_relay(k, t, tp_peer(k)).start()
        remote(
            outer_context.at[:, ctx_cols(t)],
            outer_context.at[:, ctx_cols(t)],
            cx_s.at[0],
            cx_r.at[0],
            {"sp": s},
        ).wait_recv()
        for k in range(1, n_tp):
            ctx_relay(k, t, tp_peer(k)).start()
        relay(0, 1, True)
        send_own(2)

        lat[pos, t] = latents[...]
        for k in range(1, n_tp):
            lat_arrival(k).wait_recv()
        modulation_now()
        shift = mod_part(0)
        scale = mod_part(1)

        def modulated(x, row):
            x = x.astype(F32)
            x = x * lax.rsqrt(jnp.mean(x * x, axis=-1, keepdims=True) + EPS) * norm_gain[...]
            return (x * (1.0 + scale[row : row + 1]) + shift[row : row + 1]).astype(BF16)

        piece = min(32, ctx_rows)

        def put(x, at):
            count = x.shape[0]
            at = pl.multiple_of(at, piece)
            for o in range(n_sp):
                hid[o, pl.ds(at, count)] = x[:, o * depth : (o + 1) * depth]

        for i in range(n_tp):
            put(modulated(lat[pos, i], 0), pos * length + i * rows)
        for i in range(ctx_rows // piece):
            put(
                modulated(context[i * piece : (i + 1) * piece], 1),
                lat_all + pos * ctx_rows + i * piece,
            )
        for k in range(1, n_tp):
            lat_relay(k, tp_from(k), t).wait_recv()
        relay(1, 1, True)
        for i in range(n_tp):
            put(modulated(lat[1 - pos, i], 0), (1 - pos) * length + i * rows)
        for k in range(1, n_tp):
            ctx_relay(k, tp_from(k), t).wait_recv()
        for i in range(ctx_rows // piece):
            put(
                modulated(outer_context[i * piece : (i + 1) * piece], 1),
                lat_all + (1 - pos) * ctx_rows + i * piece,
            )

        low = dot_nt(hid[0], decay_down[:, 0:depth])
        for o in range(1, n_sp):
            low = low + dot_nt(hid[o], decay_down[:, o * depth : (o + 1) * depth])
        low = low.astype(BF16)
        relay(2, 1, True)

        def log_decays(z):
            x = dot(low[:, z * rank : (z + 1) * rank], decay_up[z]) + decay_bias[z : z + 1]
            return log_sigmoid(x) / SHARP

        row_id = lax.broadcasted_iota(jnp.int32, (lat_all, lat_all), 0)
        col_id = lax.broadcasted_iota(jnp.int32, (lat_all, lat_all), 1)
        same = row_id // BLOCK == col_id // BLOCK
        within_mask = [same & (col_id <= row_id), same & (col_id >= row_id)]
        extras[pos] = decay_extra[...]
        extra_arrival().wait_recv()

        def extra_sums(z):
            columns = []
            for g in range(heads):
                line = jnp.concatenate([extras[i, z, g : g + 1, :] for i in range(2)], axis=1)
                columns.append(
                    jnp.sum(jnp.where(within_mask[z], line, 0.0), axis=1, keepdims=True)
                )
            return jnp.concatenate([jnp.broadcast_to(c, (lat_all, DK)) for c in columns], axis=1)

        decays = [log_decays(z) for z in range(2)]
        within = [sums(within_mask[z], decays[z][:lat_all]) + extra_sums(z) for z in range(2)]
        blocks = lat_all // BLOCK
        totals = [
            [within[0][(b + 1) * BLOCK - 1 : (b + 1) * BLOCK] for b in range(blocks)],
            [within[1][b * BLOCK : b * BLOCK + 1] for b in range(blocks)],
        ]
        none = jnp.zeros_like(totals[0][0])

        def between(z, lo, hi):
            value = none
            for b in range(lo, hi):
                value = value + totals[z][b]
            return value

        crow = lax.broadcasted_iota(jnp.int32, (total - lat_all, total - lat_all), 0)
        ccol = lax.broadcasted_iota(jnp.int32, (total - lat_all, total - lat_all), 1)
        after = [
            sums(ccol > crow, decays[0][lat_all:]),
            sums(ccol < crow, decays[1][lat_all:]),
        ]
        lat_total = [between(z, 0, blocks) for z in range(2)]
        ctx_total = [
            after[0][0:1] + decays[0][lat_all : lat_all + 1],
            after[1][total - lat_all - 1 :] + decays[1][total - 1 :],
        ]
        tots[pair] = jnp.concatenate(lat_total + ctx_total, axis=0)
        for k in range(1, n_pairs):
            to = lax.rem(pair + k, n_pairs)
            tot_copy(k, pair, worker_of(to)).start()

        for copy in local[1:5]:
            copy.wait()
        acc_k[...] = dot(hid[s], whole(wk, s))
        acc_v[...] = dot(hid[s], whole(wv, s))
        multiply(0, 1, acc_k, total)
        multiply(1, 1, acc_v, total)
        for k in range(1, n_pairs):
            tot_copy(k, lax.rem(pair - k + n_pairs, n_pairs), s).wait_recv()
        before = [none, none]
        suffix = [none, none]
        for u in range(n_pairs):
            line = tots[u]
            below = jnp.where(u < pair, 1.0, 0.0)
            above = jnp.where(u > pair, 1.0, 0.0)
            before[0] = before[0] + below * line[0:1]
            before[1] = before[1] + above * line[1:2]
            suffix[0] = suffix[0] + above * line[2:3]
            suffix[1] = suffix[1] + below * line[3:4]
        ctx_weight = [jnp.exp(after[z] + suffix[z]) for z in range(2)]

        def per_block(f):
            return jnp.concatenate([f(b) for b in range(blocks)], axis=0)

        def rows_of(x, b):
            return x[b * BLOCK : (b + 1) * BLOCK]

        ending = [
            jnp.exp(
                per_block(
                    lambda b: totals[0][b] - rows_of(within[0], b) + between(0, b + 1, blocks)
                )
            ),
            jnp.exp(per_block(lambda b: totals[1][b] - rows_of(within[1], b) + between(1, 0, b))),
        ]
        for j in range(2, max(n_sp - 1, 2)):
            relay(0, j, True)
            multiply(0, j, acc_k, total)
            relay(1, j, True)
            multiply(1, j, acc_v, total)
        keys = acc_k[...].astype(BF16)
        values = acc_v[...].astype(BF16)
        ckeys = keys[lat_all:].astype(F32)
        cvals = values[lat_all:]
        keys = keys[:lat_all].astype(F32)
        values = values[:lat_all]

        def columns(g, n):
            return slice(g * n, (g + 1) * n)

        for z in range(2):
            ended = (keys * ending[z]).astype(BF16)
            cended = (ckeys * ctx_weight[z]).astype(BF16)
            lift = CTX_LIFT * jnp.exp(before[z])
            lift_on = CTX_LIFT * jnp.exp(before[z] + lat_total[z])
            for g in range(heads):
                c = dot_tn(cvals[:, columns(g, dv)], cended[:, columns(g, DK)])
                g_out[z, g] = c.astype(BF16)
                own = dot_tn(values[:, columns(g, dv)], ended[:, columns(g, DK)])
                f_out[z, g] = (own + lift_on[:, columns(g, DK)] * c).astype(BF16)
                if n_pairs > 2:
                    c_state[z, g] = c
                    l_state[z, g] = own + lift_on[:, columns(g, DK)] * c
                state[z, g] = lift[:, columns(g, DK)] * c

                @pl.when(lone(has_succ(z), has_pred(z)))
                def _():
                    f_copy(z, g).start()

                @pl.when(lone(has_pred(z), has_succ(z)))
                def _():
                    g_copy(z, g).start()

        if n_pairs > 2:
            for z in range(2):

                @pl.when(jnp.logical_and(has_pred(z), has_succ(z)))
                def _():
                    for g in range(heads):
                        f_copy(z, g).wait_recv()
                        on = jnp.exp(lat_total[z])[:, columns(g, DK)]
                        f_out[z, g] = (l_state[z, g] + on * f_in[z, g].astype(F32)).astype(BF16)
                        f_copy(z, g).start()

                @pl.when(jnp.logical_and(has_pred(z), has_succ(z)))
                def _():
                    for g in range(heads):
                        g_copy(z, g).wait_recv()
                        g_out[z, g] = (c_state[z, g] + g_in[z, g].astype(F32)).astype(BF16)
                        g_copy(z, g).start()

        for z in range(2):
            close = (keys * jnp.exp(-within[z])).astype(BF16)
            near = keys * jnp.exp(per_block(lambda b: totals[z][b] - rows_of(within[z], b)))
            for i in range(blocks):
                for j in range(blocks):
                    if i == j:
                        block = rows_of(close, j)
                    elif (j < i) == (z == 0):
                        gap = between(z, min(i, j) + 1, max(i, j))
                        block = (rows_of(near, j) * jnp.exp(gap)).astype(BF16)
                    else:
                        block = jnp.zeros((BLOCK, heads * DK), BF16)
                    key_rows[z, i, j * BLOCK : (j + 1) * BLOCK] = block
        reach = [jnp.exp(within[z]) for z in range(2)]
        lifted_by = [
            jnp.exp(per_block(lambda b: rows_of(within[0], b) + between(0, 0, b))),
            jnp.exp(per_block(lambda b: rows_of(within[1], b) + between(1, b + 1, blocks))),
        ]

        for copy in local[5:7]:
            copy.wait()
        acc_q[...] = dot(hid[s, 0:lat_all], whole(wq, s))
        for j in range(1, max(n_sp - 1, 2)):
            if j > 1:
                relay(2, j, True)
            multiply(2, j, acc_q, lat_all)
        queries = acc_q[...].astype(BF16).astype(F32)

        for z in range(2):
            near_rows = (queries * reach[z]).astype(BF16)
            far_rows = (queries * lifted_by[z]).astype(BF16)
            for b in range(blocks):
                query_rows[0, z, b] = rows_of(near_rows, b)
                query_rows[1, z, b] = rows_of(far_rows, b)
        turn = blocks // 2
        row_in = lax.broadcasted_iota(jnp.int32, (BLOCK, lat_all), 0)
        col_in = lax.broadcasted_iota(jnp.int32, (BLOCK, lat_all), 1)

        def inside(where, g):
            lines = []
            for b in range(turn):
                i = where * turn + b
                ids = row_in + i * BLOCK
                masks = [col_in <= ids, col_in >= ids]
                line = 0.0
                for z in range(2):
                    score = dot_nt(
                        query_rows[0, z, i, :, columns(g, DK)], key_rows[z, i, :, columns(g, DK)]
                    )
                    line = line + jnp.where(masks[z], score, 0.0)
                lines.append(line.astype(BF16))
            return dot(jnp.concatenate(lines, axis=0), values[:, columns(g, dv)])

        def finish(where, g, mixed):
            for z in range(2):
                rows_z = query_rows[1, z, pl.ds(where * turn, turn), :, columns(g, DK)]
                mixed = mixed + dot_nt(rows_z.reshape(length, DK), state[z, g].astype(BF16))
            by = lax.rsqrt(jnp.mean(mixed * mixed, axis=-1, keepdims=True) + EPS)
            normed[where, g] = (mixed * by * head_gain[...]).astype(BF16)

        first = [inside(1 - pos, g) for g in range(heads)]
        for z in range(2):
            lift = CTX_LIFT * jnp.exp(before[z])

            @pl.when(has_pred(z))
            def _():
                for g in range(heads):
                    if n_pairs == 2:
                        f_copy(z, g).wait_recv()
                    else:

                        @pl.when(jnp.logical_not(has_succ(z)))
                        def _():
                            f_copy(z, g).wait_recv()

                    state[z, g] += f_in[z, g].astype(F32)

            @pl.when(has_succ(z))
            def _():
                for g in range(heads):
                    if n_pairs == 2:
                        g_copy(z, g).wait_recv()
                    else:

                        @pl.when(jnp.logical_not(has_pred(z)))
                        def _():
                            g_copy(z, g).wait_recv()

                    state[z, g] += lift[:, columns(g, DK)] * g_in[z, g].astype(F32)

        for g in range(heads):
            finish(1 - pos, g, first[g])
            o_copy(g, 1 - pos, partner).start()
        for g in range(heads):
            finish(pos, g, inside(pos, g))

    pl.when(is_worker)(work)

    @pl.when(is_outer)
    def _():
        for copy in local[1:7]:
            copy.wait()
        for m in range(3):
            relay(m, 1, False)
        for j in range(2, n_sp - 1):
            relay(0, j, False)
            relay(1, j, False)
        for j in range(2, n_sp - 1):
            relay(2, j, False)
        modulation_now()
        for g in range(heads):
            o_copy(g, pos, s).wait_recv()

    gate = mod_part(2)[0:1]
    local[7].wait()
    chunks = rs_s.shape[1]
    span = width // chunks
    rs_copies = []
    for c in range(chunks):
        cols = slice(c * span, (c + 1) * span)
        product = dot(normed[pos, 0], wo[0:dv, cols])
        for g in range(1, heads):
            product = product + dot(normed[pos, g], wo[g * dv : (g + 1) * dv, cols])
        product = product.astype(BF16)
        for i in range(n_tp):
            part[i, :, cols] = product[i * rows : (i + 1) * rows]
        for k in range(1, n_tp):
            to = tp_peer(k)
            copy = remote(
                part.at[to, :, pl.ds(c * span, span)],
                rs.at[k, :, pl.ds(c * span, span)],
                rs_s.at[k, c],
                rs_r.at[k, c],
                {"tp": to},
            )
            copy.start()
            rs_copies.append(copy)
    for c in range(chunks):
        cols = slice(c * span, (c + 1) * span)
        summed = part[t, :, cols].astype(F32)
        for k in range(1, n_tp):
            rs_copies[c * (n_tp - 1) + k - 1].wait_recv()
            summed = summed + rs[k, :, cols].astype(F32)
        projected = summed.astype(BF16).astype(F32)
        out[:, cols] = (latents[:, cols].astype(F32) + gate[:, cols] * projected).astype(BF16)

    for copy in rs_copies:
        copy.wait_send()
    for k in range(1, n_tp):
        mod_tp(k, t, tp_peer(k)).wait_send()
    for k in range(1, n_sp):
        mod_sp(k, s, sp_peer(k)).wait_send()

    @pl.when(is_outer)
    def _():
        outer_lat().wait_send()
        extra_copy().wait_send()
        ctx_copy().wait_send()

    @pl.when(is_worker)
    def _():
        for k in range(1, n_tp):
            lat_copy(k).wait_send()
            lat_relay(k, t, tp_peer(k)).wait_send()
            ctx_relay(k, t, tp_peer(k)).wait_send()
        for k in range(1, n_pairs):
            tot_copy(k, pair, s).wait_send()
        for g in range(heads):
            o_copy(g, 1 - pos, partner).wait_send()
            for z in range(2):

                @pl.when(has_succ(z))
                def _():
                    f_copy(z, g).wait_send()

                @pl.when(has_pred(z))
                def _():
                    g_copy(z, g).wait_send()

    for m in range(3):
        for r in range(2):

            @pl.when(onward(r))
            def _():
                ring_copy(m, r, 0, True).wait_send()

            for j in range(1, n_sp - 1):

                @pl.when(exists(r, j))
                def _():
                    @pl.when(onward(r))
                    def _():
                        ring_copy(m, r, j).wait_send()

                    @pl.when(is_worker)
                    def _():
                        mate_copy(m, r, j, h).wait_send()


def chain_per_device(n_sp, n_tp, *args):
    (latents, sv, context, cv, gain, modulator, wq, wk, wv, down, up, bias, extra, hg, wo) = args
    rows, width = latents.shape
    ctx_rows = context.shape[0]
    n_dev = n_sp * n_tp
    n_pairs = n_sp // 2
    length = rows * n_tp
    total = 2 * (length + ctx_rows)
    depth = wq.shape[0]
    kw, vw = wk.shape[1], wv.shape[1]
    heads = bias.shape[1] // DK
    dv = hg.shape[0]
    chunks = 4
    vmem = pl.BlockSpec(memory_space=pltpu.VMEM)
    hbm = pl.BlockSpec(memory_space=pl.ANY)
    dma = pltpu.SemaphoreType.DMA
    states = (2, heads, dv, DK)
    chained = states if n_pairs > 2 else (2, heads, 8, DK)
    scratch = [
        pltpu.VMEM(latents.shape, BF16),
        pltpu.VMEM(sv.shape, F32),
        pltpu.VMEM(context.shape, BF16),
        pltpu.VMEM(cv.shape, F32),
        pltpu.VMEM((1, width), F32),
        pltpu.VMEM(down.shape[::-1], BF16),
        pltpu.VMEM(up.shape, BF16),
        pltpu.VMEM(bias.shape, F32),
        pltpu.VMEM((2, heads, length), F32),
        pltpu.VMEM((1, dv), F32),
        pltpu.VMEM(modulator.shape, BF16),
        pltpu.VMEM((n_dev, 2, modulator.shape[1]), F32),
        pltpu.VMEM((2, n_tp, rows, width), BF16),
        pltpu.VMEM((ctx_rows, width), BF16),
        pltpu.VMEM((2, 2, heads, length), F32),
        pltpu.VMEM((n_sp, total, depth), BF16),
        pltpu.VMEM((n_sp, 2, depth // 2, kw), BF16),
        pltpu.VMEM((n_sp, 2, depth // 2, vw), BF16),
        pltpu.VMEM((n_sp, 2, depth // 2, kw), BF16),
        pltpu.VMEM(wo.shape, BF16),
        pltpu.VMEM((total, kw), F32),
        pltpu.VMEM((total, vw), F32),
        pltpu.VMEM((2 * length, kw), F32),
        pltpu.VMEM((n_pairs, 4, kw), F32),
        pltpu.VMEM((2, 2 * length // BLOCK, 2 * length, kw), BF16),
        pltpu.VMEM((2, 2, 2 * length // BLOCK, BLOCK, kw), BF16),
        pltpu.VMEM(chained, F32),
        pltpu.VMEM(chained, F32),
        pltpu.VMEM(states, BF16),
        pltpu.VMEM(states, BF16),
        pltpu.VMEM(states, BF16),
        pltpu.VMEM(states, BF16),
        pltpu.VMEM(states, F32),
        pltpu.VMEM((2, heads, length, dv), BF16),
        pltpu.VMEM((n_tp, rows, width), BF16),
        pltpu.VMEM((n_tp, rows, width), BF16),
        dma((18,)),
        dma((n_tp,)),
        dma((n_tp,)),
        dma((n_sp,)),
        dma((n_sp,)),
        dma((2, n_tp)),
        dma((2, n_tp)),
        dma,
        dma,
        dma((n_tp,)),
        dma((n_tp,)),
        dma,
        dma,
        dma((3, 2, n_sp)),
        dma((3, 2, n_sp)),
        dma((3, 2, n_sp)),
        dma((3, 2, n_sp)),
        dma((n_pairs,)),
        dma((n_pairs,)),
        dma((2, heads)),
        dma((2, heads)),
        dma((2, heads)),
        dma((2, heads)),
        dma((heads,)),
        dma((heads,)),
        dma((n_tp, chunks)),
        dma((n_tp, chunks)),
    ]
    return pl.pallas_call(
        functools.partial(chain_kernel, n_sp, n_tp),
        out_shape=jax.ShapeDtypeStruct(latents.shape, BF16),
        in_specs=[hbm] * 15,
        out_specs=vmem,
        scratch_shapes=scratch,
        compiler_params=pltpu.CompilerParams(
            collective_id=0, has_side_effects=True, vmem_limit_bytes=56 * 1024 * 1024
        ),
    )(
        latents,
        sv,
        context,
        cv,
        gain.reshape(1, -1),
        modulator,
        wq,
        wk,
        wv,
        down.T,
        up,
        bias,
        extra.transpose(0, 2, 1),
        hg.reshape(1, -1),
        wo,
    )


def kernel(
    n_sp,
    n_tp,
    latents_in,
    sample_vector_in,
    context_in,
    context_vector_in,
    norm_gain_in,
    modulator,
    query_weight,
    key_weight,
    value_weight,
    decay_down_in,
    decay_up_in,
    decay_bias_in,
    decay_extra_in,
    head_gain_in,
    out_weight,
    out,
    latents,
    sample_vector,
    context,
    context_vector,
    norm_gain,
    decay_down,
    decay_up,
    decay_bias,
    decay_extra,
    head_gain,
    mod_w,
    mods,
    lat,
    ctx,
    extras,
    hid,
    wk,
    wv,
    wq,
    wo,
    acc_k,
    acc_v,
    acc_q,
    key_rows,
    o_out,
    normed,
    part,
    rs,
    loc_sem,
    mt_s,
    mt_r,
    ms_s,
    ms_r,
    lo_s,
    lo_r,
    cx_s,
    cx_r,
    ex_s,
    ex_r,
    em_s,
    em_r,
    lp_s,
    lp_r,
    cp_s,
    cp_r,
    hd_s,
    hd_r,
    w_s,
    w_r,
    o_s,
    o_r,
    rs_s,
    rs_r,
):
    s = lax.axis_index("sp")
    t = lax.axis_index("tp")
    d = lax.axis_index("dp")
    h = lax.rem(d, 2)
    mate = d + 1 - 2 * h
    n_dev = n_sp * n_tp
    me = s * n_tp + t
    first_plane = n_sp // 2 - 1
    last_plane = n_sp // 2
    side = s - first_plane
    target = first_plane + h
    is_worker = jnp.logical_and(s >= first_plane, s <= last_plane)
    is_leader = s == target
    is_follower = jnp.logical_and(is_worker, s != target)
    is_sender = s != target
    rows, width = latents.shape
    ctx_rows = context.shape[0]
    length = rows * n_tp
    lat_all = n_sp * length
    total = hid.shape[1]
    depth = hid.shape[2]
    heads = decay_bias.shape[1] // DK
    dv = head_gain.shape[1]
    rank = decay_up.shape[1]
    span_t = width // n_tp

    def remote(src, dst, send, recv, device):
        return pltpu.make_async_remote_copy(
            src_ref=src,
            dst_ref=dst,
            send_sem=send,
            recv_sem=recv,
            device_id=device,
            device_id_type=MESH,
        )

    def tp_peer(k):
        return lax.rem(t + k, n_tp)

    def tp_from(k):
        return lax.rem(t - k + n_tp, n_tp)

    def sp_peer(k):
        return lax.rem(s + k, n_sp)

    def sp_from(k):
        return lax.rem(s - k + n_sp, n_sp)

    def head_cols(size):
        return pl.ds(pl.multiple_of(h * size, DK), size)

    weights = ((key_weight, wk, DK), (value_weight, wv, dv), (query_weight, wq, DK))
    own_weight = [
        pltpu.make_async_copy(source.at[:, head_cols(size)], slots.at[s], loc_sem.at[1 + m])
        for m, (source, slots, size) in enumerate(weights)
    ]
    mod_load = pltpu.make_async_copy(modulator, mod_w, loc_sem.at[0])
    out_load = pltpu.make_async_copy(out_weight, wo, loc_sem.at[4])
    barrier = pltpu.get_barrier_semaphore()
    for k in range(1, n_tp):
        pl.semaphore_signal(barrier, inc=1, device_id={"tp": tp_peer(k)}, device_id_type=MESH)
    for k in range(1, n_sp):
        pl.semaphore_signal(barrier, inc=1, device_id={"sp": sp_peer(k)}, device_id_type=MESH)
    pl.semaphore_signal(barrier, inc=1, device_id={"dp": mate}, device_id_type=MESH)
    small = [
        pltpu.make_async_copy(source, where, loc_sem.at[8 + i])
        for i, (source, where) in enumerate(
            (
                (sample_vector_in, sample_vector),
                (context_vector_in, context_vector),
                (latents_in, latents),
                (context_in, context),
                (decay_extra_in, decay_extra),
                (norm_gain_in, norm_gain),
                (decay_down_in, decay_down),
                (decay_up_in, decay_up),
                (decay_bias_in, decay_bias),
                (head_gain_in, head_gain),
            )
        )
    ]
    for copy in small[:5] + own_weight + [mod_load] + small[5:] + [out_load]:
        copy.start()
    for copy in small[2:5] + own_weight:
        copy.wait()
    pl.semaphore_wait(barrier, n_tp + n_sp - 1)

    def onward(r):
        return s + 1 <= last_plane if r == 0 else s - 1 >= first_plane

    def exists(r, j):
        if r == 0:
            return jnp.logical_and(s <= last_plane, s - j >= 0)
        return jnp.logical_and(s >= first_plane, s + j < n_sp)

    def origin_of(r, j):
        return s - j if r == 0 else s + j

    def ring_copy(m, r, j):
        view = weights[m][1].at[origin_of(r, j)]
        to = s + 1 if r == 0 else s - 1
        return remote(view, view, w_s.at[m, r, j], w_r.at[m, r, j], {"sp": to})

    def ring_arrival(m, r, j):
        view = weights[m][1].at[origin_of(r, j)]
        return remote(view, view, w_s.at[m, r, j - 1], w_r.at[m, r, j - 1], {"sp": s})

    def relay(m, j):
        for r in range(2):

            @pl.when(exists(r, j))
            def _():
                ring_arrival(m, r, j).wait_recv()

                @pl.when(onward(r))
                def _():
                    ring_copy(m, r, j).start()

    def multiply(m, j, acc, count):
        slots = weights[m][1]
        for r in range(2):

            @pl.when(exists(r, j))
            def _():
                origin = origin_of(r, j)
                acc[...] += dot(hid[origin, 0:count], slots[origin])

    def lat_in(b, to):
        view = lat.at[b, t]
        return remote(latents, view, lo_s, lo_r.at[b], {"sp": to})

    def extra_in(b, to):
        return remote(decay_extra, extras.at[b], ex_s, ex_r.at[b], {"sp": to})

    def ctx_cols(owner):
        return pl.ds(pl.multiple_of(owner * span_t, span_t), span_t)

    def ctx_in(b, to):
        return remote(
            context.at[:, ctx_cols(t)],
            ctx.at[b, :, ctx_cols(t)],
            cx_s,
            cx_r.at[b],
            {"sp": to},
        )

    def lat_plane(b, k, owner, to):
        view = lat.at[b, owner]
        return remote(view, view, lp_s.at[b, k], lp_r.at[b, k], {"tp": to})

    def lat_own(k):
        return remote(latents, lat.at[s, t], lp_s.at[s, k], lp_r.at[s, k], {"tp": tp_peer(k)})

    def ctx_plane(b, k, owner, to):
        view = ctx.at[b, :, ctx_cols(owner)]
        return remote(view, view, cp_s.at[b, k], cp_r.at[b, k], {"tp": to})

    def hid_copy(i, at, count):
        view = hid.at[:, pl.ds(pl.multiple_of(at, 16), count)]
        return remote(view, view, hd_s.at[i], hd_r.at[i], {"dp": mate})

    def lat_hid(b):
        return hid_copy(b, b * length, length)

    def ctx_hid(b):
        return hid_copy(n_sp + b, lat_all + b * ctx_rows, ctx_rows)

    def extra_mate():
        return remote(extras, extras, em_s, em_r, {"dp": mate})

    def others():
        towards = 1 - 2 * side
        steps = sorted(range(-first_plane, n_sp // 2 + 1), key=abs)
        return [s + towards * step for step in steps if step]

    @pl.when(is_sender)
    def _():
        lat_in(s, target).start()
        extra_in(s, target).start()
        ctx_in(s, target).start()

    @pl.when(is_leader)
    def _():
        for k in range(1, n_tp):
            lat_own(k).start()

    for m in range(3):
        for r in range(2):

            @pl.when(onward(r))
            def _():
                ring_copy(m, r, 0).start()

    small[0].wait()
    small[1].wait()
    is_first = lax.broadcasted_iota(jnp.int32, (16, width), 0) == 0
    vectors = jnp.where(is_first, sample_vector[...], context_vector[...])
    conditions = (vectors / (1.0 + jnp.exp(-vectors))).astype(BF16)
    mod_load.wait()
    mods[me] = dot(conditions, mod_w[...])[0:2]

    def mod_tp(k, owner, to):
        view = mods.at[s * n_tp + owner]
        return remote(view, view, mt_s.at[k], mt_r.at[k], {"tp": to})

    def mod_sp(k, owner, to):
        view = mods.at[pl.ds(owner * n_tp, n_tp)]
        return remote(view, view, ms_s.at[k], ms_r.at[k], {"sp": to})

    for k in range(1, n_tp):
        mod_tp(k, t, tp_peer(k)).start()
    for k in range(1, n_tp):
        mod_tp(k, tp_from(k), t).wait_recv()
    for k in range(1, n_sp):
        mod_sp(k, s, sp_peer(k)).start()
    for copy in small[5:]:
        copy.wait()

    def mod_part(i):
        return jnp.concatenate([mods[j] for j in range(n_dev)], axis=1)[
            :, i * width : (i + 1) * width
        ]

    def mods_arrive():
        for k in range(1, n_sp):
            mod_sp(k, sp_from(k), s).wait_recv()

    piece = min(32, ctx_rows)

    def put(x, row, at):
        count = x.shape[0]
        x = x.astype(F32)
        x = x * lax.rsqrt(jnp.mean(x * x, axis=-1, keepdims=True) + EPS) * norm_gain[...]
        scale = mod_part(1)[row : row + 1]
        shift = mod_part(0)[row : row + 1]
        x = (x * (1.0 + scale) + shift).astype(BF16)
        at = pl.multiple_of(at, piece)
        for o in range(n_sp):
            hid[o, pl.ds(at, count)] = x[:, o * depth : (o + 1) * depth]

    def o_copy(b):
        lead = jnp.where(side == h, d, mate)
        return remote(
            o_out.at[b], normed.at[h], o_s.at[b], o_r.at[h], {"sp": b, "dp": lead}
        )

    def o_mate():
        return remote(o_out.at[s], normed.at[h], o_s.at[s], o_r.at[h], {"dp": mate})

    def o_arrival(c):
        return remote(normed.at[c], normed.at[c], o_s.at[s], o_r.at[c], {"dp": mate})

    def work():
        blocks = lat_all // BLOCK
        per = length // BLOCK

        @pl.when(is_leader)
        def _():
            for b in others():
                remote(lat.at[b, t], lat.at[b, t], lo_s, lo_r.at[b], {"sp": s}).wait_recv()
                for k in range(1, n_tp):
                    lat_plane(b, k, t, tp_peer(k)).start()
            for b in others():
                view = ctx.at[b, :, ctx_cols(t)]
                remote(view, view, cx_s, cx_r.at[b], {"sp": s}).wait_recv()
                for k in range(1, n_tp):
                    ctx_plane(b, k, t, tp_peer(k)).start()
            lat[s, t] = latents[...]
            mods_arrive()
            for i, b in enumerate([s] + others()):
                for k in range(1, n_tp):
                    lat_plane(b, k, tp_from(k), t).wait_recv()
                for u in range(n_tp):
                    put(lat[b, u], 0, b * length + u * rows)
                lat_hid(b).start()
                if i == 0:
                    relay(0, 1)
                    extras[s] = decay_extra[...]
                    for c in others():
                        remote(
                            extras.at[c], extras.at[c], ex_s, ex_r.at[c], {"sp": s}
                        ).wait_recv()
                    extra_mate().start()
                if i == 2:
                    relay(1, 1)

        @pl.when(is_follower)
        def _():
            relay(0, 1)
            relay(1, 1)
            mods_arrive()
            extra_mate().wait_recv()
            for b in range(n_sp):
                lat_hid(b).wait_recv()

        def lows(lo, hi):
            value = dot_nt(hid[0, lo:hi], decay_down[:, 0:depth])
            for o in range(1, n_sp):
                value = value + dot_nt(
                    hid[o, lo:hi], decay_down[:, o * depth : (o + 1) * depth]
                )
            return value.astype(BF16)

        def log_decays(low, z):
            x = dot(low[:, z * rank : (z + 1) * rank], decay_up[z, :, head_cols(DK)])
            return log_sigmoid(x + decay_bias[z : z + 1, head_cols(DK)]) / SHARP

        low = lows(0, lat_all)
        relay(2, 1)
        decays = [log_decays(low, z) for z in range(2)]
        group = 2 * length
        row_id = lax.broadcasted_iota(jnp.int32, (group, group), 0)
        col_id = lax.broadcasted_iota(jnp.int32, (group, group), 1)
        same = row_id // BLOCK == col_id // BLOCK
        inner = [same & (col_id <= row_id), same & (col_id >= row_id)]

        def within_of(z):
            pieces = []
            for i in range(lat_all // group):
                line = jnp.concatenate(
                    [extras[2 * i + e, z, pl.ds(h, 1), :] for e in range(2)], axis=1
                )
                extra = jnp.sum(jnp.where(inner[z], line, 0.0), axis=1, keepdims=True)
                pieces.append(sums(inner[z], decays[z][i * group : (i + 1) * group]) + extra)
            return jnp.concatenate(pieces, axis=0)

        within = [within_of(z) for z in range(2)]
        totals = [
            [within[0][(b + 1) * BLOCK - 1 : (b + 1) * BLOCK] for b in range(blocks)],
            [within[1][b * BLOCK : b * BLOCK + 1] for b in range(blocks)],
        ]
        none = jnp.zeros_like(totals[0][0])

        def between(z, lo, hi):
            value = none
            for b in range(lo, hi):
                value = value + totals[z][b]
            return value

        def per_block(f):
            return jnp.concatenate([f(b) for b in range(blocks)], axis=0)

        def rows_of(x, b):
            return x[b * BLOCK : (b + 1) * BLOCK]

        def key_span(z, i):
            if z == 0:
                return 0, min(-(-(i + 1) * BLOCK // DK) * DK, lat_all)
            return i * BLOCK // DK * DK, lat_all

        reach = [jnp.exp(within[z]) for z in range(2)]
        lifted_by = [
            jnp.exp(per_block(lambda b: rows_of(within[0], b) + between(0, 0, b))),
            jnp.exp(per_block(lambda b: rows_of(within[1], b) + between(1, b + 1, blocks))),
        ]

        @pl.when(is_leader)
        def _():
            for i in range(ctx_rows // piece):
                put(
                    context[i * piece : (i + 1) * piece],
                    1,
                    lat_all + s * ctx_rows + i * piece,
                )
            ctx_hid(s).start()
            for b in others():
                for k in range(1, n_tp):
                    ctx_plane(b, k, tp_from(k), t).wait_recv()
                for i in range(ctx_rows // piece):
                    put(
                        ctx[b, i * piece : (i + 1) * piece],
                        1,
                        lat_all + b * ctx_rows + i * piece,
                    )
                ctx_hid(b).start()

        @pl.when(is_follower)
        def _():
            for b in range(n_sp):
                ctx_hid(b).wait_recv()

        low_ctx = lows(lat_all, total)
        ctx_decays = [log_decays(low_ctx, z) for z in range(2)]
        ctx_all = total - lat_all
        crow = lax.broadcasted_iota(jnp.int32, (ctx_all, ctx_all), 0)
        ccol = lax.broadcasted_iota(jnp.int32, (ctx_all, ctx_all), 1)
        ctx_weight = [
            jnp.exp(sums(ccol > crow, ctx_decays[0])),
            jnp.exp(sums(ccol < crow, ctx_decays[1])),
        ]

        acc_k[...] = dot(hid[s], wk[s])
        acc_v[...] = dot(hid[s], wv[s])
        acc_q[...] = dot(hid[s, 0:lat_all], wq[s])
        multiply(0, 1, acc_k, total)
        multiply(1, 1, acc_v, total)
        multiply(2, 1, acc_q, lat_all)
        far = range(2, n_sp // 2 + 1)
        for j in far:
            relay(0, j)
            multiply(0, j, acc_k, total)
        keys = acc_k[...].astype(BF16).astype(F32)
        ckeys = keys[lat_all:]
        keys = keys[:lat_all]
        for z in range(2):
            close = (keys * jnp.exp(-within[z])).astype(BF16)
            near = keys * jnp.exp(per_block(lambda b: totals[z][b] - rows_of(within[z], b)))
            for i in range(blocks):
                lo, hi = key_span(z, i)
                for j in range(lo // BLOCK, hi // BLOCK):
                    if (j > i) if z == 0 else (j < i):
                        block = jnp.zeros((BLOCK, DK), BF16)
                    elif i == j:
                        block = rows_of(close, j)
                    else:
                        gap = between(z, min(i, j) + 1, max(i, j))
                        block = (rows_of(near, j) * jnp.exp(gap)).astype(BF16)
                    key_rows[z, i, j * BLOCK : (j + 1) * BLOCK] = block
        for j in far:
            relay(1, j)
            multiply(1, j, acc_v, total)
        values = acc_v[...].astype(BF16)
        cvals = values[lat_all:]
        values = values[:lat_all]
        state = [
            (CTX_LIFT * dot_tn(cvals, (ckeys * ctx_weight[z]).astype(BF16))).astype(BF16)
            for z in range(2)
        ]
        for j in far:
            relay(2, j)
            multiply(2, j, acc_q, lat_all)
        queries = acc_q[...].astype(BF16).astype(F32)
        query_dec = [(queries * reach[z]).astype(BF16) for z in range(2)]
        lifted = [(queries * lifted_by[z]).astype(BF16) for z in range(2)]

        tri_row = lax.broadcasted_iota(jnp.int32, (BLOCK, lat_all), 0)
        tri_col = lax.broadcasted_iota(jnp.int32, (BLOCK, lat_all), 1)

        def attend(b):
            lines = []
            for i in range(b * per, (b + 1) * per):
                full = []
                for z in range(2):
                    lo, hi = key_span(z, i)
                    score = dot_nt(rows_of(query_dec[z], i), key_rows[z, i, lo:hi])
                    ids = tri_row[:, lo:hi] + i * BLOCK
                    cols = tri_col[:, lo:hi]
                    keep = cols <= ids if z == 0 else cols >= ids
                    score = jnp.where(keep, score, 0.0)
                    pads = [jnp.zeros((BLOCK, lo), F32), score, jnp.zeros((BLOCK, lat_all - hi), F32)]
                    full.append(jnp.concatenate([p for p in pads if p.shape[1]], axis=1))
                lines.append((full[0] + full[1]).astype(BF16))
            mixed = dot(jnp.concatenate(lines, axis=0), values)
            for z in range(2):
                mixed = mixed + dot_nt(lifted[z][b * length : (b + 1) * length], state[z])
            by = lax.rsqrt(jnp.mean(mixed * mixed, axis=-1, keepdims=True) + EPS)
            return (mixed * by * head_gain[...]).astype(BF16)

        for w in range(2):

            @pl.when(side == w)
            def _():
                here = first_plane + w
                order = sorted(range(n_sp), key=lambda b: -abs(b - here))
                for b in order:
                    if b != here:
                        o_out[b] = attend(b)
                        o_copy(b).start()
                        continue
                    result = attend(b)

                    @pl.when(is_leader)
                    def _():
                        normed[h] = result

                    @pl.when(is_follower)
                    def _():
                        o_out[b] = result
                        o_mate().start()

    pl.when(is_worker)(work)

    @pl.when(jnp.logical_not(is_worker))
    def _():
        mods_arrive()

    @pl.when(is_leader)
    def _():
        o_arrival(1 - h).wait_recv()

    @pl.when(is_sender)
    def _():
        for c in range(heads):
            o_arrival(c).wait_recv()

    gate = mod_part(2)[0:1]
    out_load.wait()
    chunks = rs_s.shape[1]
    span = width // chunks
    rs_copies = []
    for c in range(chunks):
        cols = slice(c * span, (c + 1) * span)
        product = dot(normed[0], wo[0:dv, cols])
        for g in range(1, heads):
            product = product + dot(normed[g], wo[g * dv : (g + 1) * dv, cols])
        product = product.astype(BF16)
        for i in range(n_tp):
            part[i, :, cols] = product[i * rows : (i + 1) * rows]
        for k in range(1, n_tp):
            to = tp_peer(k)
            copy = remote(
                part.at[to, :, pl.ds(c * span, span)],
                rs.at[k, :, pl.ds(c * span, span)],
                rs_s.at[k, c],
                rs_r.at[k, c],
                {"tp": to},
            )
            copy.start()
            rs_copies.append(copy)
    for c in range(chunks):
        cols = slice(c * span, (c + 1) * span)
        summed = part[t, :, cols].astype(F32)
        for k in range(1, n_tp):
            rs_copies[c * (n_tp - 1) + k - 1].wait_recv()
            summed = summed + rs[k, :, cols].astype(F32)
        projected = summed.astype(BF16).astype(F32)
        out[:, cols] = (latents[:, cols].astype(F32) + gate[:, cols] * projected).astype(BF16)

    for copy in rs_copies:
        copy.wait_send()
    for k in range(1, n_tp):
        mod_tp(k, t, tp_peer(k)).wait_send()
    for k in range(1, n_sp):
        mod_sp(k, s, sp_peer(k)).wait_send()

    @pl.when(is_sender)
    def _():
        lat_in(s, target).wait_send()
        extra_in(s, target).wait_send()
        ctx_in(s, target).wait_send()

    @pl.when(is_leader)
    def _():
        extra_mate().wait_send()
        for k in range(1, n_tp):
            lat_own(k).wait_send()
            for b in others():
                lat_plane(b, k, t, tp_peer(k)).wait_send()
                ctx_plane(b, k, t, tp_peer(k)).wait_send()
        for b in range(n_sp):
            lat_hid(b).wait_send()
            ctx_hid(b).wait_send()

    @pl.when(is_follower)
    def _():
        o_mate().wait_send()

    @pl.when(is_worker)
    def _():
        for b in others():
            o_copy(b).wait_send()

    for m in range(3):
        for r in range(2):

            @pl.when(onward(r))
            def _():
                ring_copy(m, r, 0).wait_send()

            for j in range(1, n_sp // 2 + 1):

                @pl.when(jnp.logical_and(exists(r, j), onward(r)))
                def _():
                    ring_copy(m, r, j).wait_send()


def per_device(n_sp, n_tp, *args):
    (latents, sv, context, cv, gain, modulator, wq, wk, wv, down, up, bias, extra, hg, wo) = args
    heads = bias.shape[1] // DK
    if n_sp != 4 or heads != 2:
        return chain_per_device(n_sp, n_tp, *args)
    rows, width = latents.shape
    ctx_rows = context.shape[0]
    n_dev = n_sp * n_tp
    length = rows * n_tp
    lat_all = n_sp * length
    total = n_sp * (length + ctx_rows)
    depth = wq.shape[0]
    dv = hg.shape[0]
    chunks = 4
    vmem = pl.BlockSpec(memory_space=pltpu.VMEM)
    hbm = pl.BlockSpec(memory_space=pl.ANY)
    dma = pltpu.SemaphoreType.DMA
    scratch = [
        pltpu.VMEM(latents.shape, BF16),
        pltpu.VMEM(sv.shape, F32),
        pltpu.VMEM(context.shape, BF16),
        pltpu.VMEM(cv.shape, F32),
        pltpu.VMEM((1, width), F32),
        pltpu.VMEM(down.shape[::-1], BF16),
        pltpu.VMEM(up.shape, BF16),
        pltpu.VMEM(bias.shape, F32),
        pltpu.VMEM((2, heads, length), F32),
        pltpu.VMEM((1, dv), F32),
        pltpu.VMEM(modulator.shape, BF16),
        pltpu.VMEM((n_dev, 2, modulator.shape[1]), F32),
        pltpu.VMEM((n_sp, n_tp, rows, width), BF16),
        pltpu.VMEM((n_sp, ctx_rows, width), BF16),
        pltpu.VMEM((n_sp, 2, heads, length), F32),
        pltpu.VMEM((n_sp, total, depth), BF16),
        pltpu.VMEM((n_sp, depth, DK), BF16),
        pltpu.VMEM((n_sp, depth, dv), BF16),
        pltpu.VMEM((n_sp, depth, DK), BF16),
        pltpu.VMEM(wo.shape, BF16),
        pltpu.VMEM((total, DK), F32),
        pltpu.VMEM((total, dv), F32),
        pltpu.VMEM((lat_all, DK), F32),
        pltpu.VMEM((2, lat_all // BLOCK, lat_all, DK), BF16),
        pltpu.VMEM((n_sp, length, dv), BF16),
        pltpu.VMEM((heads, length, dv), BF16),
        pltpu.VMEM((n_tp, rows, width), BF16),
        pltpu.VMEM((n_tp, rows, width), BF16),
        dma((18,)),
        dma((n_tp,)),
        dma((n_tp,)),
        dma((n_sp,)),
        dma((n_sp,)),
        dma,
        dma((n_sp,)),
        dma,
        dma((n_sp,)),
        dma,
        dma((n_sp,)),
        dma,
        dma,
        dma((n_sp, n_tp)),
        dma((n_sp, n_tp)),
        dma((n_sp, n_tp)),
        dma((n_sp, n_tp)),
        dma((2 * n_sp,)),
        dma((2 * n_sp,)),
        dma((3, 2, n_sp)),
        dma((3, 2, n_sp)),
        dma((n_sp,)),
        dma((heads,)),
        dma((n_tp, chunks)),
        dma((n_tp, chunks)),
    ]
    return pl.pallas_call(
        functools.partial(kernel, n_sp, n_tp),
        out_shape=jax.ShapeDtypeStruct(latents.shape, BF16),
        in_specs=[hbm] * 15,
        out_specs=vmem,
        scratch_shapes=scratch,
        compiler_params=pltpu.CompilerParams(
            collective_id=0, has_side_effects=True, vmem_limit_bytes=56 * 1024 * 1024
        ),
    )(
        latents,
        sv,
        context,
        cv,
        gain.reshape(1, -1),
        modulator,
        wq,
        wk,
        wv,
        down.T,
        up,
        bias,
        extra.transpose(0, 2, 1),
        hg.reshape(1, -1),
        wo,
    )


def solution(mesh):
    placed = (
        P(("dp", "sp", "tp"), None),
        P("dp", None),
        P(("dp", "sp"), None),
        P(),
        P(),
        P(None, ("sp", "tp")),
        P("sp", "tp"),
        P("sp", "tp"),
        P("sp", "tp"),
        P(),
        P(None, None, "tp"),
        P(None, "tp"),
        P(None, ("dp", "sp"), "tp"),
        P(),
        P("tp", None),
    )
    return jax.shard_map(
        functools.partial(per_device, mesh.shape["sp"], mesh.shape["tp"]),
        mesh=mesh,
        in_specs=placed,
        out_specs=P(("dp", "sp", "tp"), None),
        check_vma=False,
    )
```

```python
import functools

import jax
import jax.numpy as jnp
from jax import lax
from jax.experimental import pallas as pl
from jax.experimental.pallas import tpu as pltpu
from jax.sharding import PartitionSpec as P

DK = 128
BLOCK = 64
CTX_LIFT = 4
EPS = 1e-06
SHARP = 16.0
F32 = jnp.float32
BF16 = jnp.bfloat16
MESH = pl.DeviceIdType.MESH


def dot(a, b):
    return jnp.dot(a, b, preferred_element_type=F32)


def dot_nt(a, b):
    return lax.dot_general(a, b, (((1,), (1,)), ((), ())), preferred_element_type=F32)


def dot_tn(a, b):
    return lax.dot_general(a, b, (((0,), (0,)), ((), ())), preferred_element_type=F32)


def sums(mask, values):
    high = values.astype(BF16)
    low = (values - high.astype(F32)).astype(BF16)
    width = values.shape[1]
    both = dot(mask.astype(F32).astype(BF16), jnp.concatenate([high, low], axis=1))
    return both[:, :width] + both[:, width:]


def log_sigmoid(x):
    return jnp.minimum(x, 0.0) - jnp.log1p(jnp.exp(-jnp.abs(x)))


def chain_kernel(
    n_sp,
    n_tp,
    latents_in,
    sample_vector_in,
    context_in,
    context_vector_in,
    norm_gain_in,
    modulator,
    query_weight,
    key_weight,
    value_weight,
    decay_down_in,
    decay_up_in,
    decay_bias_in,
    decay_extra_in,
    head_gain_in,
    out_weight,
    out,
    latents,
    sample_vector,
    context,
    context_vector,
    norm_gain,
    decay_down,
    decay_up,
    decay_bias,
    decay_extra,
    head_gain,
    mod_w,
    mods,
    lat,
    outer_context,
    extras,
    hid,
    wk,
    wv,
    wq,
    wo,
    acc_k,
    acc_v,
    acc_q,
    tots,
    key_rows,
    query_rows,
    c_state,
    l_state,
    f_out,
    f_in,
    g_out,
    g_in,
    state,
    normed,
    part,
    rs,
    loc_sem,
    mt_s,
    mt_r,
    ms_s,
    ms_r,
    lat_s,
    lat_r,
    lo_s,
    lo_r,
    cx_s,
    cx_r,
    up_s,
    up_r,
    w_s,
    w_r,
    p_s,
    p_r,
    tt_s,
    tt_r,
    f_s,
    f_r,
    g_s,
    g_r,
    o_s,
    o_r,
    rs_s,
    rs_r,
):
    s = lax.axis_index("sp")
    t = lax.axis_index("tp")
    d = lax.axis_index("dp")
    h = lax.rem(d, 2)
    mate = d + 1 - 2 * h
    n_dev = n_sp * n_tp
    me = s * n_tp + t
    n_pairs = n_sp // 2
    pair = s // 2
    pos = lax.rem(s, 2)
    partner = s + 1 - 2 * pos
    is_worker = pos == 1 - s // n_pairs
    is_outer = pos == s // n_pairs
    rows, width = latents.shape
    ctx_rows = context.shape[0]
    length = rows * n_tp
    lat_all = 2 * length
    total = hid.shape[1]
    depth = hid.shape[2]
    half = depth // 2
    heads = decay_bias.shape[1] // DK
    dv = head_gain.shape[1]
    rank = decay_up.shape[1]
    span_t = width // n_tp

    def remote(src, dst, send, recv, device):
        return pltpu.make_async_remote_copy(
            src_ref=src,
            dst_ref=dst,
            send_sem=send,
            recv_sem=recv,
            device_id=device,
            device_id_type=MESH,
        )

    def worker_of(p):
        return 2 * p + 1 - p // (n_pairs // 2)

    def tp_peer(k):
        return lax.rem(t + k, n_tp)

    def tp_from(k):
        return lax.rem(t - k + n_tp, n_tp)

    def sp_peer(k):
        return lax.rem(s + k, n_sp)

    def sp_from(k):
        return lax.rem(s - k + n_sp, n_sp)

    weights = ((key_weight, wk), (value_weight, wv), (query_weight, wq))
    local = [pltpu.make_async_copy(modulator, mod_w, loc_sem.at[0])]
    for m, (source, slots) in enumerate(weights):
        for i in range(2):
            local.append(
                pltpu.make_async_copy(
                    source.at[pl.ds(i * half, half)], slots.at[s, i], loc_sem.at[1 + 2 * m + i]
                )
            )
    local.append(pltpu.make_async_copy(out_weight, wo, loc_sem.at[7]))
    barrier = pltpu.get_barrier_semaphore()
    for k in range(1, n_tp):
        pl.semaphore_signal(barrier, inc=1, device_id={"tp": tp_peer(k)}, device_id_type=MESH)
    for k in range(1, n_sp):
        pl.semaphore_signal(barrier, inc=1, device_id={"sp": sp_peer(k)}, device_id_type=MESH)
    pl.semaphore_signal(barrier, inc=1, device_id={"dp": mate}, device_id_type=MESH)
    small = [
        pltpu.make_async_copy(source, target, loc_sem.at[8 + i])
        for i, (source, target) in enumerate(
            (
                (sample_vector_in, sample_vector),
                (context_vector_in, context_vector),
                (latents_in, latents),
                (context_in, context),
                (decay_extra_in, decay_extra),
                (norm_gain_in, norm_gain),
                (decay_down_in, decay_down),
                (decay_up_in, decay_up),
                (decay_bias_in, decay_bias),
                (head_gain_in, head_gain),
            )
        )
    ]
    for copy in small[:5] + local[:1] + small[5:] + local[1:]:
        copy.start()
    small[2].wait()
    small[3].wait()
    small[4].wait()
    pl.semaphore_wait(barrier, n_tp + n_sp - 1)

    def inner():
        return jnp.logical_and(s >= 1, s <= n_sp - 2)

    def onward(r):
        return s + 1 <= n_sp - 2 if r == 0 else s - 1 >= 1

    def exists(r, j):
        return jnp.logical_and(inner(), s - j >= 0 if r == 0 else s + j < n_sp)

    def origin_of(r, j):
        return s - j if r == 0 else s + j

    def ring_copy(m, r, j, first=False):
        source, slots = weights[m]
        origin = origin_of(r, j)
        src = source.at[pl.ds(h * half, half)] if first else slots.at[origin, h]
        target = s + 1 if r == 0 else s - 1
        return remote(src, slots.at[origin, h], w_s.at[m, r, j], w_r.at[m, r, j], {"sp": target})

    def ring_arrival(m, r, j):
        view = weights[m][1].at[origin_of(r, j), h]
        return remote(view, view, w_s.at[m, r, j - 1], w_r.at[m, r, j - 1], {"sp": s})

    def mate_copy(m, r, j, side):
        view = weights[m][1].at[origin_of(r, j), side]
        return remote(view, view, p_s.at[m, r, j - 1], p_r.at[m, r, j - 1], {"dp": mate})

    def send_own(m):
        for r in range(2):

            @pl.when(onward(r))
            def _():
                ring_copy(m, r, 0, True).start()

    def relay(m, j, share):
        for r in range(2):

            @pl.when(exists(r, j))
            def _():
                ring_arrival(m, r, j).wait_recv()

                @pl.when(onward(r))
                def _():
                    ring_copy(m, r, j).start()

                if share:
                    mate_copy(m, r, j, h).start()

    def whole(slots, o):
        return slots[o].reshape(depth, slots.shape[3])

    def multiply(m, j, acc, count):
        slots = weights[m][1]
        for r in range(2):

            @pl.when(exists(r, j))
            def _():
                origin = origin_of(r, j)
                mate_copy(m, r, j, 1 - h).wait_recv()
                acc[...] += dot(hid[origin, 0:count], whole(slots, origin))

    def lat_copy(k):
        return remote(latents, lat.at[pos, t], lat_s.at[0, k], lat_r.at[0, k], {"tp": tp_peer(k)})

    def lat_arrival(k):
        view = lat.at[pos, tp_from(k)]
        return remote(view, view, lat_s.at[0, k], lat_r.at[0, k], {"tp": t})

    def outer_lat():
        return remote(latents, lat.at[pos, t], lo_s, lo_r, {"sp": partner})

    def outer_lat_arrival():
        view = lat.at[1 - pos, t]
        return remote(view, view, lo_s, lo_r, {"sp": s})

    def lat_relay(k, owner, to):
        view = lat.at[1 - pos, owner]
        return remote(view, view, lat_s.at[1, k], lat_r.at[1, k], {"tp": to})

    def ctx_cols(owner):
        return pl.ds(pl.multiple_of(owner * span_t, span_t), span_t)

    def ctx_copy():
        return remote(
            context.at[:, ctx_cols(t)],
            outer_context.at[:, ctx_cols(t)],
            cx_s.at[0],
            cx_r.at[0],
            {"sp": partner},
        )

    def ctx_relay(k, owner, to):
        view = outer_context.at[:, ctx_cols(owner)]
        return remote(view, view, cx_s.at[k], cx_r.at[k], {"tp": to})

    def extra_copy():
        return remote(decay_extra, extras.at[pos], up_s, up_r, {"sp": partner})

    def extra_arrival():
        view = extras.at[1 - pos]
        return remote(view, view, up_s, up_r, {"sp": s})

    @pl.when(is_outer)
    def _():
        outer_lat().start()
        extra_copy().start()
        ctx_copy().start()
        for m in range(3):
            send_own(m)

    @pl.when(is_worker)
    def _():
        for k in range(1, n_tp):
            lat_copy(k).start()
        send_own(0)
        send_own(1)

    small[0].wait()
    small[1].wait()
    is_first = lax.broadcasted_iota(jnp.int32, (16, width), 0) == 0
    vectors = jnp.where(is_first, sample_vector[...], context_vector[...])
    conditions = (vectors / (1.0 + jnp.exp(-vectors))).astype(BF16)
    local[0].wait()
    mods[me] = dot(conditions, mod_w[...])[0:2]

    def mod_tp(k, owner, to):
        view = mods.at[s * n_tp + owner]
        return remote(view, view, mt_s.at[k], mt_r.at[k], {"tp": to})

    def mod_sp(k, owner, to):
        view = mods.at[pl.ds(owner * n_tp, n_tp)]
        return remote(view, view, ms_s.at[k], ms_r.at[k], {"sp": to})

    for k in range(1, n_tp):
        mod_tp(k, t, tp_peer(k)).start()
    for k in range(1, n_tp):
        mod_tp(k, tp_from(k), t).wait_recv()
    for k in range(1, n_sp):
        mod_sp(k, s, sp_peer(k)).start()
    for copy in small[5:]:
        copy.wait()

    def modulation_now():
        for k in range(1, n_sp):
            mod_sp(k, sp_from(k), s).wait_recv()

    def mod_part(i):
        return jnp.concatenate([mods[j] for j in range(n_dev)], axis=1)[
            :, i * width : (i + 1) * width
        ]

    def tot_copy(k, owner, to):
        view = tots.at[owner]
        return remote(view, view, tt_s.at[k], tt_r.at[k], {"sp": to})

    def has_pred(z):
        return pair > 0 if z == 0 else pair < n_pairs - 1

    def has_succ(z):
        return pair < n_pairs - 1 if z == 0 else pair > 0

    def lone(a, b):
        return jnp.logical_and(a, jnp.logical_not(b))

    def f_copy(z, g):
        to = worker_of(pair + 1) if z == 0 else worker_of(pair - 1)
        return remote(f_out.at[z, g], f_in.at[z, g], f_s.at[z, g], f_r.at[z, g], {"sp": to})

    def g_copy(z, g):
        to = worker_of(pair - 1) if z == 0 else worker_of(pair + 1)
        return remote(g_out.at[z, g], g_in.at[z, g], g_s.at[z, g], g_r.at[z, g], {"sp": to})

    def o_copy(g, where, to):
        view = normed.at[where, g]
        return remote(view, view, o_s.at[g], o_r.at[g], {"sp": to})

    def work():
        outer_lat_arrival().wait_recv()
        for k in range(1, n_tp):
            lat_relay(k, t, tp_peer(k)).start()
        remote(
            outer_context.at[:, ctx_cols(t)],
            outer_context.at[:, ctx_cols(t)],
            cx_s.at[0],
            cx_r.at[0],
            {"sp": s},
        ).wait_recv()
        for k in range(1, n_tp):
            ctx_relay(k, t, tp_peer(k)).start()
        relay(0, 1, True)
        send_own(2)

        lat[pos, t] = latents[...]
        for k in range(1, n_tp):
            lat_arrival(k).wait_recv()
        modulation_now()
        shift = mod_part(0)
        scale = mod_part(1)

        def modulated(x, row):
            x = x.astype(F32)
            x = x * lax.rsqrt(jnp.mean(x * x, axis=-1, keepdims=True) + EPS) * norm_gain[...]
            return (x * (1.0 + scale[row : row + 1]) + shift[row : row + 1]).astype(BF16)

        piece = min(32, ctx_rows)

        def put(x, at):
            count = x.shape[0]
            at = pl.multiple_of(at, piece)
            for o in range(n_sp):
                hid[o, pl.ds(at, count)] = x[:, o * depth : (o + 1) * depth]

        for i in range(n_tp):
            put(modulated(lat[pos, i], 0), pos * length + i * rows)
        for i in range(ctx_rows // piece):
            put(
                modulated(context[i * piece : (i + 1) * piece], 1),
                lat_all + pos * ctx_rows + i * piece,
            )
        for k in range(1, n_tp):
            lat_relay(k, tp_from(k), t).wait_recv()
        relay(1, 1, True)
        for i in range(n_tp):
            put(modulated(lat[1 - pos, i], 0), (1 - pos) * length + i * rows)
        for k in range(1, n_tp):
            ctx_relay(k, tp_from(k), t).wait_recv()
        for i in range(ctx_rows // piece):
            put(
                modulated(outer_context[i * piece : (i + 1) * piece], 1),
                lat_all + (1 - pos) * ctx_rows + i * piece,
            )

        low = dot_nt(hid[0], decay_down[:, 0:depth])
        for o in range(1, n_sp):
            low = low + dot_nt(hid[o], decay_down[:, o * depth : (o + 1) * depth])
        low = low.astype(BF16)
        relay(2, 1, True)

        def log_decays(z):
            x = dot(low[:, z * rank : (z + 1) * rank], decay_up[z]) + decay_bias[z : z + 1]
            return log_sigmoid(x) / SHARP

        row_id = lax.broadcasted_iota(jnp.int32, (lat_all, lat_all), 0)
        col_id = lax.broadcasted_iota(jnp.int32, (lat_all, lat_all), 1)
        same = row_id // BLOCK == col_id // BLOCK
        within_mask = [same & (col_id <= row_id), same & (col_id >= row_id)]
        extras[pos] = decay_extra[...]
        extra_arrival().wait_recv()

        def extra_sums(z):
            columns = []
            for g in range(heads):
                line = jnp.concatenate([extras[i, z, g : g + 1, :] for i in range(2)], axis=1)
                columns.append(
                    jnp.sum(jnp.where(within_mask[z], line, 0.0), axis=1, keepdims=True)
                )
            return jnp.concatenate([jnp.broadcast_to(c, (lat_all, DK)) for c in columns], axis=1)

        decays = [log_decays(z) for z in range(2)]
        within = [sums(within_mask[z], decays[z][:lat_all]) + extra_sums(z) for z in range(2)]
        blocks = lat_all // BLOCK
        totals = [
            [within[0][(b + 1) * BLOCK - 1 : (b + 1) * BLOCK] for b in range(blocks)],
            [within[1][b * BLOCK : b * BLOCK + 1] for b in range(blocks)],
        ]
        none = jnp.zeros_like(totals[0][0])

        def between(z, lo, hi):
            value = none
            for b in range(lo, hi):
                value = value + totals[z][b]
            return value

        crow = lax.broadcasted_iota(jnp.int32, (total - lat_all, total - lat_all), 0)
        ccol = lax.broadcasted_iota(jnp.int32, (total - lat_all, total - lat_all), 1)
        after = [
            sums(ccol > crow, decays[0][lat_all:]),
            sums(ccol < crow, decays[1][lat_all:]),
        ]
        lat_total = [between(z, 0, blocks) for z in range(2)]
        ctx_total = [
            after[0][0:1] + decays[0][lat_all : lat_all + 1],
            after[1][total - lat_all - 1 :] + decays[1][total - 1 :],
        ]
        tots[pair] = jnp.concatenate(lat_total + ctx_total, axis=0)
        for k in range(1, n_pairs):
            to = lax.rem(pair + k, n_pairs)
            tot_copy(k, pair, worker_of(to)).start()

        for copy in local[1:5]:
            copy.wait()
        acc_k[...] = dot(hid[s], whole(wk, s))
        acc_v[...] = dot(hid[s], whole(wv, s))
        multiply(0, 1, acc_k, total)
        multiply(1, 1, acc_v, total)
        for k in range(1, n_pairs):
            tot_copy(k, lax.rem(pair - k + n_pairs, n_pairs), s).wait_recv()
        before = [none, none]
        suffix = [none, none]
        for u in range(n_pairs):
            line = tots[u]
            below = jnp.where(u < pair, 1.0, 0.0)
            above = jnp.where(u > pair, 1.0, 0.0)
            before[0] = before[0] + below * line[0:1]
            before[1] = before[1] + above * line[1:2]
            suffix[0] = suffix[0] + above * line[2:3]
            suffix[1] = suffix[1] + below * line[3:4]
        ctx_weight = [jnp.exp(after[z] + suffix[z]) for z in range(2)]

        def per_block(f):
            return jnp.concatenate([f(b) for b in range(blocks)], axis=0)

        def rows_of(x, b):
            return x[b * BLOCK : (b + 1) * BLOCK]

        ending = [
            jnp.exp(
                per_block(
                    lambda b: totals[0][b] - rows_of(within[0], b) + between(0, b + 1, blocks)
                )
            ),
            jnp.exp(per_block(lambda b: totals[1][b] - rows_of(within[1], b) + between(1, 0, b))),
        ]
        for j in range(2, max(n_sp - 1, 2)):
            relay(0, j, True)
            multiply(0, j, acc_k, total)
            relay(1, j, True)
            multiply(1, j, acc_v, total)
        keys = acc_k[...].astype(BF16)
        values = acc_v[...].astype(BF16)
        ckeys = keys[lat_all:].astype(F32)
        cvals = values[lat_all:]
        keys = keys[:lat_all].astype(F32)
        values = values[:lat_all]

        def columns(g, n):
            return slice(g * n, (g + 1) * n)

        for z in range(2):
            ended = (keys * ending[z]).astype(BF16)
            cended = (ckeys * ctx_weight[z]).astype(BF16)
            lift = CTX_LIFT * jnp.exp(before[z])
            lift_on = CTX_LIFT * jnp.exp(before[z] + lat_total[z])
            for g in range(heads):
                c = dot_tn(cvals[:, columns(g, dv)], cended[:, columns(g, DK)])
                g_out[z, g] = c.astype(BF16)
                own = dot_tn(values[:, columns(g, dv)], ended[:, columns(g, DK)])
                f_out[z, g] = (own + lift_on[:, columns(g, DK)] * c).astype(BF16)
                if n_pairs > 2:
                    c_state[z, g] = c
                    l_state[z, g] = own + lift_on[:, columns(g, DK)] * c
                state[z, g] = lift[:, columns(g, DK)] * c

                @pl.when(lone(has_succ(z), has_pred(z)))
                def _():
                    f_copy(z, g).start()

                @pl.when(lone(has_pred(z), has_succ(z)))
                def _():
                    g_copy(z, g).start()

        if n_pairs > 2:
            for z in range(2):

                @pl.when(jnp.logical_and(has_pred(z), has_succ(z)))
                def _():
                    for g in range(heads):
                        f_copy(z, g).wait_recv()
                        on = jnp.exp(lat_total[z])[:, columns(g, DK)]
                        f_out[z, g] = (l_state[z, g] + on * f_in[z, g].astype(F32)).astype(BF16)
                        f_copy(z, g).start()

                @pl.when(jnp.logical_and(has_pred(z), has_succ(z)))
                def _():
                    for g in range(heads):
                        g_copy(z, g).wait_recv()
                        g_out[z, g] = (c_state[z, g] + g_in[z, g].astype(F32)).astype(BF16)
                        g_copy(z, g).start()

        for z in range(2):
            close = (keys * jnp.exp(-within[z])).astype(BF16)
            near = keys * jnp.exp(per_block(lambda b: totals[z][b] - rows_of(within[z], b)))
            for i in range(blocks):
                for j in range(blocks):
                    if i == j:
                        block = rows_of(close, j)
                    elif (j < i) == (z == 0):
                        gap = between(z, min(i, j) + 1, max(i, j))
                        block = (rows_of(near, j) * jnp.exp(gap)).astype(BF16)
                    else:
                        block = jnp.zeros((BLOCK, heads * DK), BF16)
                    key_rows[z, i, j * BLOCK : (j + 1) * BLOCK] = block
        reach = [jnp.exp(within[z]) for z in range(2)]
        lifted_by = [
            jnp.exp(per_block(lambda b: rows_of(within[0], b) + between(0, 0, b))),
            jnp.exp(per_block(lambda b: rows_of(within[1], b) + between(1, b + 1, blocks))),
        ]

        for copy in local[5:7]:
            copy.wait()
        acc_q[...] = dot(hid[s, 0:lat_all], whole(wq, s))
        for j in range(1, max(n_sp - 1, 2)):
            if j > 1:
                relay(2, j, True)
            multiply(2, j, acc_q, lat_all)
        queries = acc_q[...].astype(BF16).astype(F32)

        for z in range(2):
            near_rows = (queries * reach[z]).astype(BF16)
            far_rows = (queries * lifted_by[z]).astype(BF16)
            for b in range(blocks):
                query_rows[0, z, b] = rows_of(near_rows, b)
                query_rows[1, z, b] = rows_of(far_rows, b)
        turn = blocks // 2
        row_in = lax.broadcasted_iota(jnp.int32, (BLOCK, lat_all), 0)
        col_in = lax.broadcasted_iota(jnp.int32, (BLOCK, lat_all), 1)

        def inside(where, g):
            lines = []
            for b in range(turn):
                i = where * turn + b
                ids = row_in + i * BLOCK
                masks = [col_in <= ids, col_in >= ids]
                line = 0.0
                for z in range(2):
                    score = dot_nt(
                        query_rows[0, z, i, :, columns(g, DK)], key_rows[z, i, :, columns(g, DK)]
                    )
                    line = line + jnp.where(masks[z], score, 0.0)
                lines.append(line.astype(BF16))
            return dot(jnp.concatenate(lines, axis=0), values[:, columns(g, dv)])

        def finish(where, g, mixed):
            for z in range(2):
                rows_z = query_rows[1, z, pl.ds(where * turn, turn), :, columns(g, DK)]
                mixed = mixed + dot_nt(rows_z.reshape(length, DK), state[z, g].astype(BF16))
            by = lax.rsqrt(jnp.mean(mixed * mixed, axis=-1, keepdims=True) + EPS)
            normed[where, g] = (mixed * by * head_gain[...]).astype(BF16)

        first = [inside(1 - pos, g) for g in range(heads)]
        for z in range(2):
            lift = CTX_LIFT * jnp.exp(before[z])

            @pl.when(has_pred(z))
            def _():
                for g in range(heads):
                    if n_pairs == 2:
                        f_copy(z, g).wait_recv()
                    else:

                        @pl.when(jnp.logical_not(has_succ(z)))
                        def _():
                            f_copy(z, g).wait_recv()

                    state[z, g] += f_in[z, g].astype(F32)

            @pl.when(has_succ(z))
            def _():
                for g in range(heads):
                    if n_pairs == 2:
                        g_copy(z, g).wait_recv()
                    else:

                        @pl.when(jnp.logical_not(has_pred(z)))
                        def _():
                            g_copy(z, g).wait_recv()

                    state[z, g] += lift[:, columns(g, DK)] * g_in[z, g].astype(F32)

        for g in range(heads):
            finish(1 - pos, g, first[g])
            o_copy(g, 1 - pos, partner).start()
        for g in range(heads):
            finish(pos, g, inside(pos, g))

    pl.when(is_worker)(work)

    @pl.when(is_outer)
    def _():
        for copy in local[1:7]:
            copy.wait()
        for m in range(3):
            relay(m, 1, False)
        for j in range(2, n_sp - 1):
            relay(0, j, False)
            relay(1, j, False)
        for j in range(2, n_sp - 1):
            relay(2, j, False)
        modulation_now()
        for g in range(heads):
            o_copy(g, pos, s).wait_recv()

    gate = mod_part(2)[0:1]
    local[7].wait()
    chunks = rs_s.shape[1]
    span = width // chunks
    rs_copies = []
    for c in range(chunks):
        cols = slice(c * span, (c + 1) * span)
        product = dot(normed[pos, 0], wo[0:dv, cols])
        for g in range(1, heads):
            product = product + dot(normed[pos, g], wo[g * dv : (g + 1) * dv, cols])
        product = product.astype(BF16)
        for i in range(n_tp):
            part[i, :, cols] = product[i * rows : (i + 1) * rows]
        for k in range(1, n_tp):
            to = tp_peer(k)
            copy = remote(
                part.at[to, :, pl.ds(c * span, span)],
                rs.at[k, :, pl.ds(c * span, span)],
                rs_s.at[k, c],
                rs_r.at[k, c],
                {"tp": to},
            )
            copy.start()
            rs_copies.append(copy)
    for c in range(chunks):
        cols = slice(c * span, (c + 1) * span)
        summed = part[t, :, cols].astype(F32)
        for k in range(1, n_tp):
            rs_copies[c * (n_tp - 1) + k - 1].wait_recv()
            summed = summed + rs[k, :, cols].astype(F32)
        projected = summed.astype(BF16).astype(F32)
        out[:, cols] = (latents[:, cols].astype(F32) + gate[:, cols] * projected).astype(BF16)

    for copy in rs_copies:
        copy.wait_send()
    for k in range(1, n_tp):
        mod_tp(k, t, tp_peer(k)).wait_send()
    for k in range(1, n_sp):
        mod_sp(k, s, sp_peer(k)).wait_send()

    @pl.when(is_outer)
    def _():
        outer_lat().wait_send()
        extra_copy().wait_send()
        ctx_copy().wait_send()

    @pl.when(is_worker)
    def _():
        for k in range(1, n_tp):
            lat_copy(k).wait_send()
            lat_relay(k, t, tp_peer(k)).wait_send()
            ctx_relay(k, t, tp_peer(k)).wait_send()
        for k in range(1, n_pairs):
            tot_copy(k, pair, s).wait_send()
        for g in range(heads):
            o_copy(g, 1 - pos, partner).wait_send()
            for z in range(2):

                @pl.when(has_succ(z))
                def _():
                    f_copy(z, g).wait_send()

                @pl.when(has_pred(z))
                def _():
                    g_copy(z, g).wait_send()

    for m in range(3):
        for r in range(2):

            @pl.when(onward(r))
            def _():
                ring_copy(m, r, 0, True).wait_send()

            for j in range(1, n_sp - 1):

                @pl.when(exists(r, j))
                def _():
                    @pl.when(onward(r))
                    def _():
                        ring_copy(m, r, j).wait_send()

                    @pl.when(is_worker)
                    def _():
                        mate_copy(m, r, j, h).wait_send()


def chain_per_device(n_sp, n_tp, *args):
    (latents, sv, context, cv, gain, modulator, wq, wk, wv, down, up, bias, extra, hg, wo) = args
    rows, width = latents.shape
    ctx_rows = context.shape[0]
    n_dev = n_sp * n_tp
    n_pairs = n_sp // 2
    length = rows * n_tp
    total = 2 * (length + ctx_rows)
    depth = wq.shape[0]
    kw, vw = wk.shape[1], wv.shape[1]
    heads = bias.shape[1] // DK
    dv = hg.shape[0]
    chunks = 4
    vmem = pl.BlockSpec(memory_space=pltpu.VMEM)
    hbm = pl.BlockSpec(memory_space=pl.ANY)
    dma = pltpu.SemaphoreType.DMA
    states = (2, heads, dv, DK)
    chained = states if n_pairs > 2 else (2, heads, 8, DK)
    scratch = [
        pltpu.VMEM(latents.shape, BF16),
        pltpu.VMEM(sv.shape, F32),
        pltpu.VMEM(context.shape, BF16),
        pltpu.VMEM(cv.shape, F32),
        pltpu.VMEM((1, width), F32),
        pltpu.VMEM(down.shape[::-1], BF16),
        pltpu.VMEM(up.shape, BF16),
        pltpu.VMEM(bias.shape, F32),
        pltpu.VMEM((2, heads, length), F32),
        pltpu.VMEM((1, dv), F32),
        pltpu.VMEM(modulator.shape, BF16),
        pltpu.VMEM((n_dev, 2, modulator.shape[1]), F32),
        pltpu.VMEM((2, n_tp, rows, width), BF16),
        pltpu.VMEM((ctx_rows, width), BF16),
        pltpu.VMEM((2, 2, heads, length), F32),
        pltpu.VMEM((n_sp, total, depth), BF16),
        pltpu.VMEM((n_sp, 2, depth // 2, kw), BF16),
        pltpu.VMEM((n_sp, 2, depth // 2, vw), BF16),
        pltpu.VMEM((n_sp, 2, depth // 2, kw), BF16),
        pltpu.VMEM(wo.shape, BF16),
        pltpu.VMEM((total, kw), F32),
        pltpu.VMEM((total, vw), F32),
        pltpu.VMEM((2 * length, kw), F32),
        pltpu.VMEM((n_pairs, 4, kw), F32),
        pltpu.VMEM((2, 2 * length // BLOCK, 2 * length, kw), BF16),
        pltpu.VMEM((2, 2, 2 * length // BLOCK, BLOCK, kw), BF16),
        pltpu.VMEM(chained, F32),
        pltpu.VMEM(chained, F32),
        pltpu.VMEM(states, BF16),
        pltpu.VMEM(states, BF16),
        pltpu.VMEM(states, BF16),
        pltpu.VMEM(states, BF16),
        pltpu.VMEM(states, F32),
        pltpu.VMEM((2, heads, length, dv), BF16),
        pltpu.VMEM((n_tp, rows, width), BF16),
        pltpu.VMEM((n_tp, rows, width), BF16),
        dma((18,)),
        dma((n_tp,)),
        dma((n_tp,)),
        dma((n_sp,)),
        dma((n_sp,)),
        dma((2, n_tp)),
        dma((2, n_tp)),
        dma,
        dma,
        dma((n_tp,)),
        dma((n_tp,)),
        dma,
        dma,
        dma((3, 2, n_sp)),
        dma((3, 2, n_sp)),
        dma((3, 2, n_sp)),
        dma((3, 2, n_sp)),
        dma((n_pairs,)),
        dma((n_pairs,)),
        dma((2, heads)),
        dma((2, heads)),
        dma((2, heads)),
        dma((2, heads)),
        dma((heads,)),
        dma((heads,)),
        dma((n_tp, chunks)),
        dma((n_tp, chunks)),
    ]
    return pl.pallas_call(
        functools.partial(chain_kernel, n_sp, n_tp),
        out_shape=jax.ShapeDtypeStruct(latents.shape, BF16),
        in_specs=[hbm] * 15,
        out_specs=vmem,
        scratch_shapes=scratch,
        compiler_params=pltpu.CompilerParams(
            collective_id=0, has_side_effects=True, vmem_limit_bytes=56 * 1024 * 1024
        ),
    )(
        latents,
        sv,
        context,
        cv,
        gain.reshape(1, -1),
        modulator,
        wq,
        wk,
        wv,
        down.T,
        up,
        bias,
        extra.transpose(0, 2, 1),
        hg.reshape(1, -1),
        wo,
    )


def kernel(
    n_sp,
    n_tp,
    latents_in,
    sample_vector_in,
    context_in,
    context_vector_in,
    norm_gain_in,
    modulator,
    query_weight,
    key_weight,
    value_weight,
    decay_down_in,
    decay_up_in,
    decay_bias_in,
    decay_extra_in,
    head_gain_in,
    out_weight,
    out,
    latents,
    sample_vector,
    context,
    context_vector,
    norm_gain,
    decay_down,
    decay_up,
    decay_bias,
    decay_extra,
    head_gain,
    mod_w,
    mods,
    lat,
    ctx,
    extras,
    hid,
    wk,
    wv,
    wq,
    wo,
    acc_k,
    acc_v,
    acc_q,
    key_rows,
    o_out,
    normed,
    part,
    rs,
    loc_sem,
    mt_s,
    mt_r,
    ms_s,
    ms_r,
    lo_s,
    lo_r,
    cx_s,
    cx_r,
    ex_s,
    ex_r,
    em_s,
    em_r,
    lp_s,
    lp_r,
    cp_s,
    cp_r,
    hd_s,
    hd_r,
    w_s,
    w_r,
    o_s,
    o_r,
    rs_s,
    rs_r,
    vouch,
):
    s = lax.axis_index("sp")
    t = lax.axis_index("tp")
    d = lax.axis_index("dp")
    h = lax.rem(d, 2)
    mate = d + 1 - 2 * h
    n_dev = n_sp * n_tp
    me = s * n_tp + t
    first_plane = n_sp // 2 - 1
    last_plane = n_sp // 2
    side = s - first_plane
    target = first_plane + h
    is_worker = jnp.logical_and(s >= first_plane, s <= last_plane)
    is_leader = s == target
    is_follower = jnp.logical_and(is_worker, s != target)
    is_sender = s != target
    rows, width = latents.shape
    ctx_rows = context.shape[0]
    length = rows * n_tp
    lat_all = n_sp * length
    total = hid.shape[1]
    depth = hid.shape[2]
    heads = decay_bias.shape[1] // DK
    dv = head_gain.shape[1]
    rank = decay_up.shape[1]
    span_t = width // n_tp

    def remote(src, dst, send, recv, device):
        return pltpu.make_async_remote_copy(
            src_ref=src,
            dst_ref=dst,
            send_sem=send,
            recv_sem=recv,
            device_id=device,
            device_id_type=MESH,
        )

    def tp_peer(k):
        return lax.rem(t + k, n_tp)

    def tp_from(k):
        return lax.rem(t - k + n_tp, n_tp)

    def sp_peer(k):
        return lax.rem(s + k, n_sp)

    def sp_from(k):
        return lax.rem(s - k + n_sp, n_sp)

    def head_cols(size):
        return pl.ds(pl.multiple_of(h * size, DK), size)

    weights = ((key_weight, wk, DK), (value_weight, wv, dv), (query_weight, wq, DK))
    own_weight = [
        pltpu.make_async_copy(source.at[:, head_cols(size)], slots.at[s], loc_sem.at[1 + m])
        for m, (source, slots, size) in enumerate(weights)
    ]
    mod_load = pltpu.make_async_copy(modulator, mod_w, loc_sem.at[0])
    out_load = pltpu.make_async_copy(out_weight, wo, loc_sem.at[4])
    barrier = pltpu.get_barrier_semaphore()

    def signal(semaphore, device):
        pl.semaphore_signal(semaphore, inc=1, device_id=device, device_id_type=MESH)

    above = s + 1 < n_sp
    below = s > 0
    twist = t + 1 - 2 * lax.rem(t, 2)
    cross = lax.rem(t + 2, n_tp)
    signal(barrier, {"tp": twist})
    signal(barrier, {"tp": cross})
    signal(barrier, {"dp": mate})

    @pl.when(above)
    def _():
        signal(barrier, {"sp": s + 1})

    @pl.when(below)
    def _():
        signal(barrier, {"sp": s - 1})

    small = [
        pltpu.make_async_copy(source, where, loc_sem.at[8 + i])
        for i, (source, where) in enumerate(
            (
                (sample_vector_in, sample_vector),
                (context_vector_in, context_vector),
                (latents_in, latents),
                (context_in, context),
                (decay_extra_in, decay_extra),
                (norm_gain_in, norm_gain),
                (decay_down_in, decay_down),
                (decay_up_in, decay_up),
                (decay_bias_in, decay_bias),
                (head_gain_in, head_gain),
            )
        )
    ]
    for copy in small[:5] + own_weight + [mod_load] + small[5:] + [out_load]:
        copy.start()
    for copy in small[2:5] + own_weight:
        copy.wait()
    pl.semaphore_wait(barrier, 3 + jnp.where(above, 1, 0) + jnp.where(below, 1, 0))
    signal(vouch.at[n_sp], {"tp": twist})

    def pass_word(step):
        @pl.when(jnp.logical_and(below, s + step < n_sp))
        def _():
            signal(vouch.at[step], {"sp": s - 1})

        @pl.when(jnp.logical_and(above, s - step >= 0))
        def _():
            signal(vouch.at[0 if step == 1 else n_sp - 1], {"sp": s + 1})

    def hear_word(step):
        @pl.when(s + step + 1 < n_sp)
        def _():
            pl.semaphore_wait(vouch.at[step], 1)

        @pl.when(s - step - 1 >= 0)
        def _():
            pl.semaphore_wait(vouch.at[0 if step == 1 else n_sp - 1], 1)

    pass_word(1)

    def onward(r):
        return s + 1 <= last_plane if r == 0 else s - 1 >= first_plane

    def exists(r, j):
        if r == 0:
            return jnp.logical_and(s <= last_plane, s - j >= 0)
        return jnp.logical_and(s >= first_plane, s + j < n_sp)

    def origin_of(r, j):
        return s - j if r == 0 else s + j

    def ring_copy(m, r, j):
        view = weights[m][1].at[origin_of(r, j)]
        to = s + 1 if r == 0 else s - 1
        return remote(view, view, w_s.at[m, r, j], w_r.at[m, r, j], {"sp": to})

    def ring_arrival(m, r, j):
        view = weights[m][1].at[origin_of(r, j)]
        return remote(view, view, w_s.at[m, r, j - 1], w_r.at[m, r, j - 1], {"sp": s})

    def relay(m, j):
        for r in range(2):

            @pl.when(exists(r, j))
            def _():
                ring_arrival(m, r, j).wait_recv()

                @pl.when(onward(r))
                def _():
                    ring_copy(m, r, j).start()

    def multiply(m, j, acc, count):
        slots = weights[m][1]
        for r in range(2):

            @pl.when(exists(r, j))
            def _():
                origin = origin_of(r, j)
                acc[...] += dot(hid[origin, 0:count], slots[origin])

    def lat_in(b, to):
        view = lat.at[b, t]
        return remote(latents, view, lo_s, lo_r.at[b], {"sp": to})

    def extra_in(b, to):
        return remote(decay_extra, extras.at[b], ex_s, ex_r.at[b], {"sp": to})

    def ctx_cols(owner):
        return pl.ds(pl.multiple_of(owner * span_t, span_t), span_t)

    def ctx_in(b, to):
        return remote(
            context.at[:, ctx_cols(t)],
            ctx.at[b, :, ctx_cols(t)],
            cx_s,
            cx_r.at[b],
            {"sp": to},
        )

    def lat_plane(b, k, owner, to):
        view = lat.at[b, owner]
        return remote(view, view, lp_s.at[b, k], lp_r.at[b, k], {"tp": to})

    def lat_own(k):
        return remote(latents, lat.at[s, t], lp_s.at[s, k], lp_r.at[s, k], {"tp": tp_peer(k)})

    def ctx_plane(b, k, owner, to):
        view = ctx.at[b, :, ctx_cols(owner)]
        return remote(view, view, cp_s.at[b, k], cp_r.at[b, k], {"tp": to})

    def hid_copy(i, at, count):
        view = hid.at[:, pl.ds(pl.multiple_of(at, 16), count)]
        return remote(view, view, hd_s.at[i], hd_r.at[i], {"dp": mate})

    def lat_hid(b):
        return hid_copy(b, b * length, length)

    def ctx_hid(b):
        return hid_copy(n_sp + b, lat_all + b * ctx_rows, ctx_rows)

    def extra_mate():
        return remote(extras, extras, em_s, em_r, {"dp": mate})

    def others():
        towards = 1 - 2 * side
        steps = sorted(range(-first_plane, n_sp // 2 + 1), key=abs)
        return [s + towards * step for step in steps if step]

    adjacent = jnp.logical_or(s == target + 1, s == target - 1)

    def send_rows():
        lat_in(s, target).start()
        extra_in(s, target).start()
        ctx_in(s, target).start()

    def send_weight(m):
        for r in range(2):

            @pl.when(onward(r))
            def _():
                ring_copy(m, r, 0).start()

    pl.when(adjacent)(send_rows)

    @pl.when(is_leader)
    def _():
        for k in (1, 2, 3):

            @pl.when(tp_peer(k) != lax.rem(twist + 2, n_tp))
            def _():
                lat_own(k).start()

    send_weight(0)
    hear_word(1)
    pass_word(2)
    pl.semaphore_wait(vouch.at[n_sp], 1)
    pl.when(jnp.logical_and(is_sender, jnp.logical_not(adjacent)))(send_rows)

    @pl.when(is_leader)
    def _():
        for k in (1, 2, 3):

            @pl.when(tp_peer(k) == lax.rem(twist + 2, n_tp))
            def _():
                lat_own(k).start()

    send_weight(1)
    send_weight(2)

    small[0].wait()
    small[1].wait()
    is_first = lax.broadcasted_iota(jnp.int32, (16, width), 0) == 0
    vectors = jnp.where(is_first, sample_vector[...], context_vector[...])
    conditions = (vectors / (1.0 + jnp.exp(-vectors))).astype(BF16)
    mod_load.wait()
    mods[me] = dot(conditions, mod_w[...])[0:2]

    def mod_tp(k, owner, to):
        view = mods.at[s * n_tp + owner]
        return remote(view, view, mt_s.at[k], mt_r.at[k], {"tp": to})

    def mod_sp(k, owner, to):
        view = mods.at[pl.ds(owner * n_tp, n_tp)]
        return remote(view, view, ms_s.at[k], ms_r.at[k], {"sp": to})

    for k in range(1, n_tp):
        mod_tp(k, t, tp_peer(k)).start()
    for k in range(1, n_tp):
        mod_tp(k, tp_from(k), t).wait_recv()
    hear_word(2)
    for k in range(1, n_sp):
        mod_sp(k, s, sp_peer(k)).start()
    for copy in small[5:]:
        copy.wait()

    def mod_part(i):
        return jnp.concatenate([mods[j] for j in range(n_dev)], axis=1)[
            :, i * width : (i + 1) * width
        ]

    def mods_arrive():
        for k in range(1, n_sp):
            mod_sp(k, sp_from(k), s).wait_recv()

    piece = min(32, ctx_rows)

    def put(x, row, at):
        count = x.shape[0]
        x = x.astype(F32)
        x = x * lax.rsqrt(jnp.mean(x * x, axis=-1, keepdims=True) + EPS) * norm_gain[...]
        scale = mod_part(1)[row : row + 1]
        shift = mod_part(0)[row : row + 1]
        x = (x * (1.0 + scale) + shift).astype(BF16)
        at = pl.multiple_of(at, piece)
        for o in range(n_sp):
            hid[o, pl.ds(at, count)] = x[:, o * depth : (o + 1) * depth]

    def o_copy(b):
        lead = jnp.where(side == h, d, mate)
        return remote(
            o_out.at[b], normed.at[h], o_s.at[b], o_r.at[h], {"sp": b, "dp": lead}
        )

    def o_mate():
        return remote(o_out.at[s], normed.at[h], o_s.at[s], o_r.at[h], {"dp": mate})

    def o_arrival(c):
        return remote(normed.at[c], normed.at[c], o_s.at[s], o_r.at[c], {"dp": mate})

    def work():
        blocks = lat_all // BLOCK
        per = length // BLOCK

        @pl.when(is_leader)
        def _():
            for b in others():
                remote(lat.at[b, t], lat.at[b, t], lo_s, lo_r.at[b], {"sp": s}).wait_recv()
                for k in range(1, n_tp):
                    lat_plane(b, k, t, tp_peer(k)).start()
            for b in others():
                view = ctx.at[b, :, ctx_cols(t)]
                remote(view, view, cx_s, cx_r.at[b], {"sp": s}).wait_recv()
                for k in range(1, n_tp):
                    ctx_plane(b, k, t, tp_peer(k)).start()
            lat[s, t] = latents[...]
            mods_arrive()
            for i, b in enumerate([s] + others()):
                for k in range(1, n_tp):
                    lat_plane(b, k, tp_from(k), t).wait_recv()
                for u in range(n_tp):
                    put(lat[b, u], 0, b * length + u * rows)
                lat_hid(b).start()
                if i == 0:
                    relay(0, 1)
                    extras[s] = decay_extra[...]
                    for c in others():
                        remote(
                            extras.at[c], extras.at[c], ex_s, ex_r.at[c], {"sp": s}
                        ).wait_recv()
                    extra_mate().start()
                if i == 2:
                    relay(1, 1)

        @pl.when(is_follower)
        def _():
            relay(0, 1)
            relay(1, 1)
            mods_arrive()
            extra_mate().wait_recv()
            for b in range(n_sp):
                lat_hid(b).wait_recv()

        def lows(lo, hi):
            value = dot_nt(hid[0, lo:hi], decay_down[:, 0:depth])
            for o in range(1, n_sp):
                value = value + dot_nt(
                    hid[o, lo:hi], decay_down[:, o * depth : (o + 1) * depth]
                )
            return value.astype(BF16)

        def log_decays(low, z):
            x = dot(low[:, z * rank : (z + 1) * rank], decay_up[z, :, head_cols(DK)])
            return log_sigmoid(x + decay_bias[z : z + 1, head_cols(DK)]) / SHARP

        low = lows(0, lat_all)
        relay(2, 1)
        decays = [log_decays(low, z) for z in range(2)]
        group = 2 * length
        row_id = lax.broadcasted_iota(jnp.int32, (group, group), 0)
        col_id = lax.broadcasted_iota(jnp.int32, (group, group), 1)
        same = row_id // BLOCK == col_id // BLOCK
        inner = [same & (col_id <= row_id), same & (col_id >= row_id)]

        def within_of(z):
            pieces = []
            for i in range(lat_all // group):
                line = jnp.concatenate(
                    [extras[2 * i + e, z, pl.ds(h, 1), :] for e in range(2)], axis=1
                )
                extra = jnp.sum(jnp.where(inner[z], line, 0.0), axis=1, keepdims=True)
                pieces.append(sums(inner[z], decays[z][i * group : (i + 1) * group]) + extra)
            return jnp.concatenate(pieces, axis=0)

        within = [within_of(z) for z in range(2)]
        totals = [
            [within[0][(b + 1) * BLOCK - 1 : (b + 1) * BLOCK] for b in range(blocks)],
            [within[1][b * BLOCK : b * BLOCK + 1] for b in range(blocks)],
        ]
        none = jnp.zeros_like(totals[0][0])

        def between(z, lo, hi):
            value = none
            for b in range(lo, hi):
                value = value + totals[z][b]
            return value

        def per_block(f):
            return jnp.concatenate([f(b) for b in range(blocks)], axis=0)

        def rows_of(x, b):
            return x[b * BLOCK : (b + 1) * BLOCK]

        def key_span(z, i):
            if z == 0:
                return 0, min(-(-(i + 1) * BLOCK // DK) * DK, lat_all)
            return i * BLOCK // DK * DK, lat_all

        reach = [jnp.exp(within[z]) for z in range(2)]
        lifted_by = [
            jnp.exp(per_block(lambda b: rows_of(within[0], b) + between(0, 0, b))),
            jnp.exp(per_block(lambda b: rows_of(within[1], b) + between(1, b + 1, blocks))),
        ]

        @pl.when(is_leader)
        def _():
            for i in range(ctx_rows // piece):
                put(
                    context[i * piece : (i + 1) * piece],
                    1,
                    lat_all + s * ctx_rows + i * piece,
                )
            ctx_hid(s).start()
            for b in others():
                for k in range(1, n_tp):
                    ctx_plane(b, k, tp_from(k), t).wait_recv()
                for i in range(ctx_rows // piece):
                    put(
                        ctx[b, i * piece : (i + 1) * piece],
                        1,
                        lat_all + b * ctx_rows + i * piece,
                    )
                ctx_hid(b).start()

        @pl.when(is_follower)
        def _():
            for b in range(n_sp):
                ctx_hid(b).wait_recv()

        low_ctx = lows(lat_all, total)
        ctx_decays = [log_decays(low_ctx, z) for z in range(2)]
        ctx_all = total - lat_all
        crow = lax.broadcasted_iota(jnp.int32, (ctx_all, ctx_all), 0)
        ccol = lax.broadcasted_iota(jnp.int32, (ctx_all, ctx_all), 1)
        ctx_weight = [
            jnp.exp(sums(ccol > crow, ctx_decays[0])),
            jnp.exp(sums(ccol < crow, ctx_decays[1])),
        ]

        acc_k[...] = dot(hid[s], wk[s])
        acc_v[...] = dot(hid[s], wv[s])
        acc_q[...] = dot(hid[s, 0:lat_all], wq[s])
        multiply(0, 1, acc_k, total)
        multiply(1, 1, acc_v, total)
        multiply(2, 1, acc_q, lat_all)
        far = range(2, n_sp // 2 + 1)
        for j in far:
            relay(0, j)
            multiply(0, j, acc_k, total)
        keys = acc_k[...].astype(BF16).astype(F32)
        ckeys = keys[lat_all:]
        keys = keys[:lat_all]
        for z in range(2):
            close = (keys * jnp.exp(-within[z])).astype(BF16)
            near = keys * jnp.exp(per_block(lambda b: totals[z][b] - rows_of(within[z], b)))
            for i in range(blocks):
                lo, hi = key_span(z, i)
                for j in range(lo // BLOCK, hi // BLOCK):
                    if (j > i) if z == 0 else (j < i):
                        block = jnp.zeros((BLOCK, DK), BF16)
                    elif i == j:
                        block = rows_of(close, j)
                    else:
                        gap = between(z, min(i, j) + 1, max(i, j))
                        block = (rows_of(near, j) * jnp.exp(gap)).astype(BF16)
                    key_rows[z, i, j * BLOCK : (j + 1) * BLOCK] = block
        for j in far:
            relay(1, j)
            multiply(1, j, acc_v, total)
        values = acc_v[...].astype(BF16)
        cvals = values[lat_all:]
        values = values[:lat_all]
        state = [
            (CTX_LIFT * dot_tn(cvals, (ckeys * ctx_weight[z]).astype(BF16))).astype(BF16)
            for z in range(2)
        ]
        for j in far:
            relay(2, j)
            multiply(2, j, acc_q, lat_all)
        tri_row = lax.broadcasted_iota(jnp.int32, (BLOCK, lat_all), 0)
        tri_col = lax.broadcasted_iota(jnp.int32, (BLOCK, lat_all), 1)

        def attend(b):
            lines = []
            part_of = slice(b * length, (b + 1) * length)
            queries = acc_q[part_of].astype(BF16).astype(F32)
            query_dec = [(queries * reach[z][part_of]).astype(BF16) for z in range(2)]
            lifted = [(queries * lifted_by[z][part_of]).astype(BF16) for z in range(2)]
            for i in range(b * per, (b + 1) * per):
                full = []
                for z in range(2):
                    lo, hi = key_span(z, i)
                    score = dot_nt(rows_of(query_dec[z], i - b * per), key_rows[z, i, lo:hi])
                    ids = tri_row[:, lo:hi] + i * BLOCK
                    cols = tri_col[:, lo:hi]
                    keep = cols <= ids if z == 0 else cols >= ids
                    score = jnp.where(keep, score, 0.0)
                    pads = [jnp.zeros((BLOCK, lo), F32), score, jnp.zeros((BLOCK, lat_all - hi), F32)]
                    full.append(jnp.concatenate([p for p in pads if p.shape[1]], axis=1))
                lines.append((full[0] + full[1]).astype(BF16))
            mixed = dot(jnp.concatenate(lines, axis=0), values)
            for z in range(2):
                mixed = mixed + dot_nt(lifted[z], state[z])
            by = lax.rsqrt(jnp.mean(mixed * mixed, axis=-1, keepdims=True) + EPS)
            return (mixed * by * head_gain[...]).astype(BF16)

        for w in range(2):

            @pl.when(side == w)
            def _():
                here = first_plane + w
                order = sorted(range(n_sp), key=lambda b: -abs(b - here))
                for b in order:
                    if b != here:
                        o_out[b] = attend(b)
                        o_copy(b).start()
                        continue
                    result = attend(b)

                    @pl.when(is_leader)
                    def _():
                        normed[h] = result

                    @pl.when(is_follower)
                    def _():
                        o_out[b] = result
                        o_mate().start()

    pl.when(is_worker)(work)

    @pl.when(jnp.logical_not(is_worker))
    def _():
        mods_arrive()

    @pl.when(is_leader)
    def _():
        o_arrival(1 - h).wait_recv()

    @pl.when(is_sender)
    def _():
        for c in range(heads):
            o_arrival(c).wait_recv()

    gate = mod_part(2)[0:1]
    out_load.wait()
    chunks = rs_s.shape[1]
    span = width // chunks
    rs_copies = []
    for c in range(chunks):
        cols = slice(c * span, (c + 1) * span)
        product = dot(normed[0], wo[0:dv, cols])
        for g in range(1, heads):
            product = product + dot(normed[g], wo[g * dv : (g + 1) * dv, cols])
        product = product.astype(BF16)
        for i in range(n_tp):
            part[i, :, cols] = product[i * rows : (i + 1) * rows]
        for k in range(1, n_tp):
            to = tp_peer(k)
            copy = remote(
                part.at[to, :, pl.ds(c * span, span)],
                rs.at[k, :, pl.ds(c * span, span)],
                rs_s.at[k, c],
                rs_r.at[k, c],
                {"tp": to},
            )
            copy.start()
            rs_copies.append(copy)
    for c in range(chunks):
        cols = slice(c * span, (c + 1) * span)
        summed = part[t, :, cols].astype(F32)
        for k in range(1, n_tp):
            rs_copies[c * (n_tp - 1) + k - 1].wait_recv()
            summed = summed + rs[k, :, cols].astype(F32)
        projected = summed.astype(BF16).astype(F32)
        out[:, cols] = (latents[:, cols].astype(F32) + gate[:, cols] * projected).astype(BF16)

    for copy in rs_copies:
        copy.wait_send()
    for k in range(1, n_tp):
        mod_tp(k, t, tp_peer(k)).wait_send()
    for k in range(1, n_sp):
        mod_sp(k, s, sp_peer(k)).wait_send()

    @pl.when(is_sender)
    def _():
        lat_in(s, target).wait_send()
        extra_in(s, target).wait_send()
        ctx_in(s, target).wait_send()

    @pl.when(is_leader)
    def _():
        extra_mate().wait_send()
        for k in range(1, n_tp):
            lat_own(k).wait_send()
            for b in others():
                lat_plane(b, k, t, tp_peer(k)).wait_send()
                ctx_plane(b, k, t, tp_peer(k)).wait_send()
        for b in range(n_sp):
            lat_hid(b).wait_send()
            ctx_hid(b).wait_send()

    @pl.when(is_follower)
    def _():
        o_mate().wait_send()

    @pl.when(is_worker)
    def _():
        for b in others():
            o_copy(b).wait_send()

    for m in range(3):
        for r in range(2):

            @pl.when(onward(r))
            def _():
                ring_copy(m, r, 0).wait_send()

            for j in range(1, n_sp // 2 + 1):

                @pl.when(jnp.logical_and(exists(r, j), onward(r)))
                def _():
                    ring_copy(m, r, j).wait_send()


def per_device(n_sp, n_tp, *args):
    (latents, sv, context, cv, gain, modulator, wq, wk, wv, down, up, bias, extra, hg, wo) = args
    heads = bias.shape[1] // DK
    if n_sp != 4 or n_tp != 4 or heads != 2:
        return chain_per_device(n_sp, n_tp, *args)
    rows, width = latents.shape
    ctx_rows = context.shape[0]
    n_dev = n_sp * n_tp
    length = rows * n_tp
    lat_all = n_sp * length
    total = n_sp * (length + ctx_rows)
    depth = wq.shape[0]
    dv = hg.shape[0]
    chunks = 4
    vmem = pl.BlockSpec(memory_space=pltpu.VMEM)
    hbm = pl.BlockSpec(memory_space=pl.ANY)
    dma = pltpu.SemaphoreType.DMA
    scratch = [
        pltpu.VMEM(latents.shape, BF16),
        pltpu.VMEM(sv.shape, F32),
        pltpu.VMEM(context.shape, BF16),
        pltpu.VMEM(cv.shape, F32),
        pltpu.VMEM((1, width), F32),
        pltpu.VMEM(down.shape[::-1], BF16),
        pltpu.VMEM(up.shape, BF16),
        pltpu.VMEM(bias.shape, F32),
        pltpu.VMEM((2, heads, length), F32),
        pltpu.VMEM((1, dv), F32),
        pltpu.VMEM(modulator.shape, BF16),
        pltpu.VMEM((n_dev, 2, modulator.shape[1]), F32),
        pltpu.VMEM((n_sp, n_tp, rows, width), BF16),
        pltpu.VMEM((n_sp, ctx_rows, width), BF16),
        pltpu.VMEM((n_sp, 2, heads, length), F32),
        pltpu.VMEM((n_sp, total, depth), BF16),
        pltpu.VMEM((n_sp, depth, DK), BF16),
        pltpu.VMEM((n_sp, depth, dv), BF16),
        pltpu.VMEM((n_sp, depth, DK), BF16),
        pltpu.VMEM(wo.shape, BF16),
        pltpu.VMEM((total, DK), F32),
        pltpu.VMEM((total, dv), F32),
        pltpu.VMEM((lat_all, DK), F32),
        pltpu.VMEM((2, lat_all // BLOCK, lat_all, DK), BF16),
        pltpu.VMEM((n_sp, length, dv), BF16),
        pltpu.VMEM((heads, length, dv), BF16),
        pltpu.VMEM((n_tp, rows, width), BF16),
        pltpu.VMEM((n_tp, rows, width), BF16),
        dma((18,)),
        dma((n_tp,)),
        dma((n_tp,)),
        dma((n_sp,)),
        dma((n_sp,)),
        dma,
        dma((n_sp,)),
        dma,
        dma((n_sp,)),
        dma,
        dma((n_sp,)),
        dma,
        dma,
        dma((n_sp, n_tp)),
        dma((n_sp, n_tp)),
        dma((n_sp, n_tp)),
        dma((n_sp, n_tp)),
        dma((2 * n_sp,)),
        dma((2 * n_sp,)),
        dma((3, 2, n_sp)),
        dma((3, 2, n_sp)),
        dma((n_sp,)),
        dma((heads,)),
        dma((n_tp, chunks)),
        dma((n_tp, chunks)),
        pltpu.SemaphoreType.REGULAR((n_sp + n_tp,)),
    ]
    return pl.pallas_call(
        functools.partial(kernel, n_sp, n_tp),
        out_shape=jax.ShapeDtypeStruct(latents.shape, BF16),
        in_specs=[hbm] * 15,
        out_specs=vmem,
        scratch_shapes=scratch,
        compiler_params=pltpu.CompilerParams(
            collective_id=0, has_side_effects=True, vmem_limit_bytes=56 * 1024 * 1024
        ),
    )(
        latents,
        sv,
        context,
        cv,
        gain.reshape(1, -1),
        modulator,
        wq,
        wk,
        wv,
        down.T,
        up,
        bias,
        extra.transpose(0, 2, 1),
        hg.reshape(1, -1),
        wo,
    )


def solution(mesh):
    placed = (
        P(("dp", "sp", "tp"), None),
        P("dp", None),
        P(("dp", "sp"), None),
        P(),
        P(),
        P(None, ("sp", "tp")),
        P("sp", "tp"),
        P("sp", "tp"),
        P("sp", "tp"),
        P(),
        P(None, None, "tp"),
        P(None, "tp"),
        P(None, ("dp", "sp"), "tp"),
        P(),
        P("tp", None),
    )
    return jax.shard_map(
        functools.partial(per_device, mesh.shape["sp"], mesh.shape["tp"]),
        mesh=mesh,
        in_specs=placed,
        out_specs=P(("dp", "sp", "tp"), None),
        check_vma=False,
    )
```

```python
import functools

import jax
import jax.numpy as jnp
from jax import lax
from jax.experimental import pallas as pl
from jax.experimental.pallas import tpu as pltpu
from jax.sharding import PartitionSpec as P

DK = 128
BLOCK = 64
CTX_LIFT = 4
EPS = 1e-06
SHARP = 16.0
F32 = jnp.float32
BF16 = jnp.bfloat16
MESH = pl.DeviceIdType.MESH


def dot(a, b):
    return jnp.dot(a, b, preferred_element_type=F32)


def dot_nt(a, b):
    return lax.dot_general(a, b, (((1,), (1,)), ((), ())), preferred_element_type=F32)


def dot_tn(a, b):
    return lax.dot_general(a, b, (((0,), (0,)), ((), ())), preferred_element_type=F32)


def sums(mask, values):
    high = values.astype(BF16)
    low = (values - high.astype(F32)).astype(BF16)
    width = values.shape[1]
    both = dot(mask.astype(F32).astype(BF16), jnp.concatenate([high, low], axis=1))
    return both[:, :width] + both[:, width:]


def log_sigmoid(x):
    return jnp.minimum(x, 0.0) - jnp.log1p(jnp.exp(-jnp.abs(x)))


def chain_kernel(
    n_sp,
    n_tp,
    latents_in,
    sample_vector_in,
    context_in,
    context_vector_in,
    norm_gain_in,
    modulator,
    query_weight,
    key_weight,
    value_weight,
    decay_down_in,
    decay_up_in,
    decay_bias_in,
    decay_extra_in,
    head_gain_in,
    out_weight,
    out,
    latents,
    sample_vector,
    context,
    context_vector,
    norm_gain,
    decay_down,
    decay_up,
    decay_bias,
    decay_extra,
    head_gain,
    mod_w,
    mods,
    lat,
    outer_context,
    extras,
    hid,
    wk,
    wv,
    wq,
    wo,
    acc_k,
    acc_v,
    acc_q,
    tots,
    key_rows,
    query_rows,
    c_state,
    l_state,
    f_out,
    f_in,
    g_out,
    g_in,
    state,
    normed,
    part,
    rs,
    loc_sem,
    mt_s,
    mt_r,
    ms_s,
    ms_r,
    lat_s,
    lat_r,
    lo_s,
    lo_r,
    cx_s,
    cx_r,
    up_s,
    up_r,
    w_s,
    w_r,
    p_s,
    p_r,
    tt_s,
    tt_r,
    f_s,
    f_r,
    g_s,
    g_r,
    o_s,
    o_r,
    rs_s,
    rs_r,
):
    s = lax.axis_index("sp")
    t = lax.axis_index("tp")
    d = lax.axis_index("dp")
    h = lax.rem(d, 2)
    mate = d + 1 - 2 * h
    n_dev = n_sp * n_tp
    me = s * n_tp + t
    n_pairs = n_sp // 2
    pair = s // 2
    pos = lax.rem(s, 2)
    partner = s + 1 - 2 * pos
    is_worker = pos == 1 - s // n_pairs
    is_outer = pos == s // n_pairs
    rows, width = latents.shape
    ctx_rows = context.shape[0]
    length = rows * n_tp
    lat_all = 2 * length
    total = hid.shape[1]
    depth = hid.shape[2]
    half = depth // 2
    heads = decay_bias.shape[1] // DK
    dv = head_gain.shape[1]
    rank = decay_up.shape[1]
    span_t = width // n_tp

    def remote(src, dst, send, recv, device):
        return pltpu.make_async_remote_copy(
            src_ref=src,
            dst_ref=dst,
            send_sem=send,
            recv_sem=recv,
            device_id=device,
            device_id_type=MESH,
        )

    def worker_of(p):
        return 2 * p + 1 - p // (n_pairs // 2)

    def tp_peer(k):
        return lax.rem(t + k, n_tp)

    def tp_from(k):
        return lax.rem(t - k + n_tp, n_tp)

    def sp_peer(k):
        return lax.rem(s + k, n_sp)

    def sp_from(k):
        return lax.rem(s - k + n_sp, n_sp)

    weights = ((key_weight, wk), (value_weight, wv), (query_weight, wq))
    local = [pltpu.make_async_copy(modulator, mod_w, loc_sem.at[0])]
    for m, (source, slots) in enumerate(weights):
        for i in range(2):
            local.append(
                pltpu.make_async_copy(
                    source.at[pl.ds(i * half, half)], slots.at[s, i], loc_sem.at[1 + 2 * m + i]
                )
            )
    local.append(pltpu.make_async_copy(out_weight, wo, loc_sem.at[7]))
    barrier = pltpu.get_barrier_semaphore()
    for k in range(1, n_tp):
        pl.semaphore_signal(barrier, inc=1, device_id={"tp": tp_peer(k)}, device_id_type=MESH)
    for k in range(1, n_sp):
        pl.semaphore_signal(barrier, inc=1, device_id={"sp": sp_peer(k)}, device_id_type=MESH)
    pl.semaphore_signal(barrier, inc=1, device_id={"dp": mate}, device_id_type=MESH)
    small = [
        pltpu.make_async_copy(source, target, loc_sem.at[8 + i])
        for i, (source, target) in enumerate(
            (
                (sample_vector_in, sample_vector),
                (context_vector_in, context_vector),
                (latents_in, latents),
                (context_in, context),
                (decay_extra_in, decay_extra),
                (norm_gain_in, norm_gain),
                (decay_down_in, decay_down),
                (decay_up_in, decay_up),
                (decay_bias_in, decay_bias),
                (head_gain_in, head_gain),
            )
        )
    ]
    for copy in small[:5] + local[:1] + small[5:] + local[1:]:
        copy.start()
    small[2].wait()
    small[3].wait()
    small[4].wait()
    pl.semaphore_wait(barrier, n_tp + n_sp - 1)

    def inner():
        return jnp.logical_and(s >= 1, s <= n_sp - 2)

    def onward(r):
        return s + 1 <= n_sp - 2 if r == 0 else s - 1 >= 1

    def exists(r, j):
        return jnp.logical_and(inner(), s - j >= 0 if r == 0 else s + j < n_sp)

    def origin_of(r, j):
        return s - j if r == 0 else s + j

    def ring_copy(m, r, j, first=False):
        source, slots = weights[m]
        origin = origin_of(r, j)
        src = source.at[pl.ds(h * half, half)] if first else slots.at[origin, h]
        target = s + 1 if r == 0 else s - 1
        return remote(src, slots.at[origin, h], w_s.at[m, r, j], w_r.at[m, r, j], {"sp": target})

    def ring_arrival(m, r, j):
        view = weights[m][1].at[origin_of(r, j), h]
        return remote(view, view, w_s.at[m, r, j - 1], w_r.at[m, r, j - 1], {"sp": s})

    def mate_copy(m, r, j, side):
        view = weights[m][1].at[origin_of(r, j), side]
        return remote(view, view, p_s.at[m, r, j - 1], p_r.at[m, r, j - 1], {"dp": mate})

    def send_own(m):
        for r in range(2):

            @pl.when(onward(r))
            def _():
                ring_copy(m, r, 0, True).start()

    def relay(m, j, share):
        for r in range(2):

            @pl.when(exists(r, j))
            def _():
                ring_arrival(m, r, j).wait_recv()

                @pl.when(onward(r))
                def _():
                    ring_copy(m, r, j).start()

                if share:
                    mate_copy(m, r, j, h).start()

    def whole(slots, o):
        return slots[o].reshape(depth, slots.shape[3])

    def multiply(m, j, acc, count):
        slots = weights[m][1]
        for r in range(2):

            @pl.when(exists(r, j))
            def _():
                origin = origin_of(r, j)
                mate_copy(m, r, j, 1 - h).wait_recv()
                acc[...] += dot(hid[origin, 0:count], whole(slots, origin))

    def lat_copy(k):
        return remote(latents, lat.at[pos, t], lat_s.at[0, k], lat_r.at[0, k], {"tp": tp_peer(k)})

    def lat_arrival(k):
        view = lat.at[pos, tp_from(k)]
        return remote(view, view, lat_s.at[0, k], lat_r.at[0, k], {"tp": t})

    def outer_lat():
        return remote(latents, lat.at[pos, t], lo_s, lo_r, {"sp": partner})

    def outer_lat_arrival():
        view = lat.at[1 - pos, t]
        return remote(view, view, lo_s, lo_r, {"sp": s})

    def lat_relay(k, owner, to):
        view = lat.at[1 - pos, owner]
        return remote(view, view, lat_s.at[1, k], lat_r.at[1, k], {"tp": to})

    def ctx_cols(owner):
        return pl.ds(pl.multiple_of(owner * span_t, span_t), span_t)

    def ctx_copy():
        return remote(
            context.at[:, ctx_cols(t)],
            outer_context.at[:, ctx_cols(t)],
            cx_s.at[0],
            cx_r.at[0],
            {"sp": partner},
        )

    def ctx_relay(k, owner, to):
        view = outer_context.at[:, ctx_cols(owner)]
        return remote(view, view, cx_s.at[k], cx_r.at[k], {"tp": to})

    def extra_copy():
        return remote(decay_extra, extras.at[pos], up_s, up_r, {"sp": partner})

    def extra_arrival():
        view = extras.at[1 - pos]
        return remote(view, view, up_s, up_r, {"sp": s})

    @pl.when(is_outer)
    def _():
        outer_lat().start()
        extra_copy().start()
        ctx_copy().start()
        for m in range(3):
            send_own(m)

    @pl.when(is_worker)
    def _():
        for k in range(1, n_tp):
            lat_copy(k).start()
        send_own(0)
        send_own(1)

    small[0].wait()
    small[1].wait()
    is_first = lax.broadcasted_iota(jnp.int32, (16, width), 0) == 0
    vectors = jnp.where(is_first, sample_vector[...], context_vector[...])
    conditions = (vectors / (1.0 + jnp.exp(-vectors))).astype(BF16)
    local[0].wait()
    mods[me] = dot(conditions, mod_w[...])[0:2]

    def mod_tp(k, owner, to):
        view = mods.at[s * n_tp + owner]
        return remote(view, view, mt_s.at[k], mt_r.at[k], {"tp": to})

    def mod_sp(k, owner, to):
        view = mods.at[pl.ds(owner * n_tp, n_tp)]
        return remote(view, view, ms_s.at[k], ms_r.at[k], {"sp": to})

    for k in range(1, n_tp):
        mod_tp(k, t, tp_peer(k)).start()
    for k in range(1, n_tp):
        mod_tp(k, tp_from(k), t).wait_recv()
    for k in range(1, n_sp):
        mod_sp(k, s, sp_peer(k)).start()
    for copy in small[5:]:
        copy.wait()

    def modulation_now():
        for k in range(1, n_sp):
            mod_sp(k, sp_from(k), s).wait_recv()

    def mod_part(i):
        return jnp.concatenate([mods[j] for j in range(n_dev)], axis=1)[
            :, i * width : (i + 1) * width
        ]

    def tot_copy(k, owner, to):
        view = tots.at[owner]
        return remote(view, view, tt_s.at[k], tt_r.at[k], {"sp": to})

    def has_pred(z):
        return pair > 0 if z == 0 else pair < n_pairs - 1

    def has_succ(z):
        return pair < n_pairs - 1 if z == 0 else pair > 0

    def lone(a, b):
        return jnp.logical_and(a, jnp.logical_not(b))

    def f_copy(z, g):
        to = worker_of(pair + 1) if z == 0 else worker_of(pair - 1)
        return remote(f_out.at[z, g], f_in.at[z, g], f_s.at[z, g], f_r.at[z, g], {"sp": to})

    def g_copy(z, g):
        to = worker_of(pair - 1) if z == 0 else worker_of(pair + 1)
        return remote(g_out.at[z, g], g_in.at[z, g], g_s.at[z, g], g_r.at[z, g], {"sp": to})

    def o_copy(g, where, to):
        view = normed.at[where, g]
        return remote(view, view, o_s.at[g], o_r.at[g], {"sp": to})

    def work():
        outer_lat_arrival().wait_recv()
        for k in range(1, n_tp):
            lat_relay(k, t, tp_peer(k)).start()
        remote(
            outer_context.at[:, ctx_cols(t)],
            outer_context.at[:, ctx_cols(t)],
            cx_s.at[0],
            cx_r.at[0],
            {"sp": s},
        ).wait_recv()
        for k in range(1, n_tp):
            ctx_relay(k, t, tp_peer(k)).start()
        relay(0, 1, True)
        send_own(2)

        lat[pos, t] = latents[...]
        for k in range(1, n_tp):
            lat_arrival(k).wait_recv()
        modulation_now()
        shift = mod_part(0)
        scale = mod_part(1)

        def modulated(x, row):
            x = x.astype(F32)
            x = x * lax.rsqrt(jnp.mean(x * x, axis=-1, keepdims=True) + EPS) * norm_gain[...]
            return (x * (1.0 + scale[row : row + 1]) + shift[row : row + 1]).astype(BF16)

        piece = min(32, ctx_rows)

        def put(x, at):
            count = x.shape[0]
            at = pl.multiple_of(at, piece)
            for o in range(n_sp):
                hid[o, pl.ds(at, count)] = x[:, o * depth : (o + 1) * depth]

        for i in range(n_tp):
            put(modulated(lat[pos, i], 0), pos * length + i * rows)
        for i in range(ctx_rows // piece):
            put(
                modulated(context[i * piece : (i + 1) * piece], 1),
                lat_all + pos * ctx_rows + i * piece,
            )
        for k in range(1, n_tp):
            lat_relay(k, tp_from(k), t).wait_recv()
        relay(1, 1, True)
        for i in range(n_tp):
            put(modulated(lat[1 - pos, i], 0), (1 - pos) * length + i * rows)
        for k in range(1, n_tp):
            ctx_relay(k, tp_from(k), t).wait_recv()
        for i in range(ctx_rows // piece):
            put(
                modulated(outer_context[i * piece : (i + 1) * piece], 1),
                lat_all + (1 - pos) * ctx_rows + i * piece,
            )

        low = dot_nt(hid[0], decay_down[:, 0:depth])
        for o in range(1, n_sp):
            low = low + dot_nt(hid[o], decay_down[:, o * depth : (o + 1) * depth])
        low = low.astype(BF16)
        relay(2, 1, True)

        def log_decays(z):
            x = dot(low[:, z * rank : (z + 1) * rank], decay_up[z]) + decay_bias[z : z + 1]
            return log_sigmoid(x) / SHARP

        row_id = lax.broadcasted_iota(jnp.int32, (lat_all, lat_all), 0)
        col_id = lax.broadcasted_iota(jnp.int32, (lat_all, lat_all), 1)
        same = row_id // BLOCK == col_id // BLOCK
        within_mask = [same & (col_id <= row_id), same & (col_id >= row_id)]
        extras[pos] = decay_extra[...]
        extra_arrival().wait_recv()

        def extra_sums(z):
            columns = []
            for g in range(heads):
                line = jnp.concatenate([extras[i, z, g : g + 1, :] for i in range(2)], axis=1)
                columns.append(
                    jnp.sum(jnp.where(within_mask[z], line, 0.0), axis=1, keepdims=True)
                )
            return jnp.concatenate([jnp.broadcast_to(c, (lat_all, DK)) for c in columns], axis=1)

        decays = [log_decays(z) for z in range(2)]
        within = [sums(within_mask[z], decays[z][:lat_all]) + extra_sums(z) for z in range(2)]
        blocks = lat_all // BLOCK
        totals = [
            [within[0][(b + 1) * BLOCK - 1 : (b + 1) * BLOCK] for b in range(blocks)],
            [within[1][b * BLOCK : b * BLOCK + 1] for b in range(blocks)],
        ]
        none = jnp.zeros_like(totals[0][0])

        def between(z, lo, hi):
            value = none
            for b in range(lo, hi):
                value = value + totals[z][b]
            return value

        crow = lax.broadcasted_iota(jnp.int32, (total - lat_all, total - lat_all), 0)
        ccol = lax.broadcasted_iota(jnp.int32, (total - lat_all, total - lat_all), 1)
        after = [
            sums(ccol > crow, decays[0][lat_all:]),
            sums(ccol < crow, decays[1][lat_all:]),
        ]
        lat_total = [between(z, 0, blocks) for z in range(2)]
        ctx_total = [
            after[0][0:1] + decays[0][lat_all : lat_all + 1],
            after[1][total - lat_all - 1 :] + decays[1][total - 1 :],
        ]
        tots[pair] = jnp.concatenate(lat_total + ctx_total, axis=0)
        for k in range(1, n_pairs):
            to = lax.rem(pair + k, n_pairs)
            tot_copy(k, pair, worker_of(to)).start()

        for copy in local[1:5]:
            copy.wait()
        acc_k[...] = dot(hid[s], whole(wk, s))
        acc_v[...] = dot(hid[s], whole(wv, s))
        multiply(0, 1, acc_k, total)
        multiply(1, 1, acc_v, total)
        for k in range(1, n_pairs):
            tot_copy(k, lax.rem(pair - k + n_pairs, n_pairs), s).wait_recv()
        before = [none, none]
        suffix = [none, none]
        for u in range(n_pairs):
            line = tots[u]
            below = jnp.where(u < pair, 1.0, 0.0)
            above = jnp.where(u > pair, 1.0, 0.0)
            before[0] = before[0] + below * line[0:1]
            before[1] = before[1] + above * line[1:2]
            suffix[0] = suffix[0] + above * line[2:3]
            suffix[1] = suffix[1] + below * line[3:4]
        ctx_weight = [jnp.exp(after[z] + suffix[z]) for z in range(2)]

        def per_block(f):
            return jnp.concatenate([f(b) for b in range(blocks)], axis=0)

        def rows_of(x, b):
            return x[b * BLOCK : (b + 1) * BLOCK]

        ending = [
            jnp.exp(
                per_block(
                    lambda b: totals[0][b] - rows_of(within[0], b) + between(0, b + 1, blocks)
                )
            ),
            jnp.exp(per_block(lambda b: totals[1][b] - rows_of(within[1], b) + between(1, 0, b))),
        ]
        for j in range(2, max(n_sp - 1, 2)):
            relay(0, j, True)
            multiply(0, j, acc_k, total)
            relay(1, j, True)
            multiply(1, j, acc_v, total)
        keys = acc_k[...].astype(BF16)
        values = acc_v[...].astype(BF16)
        ckeys = keys[lat_all:].astype(F32)
        cvals = values[lat_all:]
        keys = keys[:lat_all].astype(F32)
        values = values[:lat_all]

        def columns(g, n):
            return slice(g * n, (g + 1) * n)

        for z in range(2):
            ended = (keys * ending[z]).astype(BF16)
            cended = (ckeys * ctx_weight[z]).astype(BF16)
            lift = CTX_LIFT * jnp.exp(before[z])
            lift_on = CTX_LIFT * jnp.exp(before[z] + lat_total[z])
            for g in range(heads):
                c = dot_tn(cvals[:, columns(g, dv)], cended[:, columns(g, DK)])
                g_out[z, g] = c.astype(BF16)
                own = dot_tn(values[:, columns(g, dv)], ended[:, columns(g, DK)])
                f_out[z, g] = (own + lift_on[:, columns(g, DK)] * c).astype(BF16)
                if n_pairs > 2:
                    c_state[z, g] = c
                    l_state[z, g] = own + lift_on[:, columns(g, DK)] * c
                state[z, g] = lift[:, columns(g, DK)] * c

                @pl.when(lone(has_succ(z), has_pred(z)))
                def _():
                    f_copy(z, g).start()

                @pl.when(lone(has_pred(z), has_succ(z)))
                def _():
                    g_copy(z, g).start()

        if n_pairs > 2:
            for z in range(2):

                @pl.when(jnp.logical_and(has_pred(z), has_succ(z)))
                def _():
                    for g in range(heads):
                        f_copy(z, g).wait_recv()
                        on = jnp.exp(lat_total[z])[:, columns(g, DK)]
                        f_out[z, g] = (l_state[z, g] + on * f_in[z, g].astype(F32)).astype(BF16)
                        f_copy(z, g).start()

                @pl.when(jnp.logical_and(has_pred(z), has_succ(z)))
                def _():
                    for g in range(heads):
                        g_copy(z, g).wait_recv()
                        g_out[z, g] = (c_state[z, g] + g_in[z, g].astype(F32)).astype(BF16)
                        g_copy(z, g).start()

        for z in range(2):
            close = (keys * jnp.exp(-within[z])).astype(BF16)
            near = keys * jnp.exp(per_block(lambda b: totals[z][b] - rows_of(within[z], b)))
            for i in range(blocks):
                for j in range(blocks):
                    if i == j:
                        block = rows_of(close, j)
                    elif (j < i) == (z == 0):
                        gap = between(z, min(i, j) + 1, max(i, j))
                        block = (rows_of(near, j) * jnp.exp(gap)).astype(BF16)
                    else:
                        block = jnp.zeros((BLOCK, heads * DK), BF16)
                    key_rows[z, i, j * BLOCK : (j + 1) * BLOCK] = block
        reach = [jnp.exp(within[z]) for z in range(2)]
        lifted_by = [
            jnp.exp(per_block(lambda b: rows_of(within[0], b) + between(0, 0, b))),
            jnp.exp(per_block(lambda b: rows_of(within[1], b) + between(1, b + 1, blocks))),
        ]

        for copy in local[5:7]:
            copy.wait()
        acc_q[...] = dot(hid[s, 0:lat_all], whole(wq, s))
        for j in range(1, max(n_sp - 1, 2)):
            if j > 1:
                relay(2, j, True)
            multiply(2, j, acc_q, lat_all)
        queries = acc_q[...].astype(BF16).astype(F32)

        for z in range(2):
            near_rows = (queries * reach[z]).astype(BF16)
            far_rows = (queries * lifted_by[z]).astype(BF16)
            for b in range(blocks):
                query_rows[0, z, b] = rows_of(near_rows, b)
                query_rows[1, z, b] = rows_of(far_rows, b)
        turn = blocks // 2
        row_in = lax.broadcasted_iota(jnp.int32, (BLOCK, lat_all), 0)
        col_in = lax.broadcasted_iota(jnp.int32, (BLOCK, lat_all), 1)

        def inside(where, g):
            lines = []
            for b in range(turn):
                i = where * turn + b
                ids = row_in + i * BLOCK
                masks = [col_in <= ids, col_in >= ids]
                line = 0.0
                for z in range(2):
                    score = dot_nt(
                        query_rows[0, z, i, :, columns(g, DK)], key_rows[z, i, :, columns(g, DK)]
                    )
                    line = line + jnp.where(masks[z], score, 0.0)
                lines.append(line.astype(BF16))
            return dot(jnp.concatenate(lines, axis=0), values[:, columns(g, dv)])

        def finish(where, g, mixed):
            for z in range(2):
                rows_z = query_rows[1, z, pl.ds(where * turn, turn), :, columns(g, DK)]
                mixed = mixed + dot_nt(rows_z.reshape(length, DK), state[z, g].astype(BF16))
            by = lax.rsqrt(jnp.mean(mixed * mixed, axis=-1, keepdims=True) + EPS)
            normed[where, g] = (mixed * by * head_gain[...]).astype(BF16)

        first = [inside(1 - pos, g) for g in range(heads)]
        for z in range(2):
            lift = CTX_LIFT * jnp.exp(before[z])

            @pl.when(has_pred(z))
            def _():
                for g in range(heads):
                    if n_pairs == 2:
                        f_copy(z, g).wait_recv()
                    else:

                        @pl.when(jnp.logical_not(has_succ(z)))
                        def _():
                            f_copy(z, g).wait_recv()

                    state[z, g] += f_in[z, g].astype(F32)

            @pl.when(has_succ(z))
            def _():
                for g in range(heads):
                    if n_pairs == 2:
                        g_copy(z, g).wait_recv()
                    else:

                        @pl.when(jnp.logical_not(has_pred(z)))
                        def _():
                            g_copy(z, g).wait_recv()

                    state[z, g] += lift[:, columns(g, DK)] * g_in[z, g].astype(F32)

        for g in range(heads):
            finish(1 - pos, g, first[g])
            o_copy(g, 1 - pos, partner).start()
        for g in range(heads):
            finish(pos, g, inside(pos, g))

    pl.when(is_worker)(work)

    @pl.when(is_outer)
    def _():
        for copy in local[1:7]:
            copy.wait()
        for m in range(3):
            relay(m, 1, False)
        for j in range(2, n_sp - 1):
            relay(0, j, False)
            relay(1, j, False)
        for j in range(2, n_sp - 1):
            relay(2, j, False)
        modulation_now()
        for g in range(heads):
            o_copy(g, pos, s).wait_recv()

    gate = mod_part(2)[0:1]
    local[7].wait()
    chunks = rs_s.shape[1]
    span = width // chunks
    rs_copies = []
    for c in range(chunks):
        cols = slice(c * span, (c + 1) * span)
        product = dot(normed[pos, 0], wo[0:dv, cols])
        for g in range(1, heads):
            product = product + dot(normed[pos, g], wo[g * dv : (g + 1) * dv, cols])
        product = product.astype(BF16)
        for i in range(n_tp):
            part[i, :, cols] = product[i * rows : (i + 1) * rows]
        for k in range(1, n_tp):
            to = tp_peer(k)
            copy = remote(
                part.at[to, :, pl.ds(c * span, span)],
                rs.at[k, :, pl.ds(c * span, span)],
                rs_s.at[k, c],
                rs_r.at[k, c],
                {"tp": to},
            )
            copy.start()
            rs_copies.append(copy)
    for c in range(chunks):
        cols = slice(c * span, (c + 1) * span)
        summed = part[t, :, cols].astype(F32)
        for k in range(1, n_tp):
            rs_copies[c * (n_tp - 1) + k - 1].wait_recv()
            summed = summed + rs[k, :, cols].astype(F32)
        projected = summed.astype(BF16).astype(F32)
        out[:, cols] = (latents[:, cols].astype(F32) + gate[:, cols] * projected).astype(BF16)

    for copy in rs_copies:
        copy.wait_send()
    for k in range(1, n_tp):
        mod_tp(k, t, tp_peer(k)).wait_send()
    for k in range(1, n_sp):
        mod_sp(k, s, sp_peer(k)).wait_send()

    @pl.when(is_outer)
    def _():
        outer_lat().wait_send()
        extra_copy().wait_send()
        ctx_copy().wait_send()

    @pl.when(is_worker)
    def _():
        for k in range(1, n_tp):
            lat_copy(k).wait_send()
            lat_relay(k, t, tp_peer(k)).wait_send()
            ctx_relay(k, t, tp_peer(k)).wait_send()
        for k in range(1, n_pairs):
            tot_copy(k, pair, s).wait_send()
        for g in range(heads):
            o_copy(g, 1 - pos, partner).wait_send()
            for z in range(2):

                @pl.when(has_succ(z))
                def _():
                    f_copy(z, g).wait_send()

                @pl.when(has_pred(z))
                def _():
                    g_copy(z, g).wait_send()

    for m in range(3):
        for r in range(2):

            @pl.when(onward(r))
            def _():
                ring_copy(m, r, 0, True).wait_send()

            for j in range(1, n_sp - 1):

                @pl.when(exists(r, j))
                def _():
                    @pl.when(onward(r))
                    def _():
                        ring_copy(m, r, j).wait_send()

                    @pl.when(is_worker)
                    def _():
                        mate_copy(m, r, j, h).wait_send()


def chain_per_device(n_sp, n_tp, *args):
    (latents, sv, context, cv, gain, modulator, wq, wk, wv, down, up, bias, extra, hg, wo) = args
    rows, width = latents.shape
    ctx_rows = context.shape[0]
    n_dev = n_sp * n_tp
    n_pairs = n_sp // 2
    length = rows * n_tp
    total = 2 * (length + ctx_rows)
    depth = wq.shape[0]
    kw, vw = wk.shape[1], wv.shape[1]
    heads = bias.shape[1] // DK
    dv = hg.shape[0]
    chunks = 4
    vmem = pl.BlockSpec(memory_space=pltpu.VMEM)
    hbm = pl.BlockSpec(memory_space=pl.ANY)
    dma = pltpu.SemaphoreType.DMA
    states = (2, heads, dv, DK)
    chained = states if n_pairs > 2 else (2, heads, 8, DK)
    scratch = [
        pltpu.VMEM(latents.shape, BF16),
        pltpu.VMEM(sv.shape, F32),
        pltpu.VMEM(context.shape, BF16),
        pltpu.VMEM(cv.shape, F32),
        pltpu.VMEM((1, width), F32),
        pltpu.VMEM(down.shape[::-1], BF16),
        pltpu.VMEM(up.shape, BF16),
        pltpu.VMEM(bias.shape, F32),
        pltpu.VMEM((2, heads, length), F32),
        pltpu.VMEM((1, dv), F32),
        pltpu.VMEM(modulator.shape, BF16),
        pltpu.VMEM((n_dev, 2, modulator.shape[1]), F32),
        pltpu.VMEM((2, n_tp, rows, width), BF16),
        pltpu.VMEM((ctx_rows, width), BF16),
        pltpu.VMEM((2, 2, heads, length), F32),
        pltpu.VMEM((n_sp, total, depth), BF16),
        pltpu.VMEM((n_sp, 2, depth // 2, kw), BF16),
        pltpu.VMEM((n_sp, 2, depth // 2, vw), BF16),
        pltpu.VMEM((n_sp, 2, depth // 2, kw), BF16),
        pltpu.VMEM(wo.shape, BF16),
        pltpu.VMEM((total, kw), F32),
        pltpu.VMEM((total, vw), F32),
        pltpu.VMEM((2 * length, kw), F32),
        pltpu.VMEM((n_pairs, 4, kw), F32),
        pltpu.VMEM((2, 2 * length // BLOCK, 2 * length, kw), BF16),
        pltpu.VMEM((2, 2, 2 * length // BLOCK, BLOCK, kw), BF16),
        pltpu.VMEM(chained, F32),
        pltpu.VMEM(chained, F32),
        pltpu.VMEM(states, BF16),
        pltpu.VMEM(states, BF16),
        pltpu.VMEM(states, BF16),
        pltpu.VMEM(states, BF16),
        pltpu.VMEM(states, F32),
        pltpu.VMEM((2, heads, length, dv), BF16),
        pltpu.VMEM((n_tp, rows, width), BF16),
        pltpu.VMEM((n_tp, rows, width), BF16),
        dma((18,)),
        dma((n_tp,)),
        dma((n_tp,)),
        dma((n_sp,)),
        dma((n_sp,)),
        dma((2, n_tp)),
        dma((2, n_tp)),
        dma,
        dma,
        dma((n_tp,)),
        dma((n_tp,)),
        dma,
        dma,
        dma((3, 2, n_sp)),
        dma((3, 2, n_sp)),
        dma((3, 2, n_sp)),
        dma((3, 2, n_sp)),
        dma((n_pairs,)),
        dma((n_pairs,)),
        dma((2, heads)),
        dma((2, heads)),
        dma((2, heads)),
        dma((2, heads)),
        dma((heads,)),
        dma((heads,)),
        dma((n_tp, chunks)),
        dma((n_tp, chunks)),
    ]
    return pl.pallas_call(
        functools.partial(chain_kernel, n_sp, n_tp),
        out_shape=jax.ShapeDtypeStruct(latents.shape, BF16),
        in_specs=[hbm] * 15,
        out_specs=vmem,
        scratch_shapes=scratch,
        compiler_params=pltpu.CompilerParams(
            collective_id=0, has_side_effects=True, vmem_limit_bytes=56 * 1024 * 1024
        ),
    )(
        latents,
        sv,
        context,
        cv,
        gain.reshape(1, -1),
        modulator,
        wq,
        wk,
        wv,
        down.T,
        up,
        bias,
        extra.transpose(0, 2, 1),
        hg.reshape(1, -1),
        wo,
    )


def kernel(
    n_sp,
    n_tp,
    latents_in,
    sample_vector_in,
    context_in,
    context_vector_in,
    norm_gain_in,
    modulator,
    query_weight,
    key_weight,
    value_weight,
    decay_down_in,
    decay_up_in,
    decay_bias_in,
    decay_extra_in,
    head_gain_in,
    out_weight,
    out,
    latents,
    sample_vector,
    context,
    context_vector,
    norm_gain,
    decay_down,
    decay_up,
    decay_bias,
    decay_extra,
    head_gain,
    mod_w,
    mods,
    lat,
    ctx,
    extras,
    hid,
    wk,
    wv,
    wq,
    wo,
    acc_k,
    acc_v,
    acc_q,
    key_rows,
    o_out,
    normed,
    duo,
    wo_twist,
    kept,
    part,
    rs,
    loc_sem,
    mt_s,
    mt_r,
    ms_s,
    ms_r,
    lo_s,
    lo_r,
    cx_s,
    cx_r,
    ex_s,
    ex_r,
    em_s,
    em_r,
    lp_s,
    lp_r,
    cp_s,
    cp_r,
    hd_s,
    hd_r,
    w_s,
    w_r,
    o_s,
    o_r,
    wx_s,
    wx_r,
    wm_s,
    wm_r,
    rs_s,
    rs_r,
    vouch,
):
    s = lax.axis_index("sp")
    t = lax.axis_index("tp")
    d = lax.axis_index("dp")
    h = lax.rem(d, 2)
    mate = d + 1 - 2 * h
    n_dev = n_sp * n_tp
    me = s * n_tp + t
    first_plane = n_sp // 2 - 1
    last_plane = n_sp // 2
    side = s - first_plane
    target = first_plane + h
    is_worker = jnp.logical_and(s >= first_plane, s <= last_plane)
    is_leader = s == target
    is_follower = jnp.logical_and(is_worker, s != target)
    is_sender = s != target
    rows, width = latents.shape
    ctx_rows = context.shape[0]
    length = rows * n_tp
    lat_all = n_sp * length
    total = hid.shape[1]
    depth = hid.shape[2]
    heads = decay_bias.shape[1] // DK
    dv = head_gain.shape[1]
    rank = decay_up.shape[1]
    span_t = width // n_tp

    def remote(src, dst, send, recv, device):
        return pltpu.make_async_remote_copy(
            src_ref=src,
            dst_ref=dst,
            send_sem=send,
            recv_sem=recv,
            device_id=device,
            device_id_type=MESH,
        )

    def tp_peer(k):
        return lax.rem(t + k, n_tp)

    def tp_from(k):
        return lax.rem(t - k + n_tp, n_tp)

    def sp_peer(k):
        return lax.rem(s + k, n_sp)

    def sp_from(k):
        return lax.rem(s - k + n_sp, n_sp)

    def head_cols(size):
        return pl.ds(pl.multiple_of(h * size, DK), size)

    weights = ((key_weight, wk, DK), (value_weight, wv, dv), (query_weight, wq, DK))
    own_weight = [
        pltpu.make_async_copy(source.at[:, head_cols(size)], slots.at[s], loc_sem.at[1 + m])
        for m, (source, slots, size) in enumerate(weights)
    ]
    mod_load = pltpu.make_async_copy(modulator, mod_w, loc_sem.at[0])
    out_load = pltpu.make_async_copy(out_weight, wo, loc_sem.at[4])
    barrier = pltpu.get_barrier_semaphore()

    def signal(semaphore, device):
        pl.semaphore_signal(semaphore, inc=1, device_id=device, device_id_type=MESH)

    above = s + 1 < n_sp
    below = s > 0
    twist = t + 1 - 2 * lax.rem(t, 2)
    cross = lax.rem(t + 2, n_tp)
    signal(barrier, {"tp": twist})
    signal(barrier, {"tp": cross})
    signal(barrier, {"dp": mate})

    @pl.when(above)
    def _():
        signal(barrier, {"sp": s + 1})

    @pl.when(below)
    def _():
        signal(barrier, {"sp": s - 1})

    small = [
        pltpu.make_async_copy(source, where, loc_sem.at[8 + i])
        for i, (source, where) in enumerate(
            (
                (sample_vector_in, sample_vector),
                (context_vector_in, context_vector),
                (latents_in, latents),
                (context_in, context),
                (decay_extra_in, decay_extra),
                (norm_gain_in, norm_gain),
                (decay_down_in, decay_down),
                (decay_up_in, decay_up),
                (decay_bias_in, decay_bias),
                (head_gain_in, head_gain),
            )
        )
    ]
    for copy in small[:5] + own_weight + [mod_load] + small[5:] + [out_load]:
        copy.start()
    for copy in small[2:5] + own_weight:
        copy.wait()
    pl.semaphore_wait(barrier, 3 + jnp.where(above, 1, 0) + jnp.where(below, 1, 0))
    signal(vouch.at[n_sp], {"tp": twist})

    def pass_word(step):
        @pl.when(jnp.logical_and(below, s + step < n_sp))
        def _():
            signal(vouch.at[step], {"sp": s - 1})

        @pl.when(jnp.logical_and(above, s - step >= 0))
        def _():
            signal(vouch.at[0 if step == 1 else n_sp - 1], {"sp": s + 1})

    def hear_word(step):
        @pl.when(s + step + 1 < n_sp)
        def _():
            pl.semaphore_wait(vouch.at[step], 1)

        @pl.when(s - step - 1 >= 0)
        def _():
            pl.semaphore_wait(vouch.at[0 if step == 1 else n_sp - 1], 1)

    pass_word(1)

    def onward(r):
        return s + 1 <= last_plane if r == 0 else s - 1 >= first_plane

    def exists(r, j):
        if r == 0:
            return jnp.logical_and(s <= last_plane, s - j >= 0)
        return jnp.logical_and(s >= first_plane, s + j < n_sp)

    def origin_of(r, j):
        return s - j if r == 0 else s + j

    def ring_copy(m, r, j):
        view = weights[m][1].at[origin_of(r, j)]
        to = s + 1 if r == 0 else s - 1
        return remote(view, view, w_s.at[m, r, j], w_r.at[m, r, j], {"sp": to})

    def ring_arrival(m, r, j):
        view = weights[m][1].at[origin_of(r, j)]
        return remote(view, view, w_s.at[m, r, j - 1], w_r.at[m, r, j - 1], {"sp": s})

    def relay(m, j):
        for r in range(2):

            @pl.when(exists(r, j))
            def _():
                ring_arrival(m, r, j).wait_recv()

                @pl.when(onward(r))
                def _():
                    ring_copy(m, r, j).start()

    def multiply(m, j, acc, count):
        slots = weights[m][1]
        for r in range(2):

            @pl.when(exists(r, j))
            def _():
                origin = origin_of(r, j)
                acc[...] += dot(hid[origin, 0:count], slots[origin])

    def lat_in(b, to):
        view = lat.at[b, t]
        return remote(latents, view, lo_s, lo_r.at[b], {"sp": to})

    def extra_in(b, to):
        return remote(decay_extra, extras.at[b], ex_s, ex_r.at[b], {"sp": to})

    def ctx_cols(owner):
        return pl.ds(pl.multiple_of(owner * span_t, span_t), span_t)

    def ctx_in(b, to):
        return remote(
            context.at[:, ctx_cols(t)],
            ctx.at[b, :, ctx_cols(t)],
            cx_s,
            cx_r.at[b],
            {"sp": to},
        )

    def lat_plane(b, k, owner, to):
        view = lat.at[b, owner]
        return remote(view, view, lp_s.at[b, k], lp_r.at[b, k], {"tp": to})

    def lat_own(k):
        return remote(latents, lat.at[s, t], lp_s.at[s, k], lp_r.at[s, k], {"tp": tp_peer(k)})

    def ctx_plane(b, k, owner, to):
        view = ctx.at[b, :, ctx_cols(owner)]
        return remote(view, view, cp_s.at[b, k], cp_r.at[b, k], {"tp": to})

    def hid_copy(i, at, count):
        view = hid.at[:, pl.ds(pl.multiple_of(at, 16), count)]
        return remote(view, view, hd_s.at[i], hd_r.at[i], {"dp": mate})

    def lat_hid(b):
        return hid_copy(b, b * length, length)

    def ctx_hid(b):
        return hid_copy(n_sp + b, lat_all + b * ctx_rows, ctx_rows)

    def extra_mate():
        return remote(extras, extras, em_s, em_r, {"dp": mate})

    def others():
        towards = 1 - 2 * side
        steps = sorted(range(-first_plane, n_sp // 2 + 1), key=abs)
        return [s + towards * step for step in steps if step]

    adjacent = jnp.logical_or(s == target + 1, s == target - 1)

    def send_rows():
        lat_in(s, target).start()
        extra_in(s, target).start()
        ctx_in(s, target).start()

    def send_weight(m):
        for r in range(2):

            @pl.when(onward(r))
            def _():
                ring_copy(m, r, 0).start()

    pl.when(adjacent)(send_rows)

    @pl.when(is_leader)
    def _():
        for k in (1, 2, 3):

            @pl.when(tp_peer(k) != lax.rem(twist + 2, n_tp))
            def _():
                lat_own(k).start()

    send_weight(0)
    hear_word(1)
    pass_word(2)
    pl.semaphore_wait(vouch.at[n_sp], 1)
    pl.when(jnp.logical_and(is_sender, jnp.logical_not(adjacent)))(send_rows)

    @pl.when(is_leader)
    def _():
        for k in (1, 2, 3):

            @pl.when(tp_peer(k) == lax.rem(twist + 2, n_tp))
            def _():
                lat_own(k).start()

    send_weight(1)
    send_weight(2)

    small[0].wait()
    small[1].wait()
    is_first = lax.broadcasted_iota(jnp.int32, (16, width), 0) == 0
    vectors = jnp.where(is_first, sample_vector[...], context_vector[...])
    conditions = (vectors / (1.0 + jnp.exp(-vectors))).astype(BF16)
    mod_load.wait()
    mods[me] = dot(conditions, mod_w[...])[0:2]

    def mod_tp(k, owner, to):
        view = mods.at[s * n_tp + owner]
        return remote(view, view, mt_s.at[k], mt_r.at[k], {"tp": to})

    def mod_sp(k, owner, to):
        view = mods.at[pl.ds(owner * n_tp, n_tp)]
        return remote(view, view, ms_s.at[k], ms_r.at[k], {"sp": to})

    for k in range(1, n_tp):
        mod_tp(k, t, tp_peer(k)).start()
    for k in range(1, n_tp):
        mod_tp(k, tp_from(k), t).wait_recv()
    hear_word(2)
    for k in range(1, n_sp):
        mod_sp(k, s, sp_peer(k)).start()
    for copy in small[5:]:
        copy.wait()

    def mod_part(i):
        return jnp.concatenate([mods[j] for j in range(n_dev)], axis=1)[
            :, i * width : (i + 1) * width
        ]

    def mods_arrive():
        for k in range(1, n_sp):
            mod_sp(k, sp_from(k), s).wait_recv()

    piece = min(32, ctx_rows)

    def put(x, row, at):
        count = x.shape[0]
        x = x.astype(F32)
        x = x * lax.rsqrt(jnp.mean(x * x, axis=-1, keepdims=True) + EPS) * norm_gain[...]
        scale = mod_part(1)[row : row + 1]
        shift = mod_part(0)[row : row + 1]
        x = (x * (1.0 + scale) + shift).astype(BF16)
        at = pl.multiple_of(at, piece)
        for o in range(n_sp):
            hid[o, pl.ds(at, count)] = x[:, o * depth : (o + 1) * depth]

    lead = jnp.where(side == h, d, mate)
    parity = lax.rem(t, 2)
    two = n_tp // 2

    def inside(b):
        return first_plane <= b <= last_plane

    def o_copies(b):
        if inside(b):
            to = {"sp": b, "dp": lead}
            return [remote(o_out.at[b], normed.at[h], o_s.at[b, 0], o_r.at[0, h], to)]
        return [
            remote(
                o_out.at[b, pl.ds(two * rank_of, two)],
                duo.at[group, h],
                o_s.at[b, group],
                o_r.at[group, h],
                {"sp": b, "tp": to, "dp": lead},
            )
            for group, (rank_of, to) in enumerate(((parity, t), (1 - parity, twist)))
        ]

    def o_mate():
        return remote(o_out.at[s], normed.at[h], o_s.at[s, 0], o_r.at[0, h], {"dp": mate})

    def o_arrival(c):
        return remote(normed.at[c], normed.at[c], o_s.at[s, 0], o_r.at[0, c], {"dp": mate})

    def duo_arrival(group, c):
        view = duo.at[group, c]
        return remote(view, view, o_s.at[s, 0], o_r.at[group, c], {"dp": mate})

    half_rows = wo.shape[0] // 2

    def wo_half(where, side_of):
        return where.at[pl.ds(pl.multiple_of(side_of * half_rows, half_rows), half_rows)]

    def wo_cross():
        return remote(wo_half(wo, h), wo_half(wo_twist, h), wx_s, wx_r, {"tp": twist})

    def wo_mate(side_of):
        view = wo_half(wo_twist, side_of)
        return remote(view, view, wm_s, wm_r, {"dp": mate})

    def work():
        blocks = lat_all // BLOCK
        per = length // BLOCK

        @pl.when(is_leader)
        def _():
            for b in others():
                remote(lat.at[b, t], lat.at[b, t], lo_s, lo_r.at[b], {"sp": s}).wait_recv()
                for k in range(1, n_tp):
                    lat_plane(b, k, t, tp_peer(k)).start()
            for b in others():
                view = ctx.at[b, :, ctx_cols(t)]
                remote(view, view, cx_s, cx_r.at[b], {"sp": s}).wait_recv()
                for k in range(1, n_tp):
                    ctx_plane(b, k, t, tp_peer(k)).start()
            lat[s, t] = latents[...]
            mods_arrive()
            for i, b in enumerate([s] + others()):
                for k in range(1, n_tp):
                    lat_plane(b, k, tp_from(k), t).wait_recv()
                for u in range(n_tp):
                    put(lat[b, u], 0, b * length + u * rows)
                lat_hid(b).start()
                if i == 0:
                    relay(0, 1)
                    extras[s] = decay_extra[...]
                    for c in others():
                        remote(
                            extras.at[c], extras.at[c], ex_s, ex_r.at[c], {"sp": s}
                        ).wait_recv()
                    extra_mate().start()
                if i == 2:
                    relay(1, 1)

        @pl.when(is_follower)
        def _():
            relay(0, 1)
            relay(1, 1)
            mods_arrive()
            extra_mate().wait_recv()
            for b in range(n_sp):
                lat_hid(b).wait_recv()

        def lows(lo, hi):
            value = dot_nt(hid[0, lo:hi], decay_down[:, 0:depth])
            for o in range(1, n_sp):
                value = value + dot_nt(
                    hid[o, lo:hi], decay_down[:, o * depth : (o + 1) * depth]
                )
            return value.astype(BF16)

        def log_decays(low, z):
            x = dot(low[:, z * rank : (z + 1) * rank], decay_up[z, :, head_cols(DK)])
            return log_sigmoid(x + decay_bias[z : z + 1, head_cols(DK)]) / SHARP

        low = lows(0, lat_all)
        relay(2, 1)
        decays = [log_decays(low, z) for z in range(2)]
        group = 2 * length
        row_id = lax.broadcasted_iota(jnp.int32, (group, group), 0)
        col_id = lax.broadcasted_iota(jnp.int32, (group, group), 1)
        same = row_id // BLOCK == col_id // BLOCK
        inner = [same & (col_id <= row_id), same & (col_id >= row_id)]

        def within_of(z):
            pieces = []
            for i in range(lat_all // group):
                line = jnp.concatenate(
                    [extras[2 * i + e, z, pl.ds(h, 1), :] for e in range(2)], axis=1
                )
                extra = jnp.sum(jnp.where(inner[z], line, 0.0), axis=1, keepdims=True)
                pieces.append(sums(inner[z], decays[z][i * group : (i + 1) * group]) + extra)
            return jnp.concatenate(pieces, axis=0)

        within = [within_of(z) for z in range(2)]
        totals = [
            [within[0][(b + 1) * BLOCK - 1 : (b + 1) * BLOCK] for b in range(blocks)],
            [within[1][b * BLOCK : b * BLOCK + 1] for b in range(blocks)],
        ]
        none = jnp.zeros_like(totals[0][0])

        def between(z, lo, hi):
            value = none
            for b in range(lo, hi):
                value = value + totals[z][b]
            return value

        def per_block(f):
            return jnp.concatenate([f(b) for b in range(blocks)], axis=0)

        def rows_of(x, b):
            return x[b * BLOCK : (b + 1) * BLOCK]

        def key_span(z, i):
            if z == 0:
                return 0, min(-(-(i + 1) * BLOCK // DK) * DK, lat_all)
            return i * BLOCK // DK * DK, lat_all

        reach = [jnp.exp(within[z]) for z in range(2)]
        lifted_by = [
            jnp.exp(per_block(lambda b: rows_of(within[0], b) + between(0, 0, b))),
            jnp.exp(per_block(lambda b: rows_of(within[1], b) + between(1, b + 1, blocks))),
        ]

        @pl.when(is_leader)
        def _():
            for i in range(ctx_rows // piece):
                put(
                    context[i * piece : (i + 1) * piece],
                    1,
                    lat_all + s * ctx_rows + i * piece,
                )
            ctx_hid(s).start()
            for b in others():
                for k in range(1, n_tp):
                    ctx_plane(b, k, tp_from(k), t).wait_recv()
                for i in range(ctx_rows // piece):
                    put(
                        ctx[b, i * piece : (i + 1) * piece],
                        1,
                        lat_all + b * ctx_rows + i * piece,
                    )
                ctx_hid(b).start()

        @pl.when(is_follower)
        def _():
            for b in range(n_sp):
                ctx_hid(b).wait_recv()

        low_ctx = lows(lat_all, total)
        ctx_decays = [log_decays(low_ctx, z) for z in range(2)]
        ctx_all = total - lat_all
        crow = lax.broadcasted_iota(jnp.int32, (ctx_all, ctx_all), 0)
        ccol = lax.broadcasted_iota(jnp.int32, (ctx_all, ctx_all), 1)
        ctx_weight = [
            jnp.exp(sums(ccol > crow, ctx_decays[0])),
            jnp.exp(sums(ccol < crow, ctx_decays[1])),
        ]

        acc_k[...] = dot(hid[s], wk[s])
        acc_v[...] = dot(hid[s], wv[s])
        acc_q[...] = dot(hid[s, 0:lat_all], wq[s])
        multiply(0, 1, acc_k, total)
        multiply(1, 1, acc_v, total)
        multiply(2, 1, acc_q, lat_all)
        far = range(2, n_sp // 2 + 1)
        for j in far:
            relay(0, j)
            multiply(0, j, acc_k, total)
        keys = acc_k[...].astype(BF16).astype(F32)
        ckeys = keys[lat_all:]
        keys = keys[:lat_all]
        for z in range(2):
            close = (keys * jnp.exp(-within[z])).astype(BF16)
            near = keys * jnp.exp(per_block(lambda b: totals[z][b] - rows_of(within[z], b)))
            for i in range(blocks):
                lo, hi = key_span(z, i)
                for j in range(lo // BLOCK, hi // BLOCK):
                    if (j > i) if z == 0 else (j < i):
                        block = jnp.zeros((BLOCK, DK), BF16)
                    elif i == j:
                        block = rows_of(close, j)
                    else:
                        gap = between(z, min(i, j) + 1, max(i, j))
                        block = (rows_of(near, j) * jnp.exp(gap)).astype(BF16)
                    key_rows[z, i, j * BLOCK : (j + 1) * BLOCK] = block
        for j in far:
            relay(1, j)
            multiply(1, j, acc_v, total)
        values = acc_v[...].astype(BF16)
        cvals = values[lat_all:]
        values = values[:lat_all]
        state = [
            (CTX_LIFT * dot_tn(cvals, (ckeys * ctx_weight[z]).astype(BF16))).astype(BF16)
            for z in range(2)
        ]
        for j in far:
            relay(2, j)
            multiply(2, j, acc_q, lat_all)
        tri_row = lax.broadcasted_iota(jnp.int32, (BLOCK, lat_all), 0)
        tri_col = lax.broadcasted_iota(jnp.int32, (BLOCK, lat_all), 1)

        def attend(b):
            lines = []
            part_of = slice(b * length, (b + 1) * length)
            queries = acc_q[part_of].astype(BF16).astype(F32)
            query_dec = [(queries * reach[z][part_of]).astype(BF16) for z in range(2)]
            lifted = [(queries * lifted_by[z][part_of]).astype(BF16) for z in range(2)]
            for i in range(b * per, (b + 1) * per):
                full = []
                for z in range(2):
                    lo, hi = key_span(z, i)
                    score = dot_nt(rows_of(query_dec[z], i - b * per), key_rows[z, i, lo:hi])
                    ids = tri_row[:, lo:hi] + i * BLOCK
                    cols = tri_col[:, lo:hi]
                    keep = cols <= ids if z == 0 else cols >= ids
                    score = jnp.where(keep, score, 0.0)
                    pads = [jnp.zeros((BLOCK, lo), F32), score, jnp.zeros((BLOCK, lat_all - hi), F32)]
                    full.append(jnp.concatenate([p for p in pads if p.shape[1]], axis=1))
                lines.append((full[0] + full[1]).astype(BF16))
            mixed = dot(jnp.concatenate(lines, axis=0), values)
            for z in range(2):
                mixed = mixed + dot_nt(lifted[z], state[z])
            by = lax.rsqrt(jnp.mean(mixed * mixed, axis=-1, keepdims=True) + EPS)
            return (mixed * by * head_gain[...]).astype(BF16)

        for w in range(2):

            @pl.when(side == w)
            def _():
                here = first_plane + w
                near = here - 1 + 2 * w
                order = sorted((b for b in range(n_sp) if not inside(b)), key=lambda b: b == near)[:1] + [here + 1 - 2 * w, near, here]

                def store(b, value):
                    for u in range(n_tp):
                        at = u if inside(b) else u % 2 * two + u // 2
                        o_out[b, at] = value[u * rows : (u + 1) * rows]

                for b in order:
                    result = attend(b)
                    if b != here:
                        store(b, result)
                        for copy in o_copies(b):
                            copy.start()
                        continue

                    @pl.when(is_leader)
                    def _():
                        for u in range(n_tp):
                            normed[h, u] = result[u * rows : (u + 1) * rows]

                    @pl.when(is_follower)
                    def _():
                        store(b, result)
                        o_mate().start()

    pl.when(is_worker)(work)

    is_outer = jnp.logical_not(is_worker)

    @pl.when(is_outer)
    def _():
        out_load.wait()
        wo_cross().start()
        mods_arrive()
        wo_cross().wait_recv()
        wo_mate(h).start()
        wo_mate(1 - h).wait_recv()
        for group in range(2):
            for c in range(heads):
                duo_arrival(group, c).wait_recv()

    @pl.when(is_leader)
    def _():
        o_arrival(1 - h).wait_recv()

    @pl.when(is_follower)
    def _():
        for c in range(heads):
            o_arrival(c).wait_recv()

    chunks = rs_s.shape[1]
    span = width // chunks

    def rs_copy(index, k, c, to):
        return remote(
            part.at[index, :, pl.ds(c * span, span)],
            rs.at[k, :, pl.ds(c * span, span)],
            rs_s.at[k, c],
            rs_r.at[k, c],
            {"tp": to},
        )

    def write_out(cols, summed):
        gate = jnp.concatenate([mods[j] for j in range(n_dev)], axis=1)[0:1, 2 * width :]
        projected = summed.astype(BF16).astype(F32)
        out[:, cols] = (latents[:, cols].astype(F32) + gate[:, cols] * projected).astype(BF16)

    @pl.when(is_worker)
    def _():
        out_load.wait()
        for c in range(chunks):
            cols = slice(c * span, (c + 1) * span)
            product = 0.0
            for g in range(heads):
                product = product + dot(
                    normed[g].reshape(length, dv), wo[g * dv : (g + 1) * dv, cols]
                )
            product = product.astype(BF16)
            for i in range(n_tp):
                part[i, :, cols] = product[i * rows : (i + 1) * rows]
            for k in range(1, n_tp):
                rs_copy(tp_peer(k), k, c, tp_peer(k)).start()
        for c in range(chunks):
            cols = slice(c * span, (c + 1) * span)
            summed = part[t, :, cols].astype(F32)
            for k in range(1, n_tp):
                rs_copy(tp_peer(k), k, c, tp_peer(k)).wait_recv()
                summed = summed + rs[k, :, cols].astype(F32)
            write_out(cols, summed)
        for c in range(chunks):
            for k in range(1, n_tp):
                rs_copy(tp_peer(k), k, c, tp_peer(k)).wait_send()

    @pl.when(is_outer)
    def _():
        for c in range(chunks):
            cols = slice(c * span, (c + 1) * span)
            product = 0.0
            for group, matrix in enumerate((wo, wo_twist)):
                for g in range(heads):
                    product = product + dot(
                        duo[group, g].reshape(two * rows, dv), matrix[g * dv : (g + 1) * dv, cols]
                    )
            low_half = t < two
            kept[:, cols] = jnp.where(low_half, product[:rows], product[rows:])
            part[0, :, cols] = jnp.where(low_half, product[rows:], product[:rows]).astype(BF16)
            rs_copy(0, 1, c, cross).start()
        for c in range(chunks):
            cols = slice(c * span, (c + 1) * span)
            rs_copy(0, 1, c, cross).wait_recv()
            write_out(cols, kept[:, cols] + rs[1, :, cols].astype(F32))
        for c in range(chunks):
            rs_copy(0, 1, c, cross).wait_send()
        wo_cross().wait_send()
        wo_mate(h).wait_send()

    for k in range(1, n_tp):
        mod_tp(k, t, tp_peer(k)).wait_send()
    for k in range(1, n_sp):
        mod_sp(k, s, sp_peer(k)).wait_send()

    @pl.when(is_sender)
    def _():
        lat_in(s, target).wait_send()
        extra_in(s, target).wait_send()
        ctx_in(s, target).wait_send()

    @pl.when(is_leader)
    def _():
        extra_mate().wait_send()
        for k in range(1, n_tp):
            lat_own(k).wait_send()
            for b in others():
                lat_plane(b, k, t, tp_peer(k)).wait_send()
                ctx_plane(b, k, t, tp_peer(k)).wait_send()
        for b in range(n_sp):
            lat_hid(b).wait_send()
            ctx_hid(b).wait_send()

    @pl.when(is_follower)
    def _():
        o_mate().wait_send()

    for w in range(2):

        @pl.when(side == w)
        def _():
            for b in range(n_sp):
                if b != first_plane + w:
                    for copy in o_copies(b):
                        copy.wait_send()

    for m in range(3):
        for r in range(2):

            @pl.when(onward(r))
            def _():
                ring_copy(m, r, 0).wait_send()

            for j in range(1, n_sp // 2 + 1):

                @pl.when(jnp.logical_and(exists(r, j), onward(r)))
                def _():
                    ring_copy(m, r, j).wait_send()


def per_device(n_sp, n_tp, *args):
    (latents, sv, context, cv, gain, modulator, wq, wk, wv, down, up, bias, extra, hg, wo) = args
    heads = bias.shape[1] // DK
    if n_sp != 4 or n_tp != 4 or heads != 2:
        return chain_per_device(n_sp, n_tp, *args)
    rows, width = latents.shape
    ctx_rows = context.shape[0]
    n_dev = n_sp * n_tp
    length = rows * n_tp
    lat_all = n_sp * length
    total = n_sp * (length + ctx_rows)
    depth = wq.shape[0]
    dv = hg.shape[0]
    chunks = 4
    vmem = pl.BlockSpec(memory_space=pltpu.VMEM)
    hbm = pl.BlockSpec(memory_space=pl.ANY)
    dma = pltpu.SemaphoreType.DMA
    scratch = [
        pltpu.VMEM(latents.shape, BF16),
        pltpu.VMEM(sv.shape, F32),
        pltpu.VMEM(context.shape, BF16),
        pltpu.VMEM(cv.shape, F32),
        pltpu.VMEM((1, width), F32),
        pltpu.VMEM(down.shape[::-1], BF16),
        pltpu.VMEM(up.shape, BF16),
        pltpu.VMEM(bias.shape, F32),
        pltpu.VMEM((2, heads, length), F32),
        pltpu.VMEM((1, dv), F32),
        pltpu.VMEM(modulator.shape, BF16),
        pltpu.VMEM((n_dev, 2, modulator.shape[1]), F32),
        pltpu.VMEM((n_sp, n_tp, rows, width), BF16),
        pltpu.VMEM((n_sp, ctx_rows, width), BF16),
        pltpu.VMEM((n_sp, 2, heads, length), F32),
        pltpu.VMEM((n_sp, total, depth), BF16),
        pltpu.VMEM((n_sp, depth, DK), BF16),
        pltpu.VMEM((n_sp, depth, dv), BF16),
        pltpu.VMEM((n_sp, depth, DK), BF16),
        pltpu.VMEM(wo.shape, BF16),
        pltpu.VMEM((total, DK), F32),
        pltpu.VMEM((total, dv), F32),
        pltpu.VMEM((lat_all, DK), F32),
        pltpu.VMEM((2, lat_all // BLOCK, lat_all, DK), BF16),
        pltpu.VMEM((n_sp, n_tp, rows, dv), BF16),
        pltpu.VMEM((heads, n_tp, rows, dv), BF16),
        pltpu.VMEM((2, heads, n_tp // 2, rows, dv), BF16),
        pltpu.VMEM(wo.shape, BF16),
        pltpu.VMEM((rows, width), F32),
        pltpu.VMEM((n_tp, rows, width), BF16),
        pltpu.VMEM((n_tp, rows, width), BF16),
        dma((18,)),
        dma((n_tp,)),
        dma((n_tp,)),
        dma((n_sp,)),
        dma((n_sp,)),
        dma,
        dma((n_sp,)),
        dma,
        dma((n_sp,)),
        dma,
        dma((n_sp,)),
        dma,
        dma,
        dma((n_sp, n_tp)),
        dma((n_sp, n_tp)),
        dma((n_sp, n_tp)),
        dma((n_sp, n_tp)),
        dma((2 * n_sp,)),
        dma((2 * n_sp,)),
        dma((3, 2, n_sp)),
        dma((3, 2, n_sp)),
        dma((n_sp, 2)),
        dma((2, heads)),
        dma,
        dma,
        dma,
        dma,
        dma((n_tp, chunks)),
        dma((n_tp, chunks)),
        pltpu.SemaphoreType.REGULAR((n_sp + n_tp,)),
    ]
    return pl.pallas_call(
        functools.partial(kernel, n_sp, n_tp),
        out_shape=jax.ShapeDtypeStruct(latents.shape, BF16),
        in_specs=[hbm] * 15,
        out_specs=vmem,
        scratch_shapes=scratch,
        compiler_params=pltpu.CompilerParams(
            collective_id=0, has_side_effects=True, vmem_limit_bytes=56 * 1024 * 1024
        ),
    )(
        latents,
        sv,
        context,
        cv,
        gain.reshape(1, -1),
        modulator,
        wq,
        wk,
        wv,
        down.T,
        up,
        bias,
        extra.transpose(0, 2, 1),
        hg.reshape(1, -1),
        wo,
    )


def solution(mesh):
    placed = (
        P(("dp", "sp", "tp"), None),
        P("dp", None),
        P(("dp", "sp"), None),
        P(),
        P(),
        P(None, ("sp", "tp")),
        P("sp", "tp"),
        P("sp", "tp"),
        P("sp", "tp"),
        P(),
        P(None, None, "tp"),
        P(None, "tp"),
        P(None, ("dp", "sp"), "tp"),
        P(),
        P("tp", None),
    )
    return jax.shard_map(
        functools.partial(per_device, mesh.shape["sp"], mesh.shape["tp"]),
        mesh=mesh,
        in_specs=placed,
        out_specs=P(("dp", "sp", "tp"), None),
        check_vma=False,
    )
```

```python
import functools

import jax
import jax.numpy as jnp
from jax import lax
from jax.experimental import pallas as pl
from jax.experimental.pallas import tpu as pltpu
from jax.sharding import PartitionSpec as P

DK = 128
BLOCK = 64
CTX_LIFT = 4
EPS = 1e-06
SHARP = 16.0
F32 = jnp.float32
BF16 = jnp.bfloat16
MESH = pl.DeviceIdType.MESH


def dot(a, b):
    return jnp.dot(a, b, preferred_element_type=F32)


def dot_nt(a, b):
    return lax.dot_general(a, b, (((1,), (1,)), ((), ())), preferred_element_type=F32)


def dot_tn(a, b):
    return lax.dot_general(a, b, (((0,), (0,)), ((), ())), preferred_element_type=F32)


def sums(mask, values):
    high = values.astype(BF16)
    low = (values - high.astype(F32)).astype(BF16)
    width = values.shape[1]
    both = dot(mask.astype(F32).astype(BF16), jnp.concatenate([high, low], axis=1))
    return both[:, :width] + both[:, width:]


def log_sigmoid(x):
    return jnp.minimum(x, 0.0) - jnp.log1p(jnp.exp(-jnp.abs(x)))


def chain_kernel(
    n_sp,
    n_tp,
    latents_in,
    sample_vector_in,
    context_in,
    context_vector_in,
    norm_gain_in,
    modulator,
    query_weight,
    key_weight,
    value_weight,
    decay_down_in,
    decay_up_in,
    decay_bias_in,
    decay_extra_in,
    head_gain_in,
    out_weight,
    out,
    latents,
    sample_vector,
    context,
    context_vector,
    norm_gain,
    decay_down,
    decay_up,
    decay_bias,
    decay_extra,
    head_gain,
    mod_w,
    mods,
    lat,
    outer_context,
    extras,
    hid,
    wk,
    wv,
    wq,
    wo,
    acc_k,
    acc_v,
    acc_q,
    tots,
    key_rows,
    query_rows,
    c_state,
    l_state,
    f_out,
    f_in,
    g_out,
    g_in,
    state,
    normed,
    part,
    rs,
    loc_sem,
    mt_s,
    mt_r,
    ms_s,
    ms_r,
    lat_s,
    lat_r,
    lo_s,
    lo_r,
    cx_s,
    cx_r,
    up_s,
    up_r,
    w_s,
    w_r,
    p_s,
    p_r,
    tt_s,
    tt_r,
    f_s,
    f_r,
    g_s,
    g_r,
    o_s,
    o_r,
    rs_s,
    rs_r,
):
    s = lax.axis_index("sp")
    t = lax.axis_index("tp")
    d = lax.axis_index("dp")
    h = lax.rem(d, 2)
    mate = d + 1 - 2 * h
    n_dev = n_sp * n_tp
    me = s * n_tp + t
    n_pairs = n_sp // 2
    pair = s // 2
    pos = lax.rem(s, 2)
    partner = s + 1 - 2 * pos
    is_worker = pos == 1 - s // n_pairs
    is_outer = pos == s // n_pairs
    rows, width = latents.shape
    ctx_rows = context.shape[0]
    length = rows * n_tp
    lat_all = 2 * length
    total = hid.shape[1]
    depth = hid.shape[2]
    half = depth // 2
    heads = decay_bias.shape[1] // DK
    dv = head_gain.shape[1]
    rank = decay_up.shape[1]
    span_t = width // n_tp

    def remote(src, dst, send, recv, device):
        return pltpu.make_async_remote_copy(
            src_ref=src,
            dst_ref=dst,
            send_sem=send,
            recv_sem=recv,
            device_id=device,
            device_id_type=MESH,
        )

    def worker_of(p):
        return 2 * p + 1 - p // (n_pairs // 2)

    def tp_peer(k):
        return lax.rem(t + k, n_tp)

    def tp_from(k):
        return lax.rem(t - k + n_tp, n_tp)

    def sp_peer(k):
        return lax.rem(s + k, n_sp)

    def sp_from(k):
        return lax.rem(s - k + n_sp, n_sp)

    weights = ((key_weight, wk), (value_weight, wv), (query_weight, wq))
    local = [pltpu.make_async_copy(modulator, mod_w, loc_sem.at[0])]
    for m, (source, slots) in enumerate(weights):
        for i in range(2):
            local.append(
                pltpu.make_async_copy(
                    source.at[pl.ds(i * half, half)], slots.at[s, i], loc_sem.at[1 + 2 * m + i]
                )
            )
    local.append(pltpu.make_async_copy(out_weight, wo, loc_sem.at[7]))
    barrier = pltpu.get_barrier_semaphore()
    for k in range(1, n_tp):
        pl.semaphore_signal(barrier, inc=1, device_id={"tp": tp_peer(k)}, device_id_type=MESH)
    for k in range(1, n_sp):
        pl.semaphore_signal(barrier, inc=1, device_id={"sp": sp_peer(k)}, device_id_type=MESH)
    pl.semaphore_signal(barrier, inc=1, device_id={"dp": mate}, device_id_type=MESH)
    small = [
        pltpu.make_async_copy(source, target, loc_sem.at[8 + i])
        for i, (source, target) in enumerate(
            (
                (sample_vector_in, sample_vector),
                (context_vector_in, context_vector),
                (latents_in, latents),
                (context_in, context),
                (decay_extra_in, decay_extra),
                (norm_gain_in, norm_gain),
                (decay_down_in, decay_down),
                (decay_up_in, decay_up),
                (decay_bias_in, decay_bias),
                (head_gain_in, head_gain),
            )
        )
    ]
    for copy in small[:5] + local[:1] + small[5:] + local[1:]:
        copy.start()
    small[2].wait()
    small[3].wait()
    small[4].wait()
    pl.semaphore_wait(barrier, n_tp + n_sp - 1)

    def inner():
        return jnp.logical_and(s >= 1, s <= n_sp - 2)

    def onward(r):
        return s + 1 <= n_sp - 2 if r == 0 else s - 1 >= 1

    def exists(r, j):
        return jnp.logical_and(inner(), s - j >= 0 if r == 0 else s + j < n_sp)

    def origin_of(r, j):
        return s - j if r == 0 else s + j

    def ring_copy(m, r, j, first=False):
        source, slots = weights[m]
        origin = origin_of(r, j)
        src = source.at[pl.ds(h * half, half)] if first else slots.at[origin, h]
        target = s + 1 if r == 0 else s - 1
        return remote(src, slots.at[origin, h], w_s.at[m, r, j], w_r.at[m, r, j], {"sp": target})

    def ring_arrival(m, r, j):
        view = weights[m][1].at[origin_of(r, j), h]
        return remote(view, view, w_s.at[m, r, j - 1], w_r.at[m, r, j - 1], {"sp": s})

    def mate_copy(m, r, j, side):
        view = weights[m][1].at[origin_of(r, j), side]
        return remote(view, view, p_s.at[m, r, j - 1], p_r.at[m, r, j - 1], {"dp": mate})

    def send_own(m):
        for r in range(2):

            @pl.when(onward(r))
            def _():
                ring_copy(m, r, 0, True).start()

    def relay(m, j, share):
        for r in range(2):

            @pl.when(exists(r, j))
            def _():
                ring_arrival(m, r, j).wait_recv()

                @pl.when(onward(r))
                def _():
                    ring_copy(m, r, j).start()

                if share:
                    mate_copy(m, r, j, h).start()

    def whole(slots, o):
        return slots[o].reshape(depth, slots.shape[3])

    def multiply(m, j, acc, count):
        slots = weights[m][1]
        for r in range(2):

            @pl.when(exists(r, j))
            def _():
                origin = origin_of(r, j)
                mate_copy(m, r, j, 1 - h).wait_recv()
                acc[...] += dot(hid[origin, 0:count], whole(slots, origin))

    def lat_copy(k):
        return remote(latents, lat.at[pos, t], lat_s.at[0, k], lat_r.at[0, k], {"tp": tp_peer(k)})

    def lat_arrival(k):
        view = lat.at[pos, tp_from(k)]
        return remote(view, view, lat_s.at[0, k], lat_r.at[0, k], {"tp": t})

    def outer_lat():
        return remote(latents, lat.at[pos, t], lo_s, lo_r, {"sp": partner})

    def outer_lat_arrival():
        view = lat.at[1 - pos, t]
        return remote(view, view, lo_s, lo_r, {"sp": s})

    def lat_relay(k, owner, to):
        view = lat.at[1 - pos, owner]
        return remote(view, view, lat_s.at[1, k], lat_r.at[1, k], {"tp": to})

    def ctx_cols(owner):
        return pl.ds(pl.multiple_of(owner * span_t, span_t), span_t)

    def ctx_copy():
        return remote(
            context.at[:, ctx_cols(t)],
            outer_context.at[:, ctx_cols(t)],
            cx_s.at[0],
            cx_r.at[0],
            {"sp": partner},
        )

    def ctx_relay(k, owner, to):
        view = outer_context.at[:, ctx_cols(owner)]
        return remote(view, view, cx_s.at[k], cx_r.at[k], {"tp": to})

    def extra_copy():
        return remote(decay_extra, extras.at[pos], up_s, up_r, {"sp": partner})

    def extra_arrival():
        view = extras.at[1 - pos]
        return remote(view, view, up_s, up_r, {"sp": s})

    @pl.when(is_outer)
    def _():
        outer_lat().start()
        extra_copy().start()
        ctx_copy().start()
        for m in range(3):
            send_own(m)

    @pl.when(is_worker)
    def _():
        for k in range(1, n_tp):
            lat_copy(k).start()
        send_own(0)
        send_own(1)

    small[0].wait()
    small[1].wait()
    is_first = lax.broadcasted_iota(jnp.int32, (16, width), 0) == 0
    vectors = jnp.where(is_first, sample_vector[...], context_vector[...])
    conditions = (vectors / (1.0 + jnp.exp(-vectors))).astype(BF16)
    local[0].wait()
    mods[me] = dot(conditions, mod_w[...])[0:2]

    def mod_tp(k, owner, to):
        view = mods.at[s * n_tp + owner]
        return remote(view, view, mt_s.at[k], mt_r.at[k], {"tp": to})

    def mod_sp(k, owner, to):
        view = mods.at[pl.ds(owner * n_tp, n_tp)]
        return remote(view, view, ms_s.at[k], ms_r.at[k], {"sp": to})

    for k in range(1, n_tp):
        mod_tp(k, t, tp_peer(k)).start()
    for k in range(1, n_tp):
        mod_tp(k, tp_from(k), t).wait_recv()
    for k in range(1, n_sp):
        mod_sp(k, s, sp_peer(k)).start()
    for copy in small[5:]:
        copy.wait()

    def modulation_now():
        for k in range(1, n_sp):
            mod_sp(k, sp_from(k), s).wait_recv()

    def mod_part(i):
        return jnp.concatenate([mods[j] for j in range(n_dev)], axis=1)[
            :, i * width : (i + 1) * width
        ]

    def tot_copy(k, owner, to):
        view = tots.at[owner]
        return remote(view, view, tt_s.at[k], tt_r.at[k], {"sp": to})

    def has_pred(z):
        return pair > 0 if z == 0 else pair < n_pairs - 1

    def has_succ(z):
        return pair < n_pairs - 1 if z == 0 else pair > 0

    def lone(a, b):
        return jnp.logical_and(a, jnp.logical_not(b))

    def f_copy(z, g):
        to = worker_of(pair + 1) if z == 0 else worker_of(pair - 1)
        return remote(f_out.at[z, g], f_in.at[z, g], f_s.at[z, g], f_r.at[z, g], {"sp": to})

    def g_copy(z, g):
        to = worker_of(pair - 1) if z == 0 else worker_of(pair + 1)
        return remote(g_out.at[z, g], g_in.at[z, g], g_s.at[z, g], g_r.at[z, g], {"sp": to})

    def o_copy(g, where, to):
        view = normed.at[where, g]
        return remote(view, view, o_s.at[g], o_r.at[g], {"sp": to})

    def work():
        outer_lat_arrival().wait_recv()
        for k in range(1, n_tp):
            lat_relay(k, t, tp_peer(k)).start()
        remote(
            outer_context.at[:, ctx_cols(t)],
            outer_context.at[:, ctx_cols(t)],
            cx_s.at[0],
            cx_r.at[0],
            {"sp": s},
        ).wait_recv()
        for k in range(1, n_tp):
            ctx_relay(k, t, tp_peer(k)).start()
        relay(0, 1, True)
        send_own(2)

        lat[pos, t] = latents[...]
        for k in range(1, n_tp):
            lat_arrival(k).wait_recv()
        modulation_now()
        shift = mod_part(0)
        scale = mod_part(1)

        def modulated(x, row):
            x = x.astype(F32)
            x = x * lax.rsqrt(jnp.mean(x * x, axis=-1, keepdims=True) + EPS) * norm_gain[...]
            return (x * (1.0 + scale[row : row + 1]) + shift[row : row + 1]).astype(BF16)

        piece = min(32, ctx_rows)

        def put(x, at):
            count = x.shape[0]
            at = pl.multiple_of(at, piece)
            for o in range(n_sp):
                hid[o, pl.ds(at, count)] = x[:, o * depth : (o + 1) * depth]

        for i in range(n_tp):
            put(modulated(lat[pos, i], 0), pos * length + i * rows)
        for i in range(ctx_rows // piece):
            put(
                modulated(context[i * piece : (i + 1) * piece], 1),
                lat_all + pos * ctx_rows + i * piece,
            )
        for k in range(1, n_tp):
            lat_relay(k, tp_from(k), t).wait_recv()
        relay(1, 1, True)
        for i in range(n_tp):
            put(modulated(lat[1 - pos, i], 0), (1 - pos) * length + i * rows)
        for k in range(1, n_tp):
            ctx_relay(k, tp_from(k), t).wait_recv()
        for i in range(ctx_rows // piece):
            put(
                modulated(outer_context[i * piece : (i + 1) * piece], 1),
                lat_all + (1 - pos) * ctx_rows + i * piece,
            )

        low = dot_nt(hid[0], decay_down[:, 0:depth])
        for o in range(1, n_sp):
            low = low + dot_nt(hid[o], decay_down[:, o * depth : (o + 1) * depth])
        low = low.astype(BF16)
        relay(2, 1, True)

        def log_decays(z):
            x = dot(low[:, z * rank : (z + 1) * rank], decay_up[z]) + decay_bias[z : z + 1]
            return log_sigmoid(x) / SHARP

        row_id = lax.broadcasted_iota(jnp.int32, (lat_all, lat_all), 0)
        col_id = lax.broadcasted_iota(jnp.int32, (lat_all, lat_all), 1)
        same = row_id // BLOCK == col_id // BLOCK
        within_mask = [same & (col_id <= row_id), same & (col_id >= row_id)]
        extras[pos] = decay_extra[...]
        extra_arrival().wait_recv()

        def extra_sums(z):
            columns = []
            for g in range(heads):
                line = jnp.concatenate([extras[i, z, g : g + 1, :] for i in range(2)], axis=1)
                columns.append(
                    jnp.sum(jnp.where(within_mask[z], line, 0.0), axis=1, keepdims=True)
                )
            return jnp.concatenate([jnp.broadcast_to(c, (lat_all, DK)) for c in columns], axis=1)

        decays = [log_decays(z) for z in range(2)]
        within = [sums(within_mask[z], decays[z][:lat_all]) + extra_sums(z) for z in range(2)]
        blocks = lat_all // BLOCK
        totals = [
            [within[0][(b + 1) * BLOCK - 1 : (b + 1) * BLOCK] for b in range(blocks)],
            [within[1][b * BLOCK : b * BLOCK + 1] for b in range(blocks)],
        ]
        none = jnp.zeros_like(totals[0][0])

        def between(z, lo, hi):
            value = none
            for b in range(lo, hi):
                value = value + totals[z][b]
            return value

        crow = lax.broadcasted_iota(jnp.int32, (total - lat_all, total - lat_all), 0)
        ccol = lax.broadcasted_iota(jnp.int32, (total - lat_all, total - lat_all), 1)
        after = [
            sums(ccol > crow, decays[0][lat_all:]),
            sums(ccol < crow, decays[1][lat_all:]),
        ]
        lat_total = [between(z, 0, blocks) for z in range(2)]
        ctx_total = [
            after[0][0:1] + decays[0][lat_all : lat_all + 1],
            after[1][total - lat_all - 1 :] + decays[1][total - 1 :],
        ]
        tots[pair] = jnp.concatenate(lat_total + ctx_total, axis=0)
        for k in range(1, n_pairs):
            to = lax.rem(pair + k, n_pairs)
            tot_copy(k, pair, worker_of(to)).start()

        for copy in local[1:5]:
            copy.wait()
        acc_k[...] = dot(hid[s], whole(wk, s))
        acc_v[...] = dot(hid[s], whole(wv, s))
        multiply(0, 1, acc_k, total)
        multiply(1, 1, acc_v, total)
        for k in range(1, n_pairs):
            tot_copy(k, lax.rem(pair - k + n_pairs, n_pairs), s).wait_recv()
        before = [none, none]
        suffix = [none, none]
        for u in range(n_pairs):
            line = tots[u]
            below = jnp.where(u < pair, 1.0, 0.0)
            above = jnp.where(u > pair, 1.0, 0.0)
            before[0] = before[0] + below * line[0:1]
            before[1] = before[1] + above * line[1:2]
            suffix[0] = suffix[0] + above * line[2:3]
            suffix[1] = suffix[1] + below * line[3:4]
        ctx_weight = [jnp.exp(after[z] + suffix[z]) for z in range(2)]

        def per_block(f):
            return jnp.concatenate([f(b) for b in range(blocks)], axis=0)

        def rows_of(x, b):
            return x[b * BLOCK : (b + 1) * BLOCK]

        ending = [
            jnp.exp(
                per_block(
                    lambda b: totals[0][b] - rows_of(within[0], b) + between(0, b + 1, blocks)
                )
            ),
            jnp.exp(per_block(lambda b: totals[1][b] - rows_of(within[1], b) + between(1, 0, b))),
        ]
        for j in range(2, max(n_sp - 1, 2)):
            relay(0, j, True)
            multiply(0, j, acc_k, total)
            relay(1, j, True)
            multiply(1, j, acc_v, total)
        keys = acc_k[...].astype(BF16)
        values = acc_v[...].astype(BF16)
        ckeys = keys[lat_all:].astype(F32)
        cvals = values[lat_all:]
        keys = keys[:lat_all].astype(F32)
        values = values[:lat_all]

        def columns(g, n):
            return slice(g * n, (g + 1) * n)

        for z in range(2):
            ended = (keys * ending[z]).astype(BF16)
            cended = (ckeys * ctx_weight[z]).astype(BF16)
            lift = CTX_LIFT * jnp.exp(before[z])
            lift_on = CTX_LIFT * jnp.exp(before[z] + lat_total[z])
            for g in range(heads):
                c = dot_tn(cvals[:, columns(g, dv)], cended[:, columns(g, DK)])
                g_out[z, g] = c.astype(BF16)
                own = dot_tn(values[:, columns(g, dv)], ended[:, columns(g, DK)])
                f_out[z, g] = (own + lift_on[:, columns(g, DK)] * c).astype(BF16)
                if n_pairs > 2:
                    c_state[z, g] = c
                    l_state[z, g] = own + lift_on[:, columns(g, DK)] * c
                state[z, g] = lift[:, columns(g, DK)] * c

                @pl.when(lone(has_succ(z), has_pred(z)))
                def _():
                    f_copy(z, g).start()

                @pl.when(lone(has_pred(z), has_succ(z)))
                def _():
                    g_copy(z, g).start()

        if n_pairs > 2:
            for z in range(2):

                @pl.when(jnp.logical_and(has_pred(z), has_succ(z)))
                def _():
                    for g in range(heads):
                        f_copy(z, g).wait_recv()
                        on = jnp.exp(lat_total[z])[:, columns(g, DK)]
                        f_out[z, g] = (l_state[z, g] + on * f_in[z, g].astype(F32)).astype(BF16)
                        f_copy(z, g).start()

                @pl.when(jnp.logical_and(has_pred(z), has_succ(z)))
                def _():
                    for g in range(heads):
                        g_copy(z, g).wait_recv()
                        g_out[z, g] = (c_state[z, g] + g_in[z, g].astype(F32)).astype(BF16)
                        g_copy(z, g).start()

        for z in range(2):
            close = (keys * jnp.exp(-within[z])).astype(BF16)
            near = keys * jnp.exp(per_block(lambda b: totals[z][b] - rows_of(within[z], b)))
            for i in range(blocks):
                for j in range(blocks):
                    if i == j:
                        block = rows_of(close, j)
                    elif (j < i) == (z == 0):
                        gap = between(z, min(i, j) + 1, max(i, j))
                        block = (rows_of(near, j) * jnp.exp(gap)).astype(BF16)
                    else:
                        block = jnp.zeros((BLOCK, heads * DK), BF16)
                    key_rows[z, i, j * BLOCK : (j + 1) * BLOCK] = block
        reach = [jnp.exp(within[z]) for z in range(2)]
        lifted_by = [
            jnp.exp(per_block(lambda b: rows_of(within[0], b) + between(0, 0, b))),
            jnp.exp(per_block(lambda b: rows_of(within[1], b) + between(1, b + 1, blocks))),
        ]

        for copy in local[5:7]:
            copy.wait()
        acc_q[...] = dot(hid[s, 0:lat_all], whole(wq, s))
        for j in range(1, max(n_sp - 1, 2)):
            if j > 1:
                relay(2, j, True)
            multiply(2, j, acc_q, lat_all)
        queries = acc_q[...].astype(BF16).astype(F32)

        for z in range(2):
            near_rows = (queries * reach[z]).astype(BF16)
            far_rows = (queries * lifted_by[z]).astype(BF16)
            for b in range(blocks):
                query_rows[0, z, b] = rows_of(near_rows, b)
                query_rows[1, z, b] = rows_of(far_rows, b)
        turn = blocks // 2
        row_in = lax.broadcasted_iota(jnp.int32, (BLOCK, lat_all), 0)
        col_in = lax.broadcasted_iota(jnp.int32, (BLOCK, lat_all), 1)

        def inside(where, g):
            lines = []
            for b in range(turn):
                i = where * turn + b
                ids = row_in + i * BLOCK
                masks = [col_in <= ids, col_in >= ids]
                line = 0.0
                for z in range(2):
                    score = dot_nt(
                        query_rows[0, z, i, :, columns(g, DK)], key_rows[z, i, :, columns(g, DK)]
                    )
                    line = line + jnp.where(masks[z], score, 0.0)
                lines.append(line.astype(BF16))
            return dot(jnp.concatenate(lines, axis=0), values[:, columns(g, dv)])

        def finish(where, g, mixed):
            for z in range(2):
                rows_z = query_rows[1, z, pl.ds(where * turn, turn), :, columns(g, DK)]
                mixed = mixed + dot_nt(rows_z.reshape(length, DK), state[z, g].astype(BF16))
            by = lax.rsqrt(jnp.mean(mixed * mixed, axis=-1, keepdims=True) + EPS)
            normed[where, g] = (mixed * by * head_gain[...]).astype(BF16)

        first = [inside(1 - pos, g) for g in range(heads)]
        for z in range(2):
            lift = CTX_LIFT * jnp.exp(before[z])

            @pl.when(has_pred(z))
            def _():
                for g in range(heads):
                    if n_pairs == 2:
                        f_copy(z, g).wait_recv()
                    else:

                        @pl.when(jnp.logical_not(has_succ(z)))
                        def _():
                            f_copy(z, g).wait_recv()

                    state[z, g] += f_in[z, g].astype(F32)

            @pl.when(has_succ(z))
            def _():
                for g in range(heads):
                    if n_pairs == 2:
                        g_copy(z, g).wait_recv()
                    else:

                        @pl.when(jnp.logical_not(has_pred(z)))
                        def _():
                            g_copy(z, g).wait_recv()

                    state[z, g] += lift[:, columns(g, DK)] * g_in[z, g].astype(F32)

        for g in range(heads):
            finish(1 - pos, g, first[g])
            o_copy(g, 1 - pos, partner).start()
        for g in range(heads):
            finish(pos, g, inside(pos, g))

    pl.when(is_worker)(work)

    @pl.when(is_outer)
    def _():
        for copy in local[1:7]:
            copy.wait()
        for m in range(3):
            relay(m, 1, False)
        for j in range(2, n_sp - 1):
            relay(0, j, False)
            relay(1, j, False)
        for j in range(2, n_sp - 1):
            relay(2, j, False)
        modulation_now()
        for g in range(heads):
            o_copy(g, pos, s).wait_recv()

    gate = mod_part(2)[0:1]
    local[7].wait()
    chunks = rs_s.shape[1]
    span = width // chunks
    rs_copies = []
    for c in range(chunks):
        cols = slice(c * span, (c + 1) * span)
        product = dot(normed[pos, 0], wo[0:dv, cols])
        for g in range(1, heads):
            product = product + dot(normed[pos, g], wo[g * dv : (g + 1) * dv, cols])
        product = product.astype(BF16)
        for i in range(n_tp):
            part[i, :, cols] = product[i * rows : (i + 1) * rows]
        for k in range(1, n_tp):
            to = tp_peer(k)
            copy = remote(
                part.at[to, :, pl.ds(c * span, span)],
                rs.at[k, :, pl.ds(c * span, span)],
                rs_s.at[k, c],
                rs_r.at[k, c],
                {"tp": to},
            )
            copy.start()
            rs_copies.append(copy)
    for c in range(chunks):
        cols = slice(c * span, (c + 1) * span)
        summed = part[t, :, cols].astype(F32)
        for k in range(1, n_tp):
            rs_copies[c * (n_tp - 1) + k - 1].wait_recv()
            summed = summed + rs[k, :, cols].astype(F32)
        projected = summed.astype(BF16).astype(F32)
        out[:, cols] = (latents[:, cols].astype(F32) + gate[:, cols] * projected).astype(BF16)

    for copy in rs_copies:
        copy.wait_send()
    for k in range(1, n_tp):
        mod_tp(k, t, tp_peer(k)).wait_send()
    for k in range(1, n_sp):
        mod_sp(k, s, sp_peer(k)).wait_send()

    @pl.when(is_outer)
    def _():
        outer_lat().wait_send()
        extra_copy().wait_send()
        ctx_copy().wait_send()

    @pl.when(is_worker)
    def _():
        for k in range(1, n_tp):
            lat_copy(k).wait_send()
            lat_relay(k, t, tp_peer(k)).wait_send()
            ctx_relay(k, t, tp_peer(k)).wait_send()
        for k in range(1, n_pairs):
            tot_copy(k, pair, s).wait_send()
        for g in range(heads):
            o_copy(g, 1 - pos, partner).wait_send()
            for z in range(2):

                @pl.when(has_succ(z))
                def _():
                    f_copy(z, g).wait_send()

                @pl.when(has_pred(z))
                def _():
                    g_copy(z, g).wait_send()

    for m in range(3):
        for r in range(2):

            @pl.when(onward(r))
            def _():
                ring_copy(m, r, 0, True).wait_send()

            for j in range(1, n_sp - 1):

                @pl.when(exists(r, j))
                def _():
                    @pl.when(onward(r))
                    def _():
                        ring_copy(m, r, j).wait_send()

                    @pl.when(is_worker)
                    def _():
                        mate_copy(m, r, j, h).wait_send()


def chain_per_device(n_sp, n_tp, *args):
    (latents, sv, context, cv, gain, modulator, wq, wk, wv, down, up, bias, extra, hg, wo) = args
    rows, width = latents.shape
    ctx_rows = context.shape[0]
    n_dev = n_sp * n_tp
    n_pairs = n_sp // 2
    length = rows * n_tp
    total = 2 * (length + ctx_rows)
    depth = wq.shape[0]
    kw, vw = wk.shape[1], wv.shape[1]
    heads = bias.shape[1] // DK
    dv = hg.shape[0]
    chunks = 4
    vmem = pl.BlockSpec(memory_space=pltpu.VMEM)
    hbm = pl.BlockSpec(memory_space=pl.ANY)
    dma = pltpu.SemaphoreType.DMA
    states = (2, heads, dv, DK)
    chained = states if n_pairs > 2 else (2, heads, 8, DK)
    scratch = [
        pltpu.VMEM(latents.shape, BF16),
        pltpu.VMEM(sv.shape, F32),
        pltpu.VMEM(context.shape, BF16),
        pltpu.VMEM(cv.shape, F32),
        pltpu.VMEM((1, width), F32),
        pltpu.VMEM(down.shape[::-1], BF16),
        pltpu.VMEM(up.shape, BF16),
        pltpu.VMEM(bias.shape, F32),
        pltpu.VMEM((2, heads, length), F32),
        pltpu.VMEM((1, dv), F32),
        pltpu.VMEM(modulator.shape, BF16),
        pltpu.VMEM((n_dev, 2, modulator.shape[1]), F32),
        pltpu.VMEM((2, n_tp, rows, width), BF16),
        pltpu.VMEM((ctx_rows, width), BF16),
        pltpu.VMEM((2, 2, heads, length), F32),
        pltpu.VMEM((n_sp, total, depth), BF16),
        pltpu.VMEM((n_sp, 2, depth // 2, kw), BF16),
        pltpu.VMEM((n_sp, 2, depth // 2, vw), BF16),
        pltpu.VMEM((n_sp, 2, depth // 2, kw), BF16),
        pltpu.VMEM(wo.shape, BF16),
        pltpu.VMEM((total, kw), F32),
        pltpu.VMEM((total, vw), F32),
        pltpu.VMEM((2 * length, kw), F32),
        pltpu.VMEM((n_pairs, 4, kw), F32),
        pltpu.VMEM((2, 2 * length // BLOCK, 2 * length, kw), BF16),
        pltpu.VMEM((2, 2, 2 * length // BLOCK, BLOCK, kw), BF16),
        pltpu.VMEM(chained, F32),
        pltpu.VMEM(chained, F32),
        pltpu.VMEM(states, BF16),
        pltpu.VMEM(states, BF16),
        pltpu.VMEM(states, BF16),
        pltpu.VMEM(states, BF16),
        pltpu.VMEM(states, F32),
        pltpu.VMEM((2, heads, length, dv), BF16),
        pltpu.VMEM((n_tp, rows, width), BF16),
        pltpu.VMEM((n_tp, rows, width), BF16),
        dma((18,)),
        dma((n_tp,)),
        dma((n_tp,)),
        dma((n_sp,)),
        dma((n_sp,)),
        dma((2, n_tp)),
        dma((2, n_tp)),
        dma,
        dma,
        dma((n_tp,)),
        dma((n_tp,)),
        dma,
        dma,
        dma((3, 2, n_sp)),
        dma((3, 2, n_sp)),
        dma((3, 2, n_sp)),
        dma((3, 2, n_sp)),
        dma((n_pairs,)),
        dma((n_pairs,)),
        dma((2, heads)),
        dma((2, heads)),
        dma((2, heads)),
        dma((2, heads)),
        dma((heads,)),
        dma((heads,)),
        dma((n_tp, chunks)),
        dma((n_tp, chunks)),
    ]
    return pl.pallas_call(
        functools.partial(chain_kernel, n_sp, n_tp),
        out_shape=jax.ShapeDtypeStruct(latents.shape, BF16),
        in_specs=[hbm] * 15,
        out_specs=vmem,
        scratch_shapes=scratch,
        compiler_params=pltpu.CompilerParams(
            collective_id=0, has_side_effects=True, vmem_limit_bytes=56 * 1024 * 1024
        ),
    )(
        latents,
        sv,
        context,
        cv,
        gain.reshape(1, -1),
        modulator,
        wq,
        wk,
        wv,
        down.T,
        up,
        bias,
        extra.transpose(0, 2, 1),
        hg.reshape(1, -1),
        wo,
    )


def kernel(
    n_sp,
    n_tp,
    latents_in,
    sample_vector_in,
    context_in,
    context_vector_in,
    norm_gain_in,
    modulator,
    query_weight,
    key_weight,
    value_weight,
    decay_down_in,
    decay_up_in,
    decay_bias_in,
    decay_extra_in,
    head_gain_in,
    out_weight,
    out,
    latents,
    sample_vector,
    context,
    context_vector,
    norm_gain,
    decay_down,
    decay_up,
    decay_bias,
    decay_extra,
    head_gain,
    mod_w,
    mods,
    lat,
    ctx,
    extras,
    hid,
    wk,
    wv,
    wq,
    wo,
    acc_k,
    acc_v,
    acc_q,
    key_rows,
    o_out,
    normed,
    duo,
    wo_twist,
    kept,
    part,
    rs,
    loc_sem,
    mt_s,
    mt_r,
    ms_s,
    ms_r,
    lo_s,
    lo_r,
    cx_s,
    cx_r,
    ex_s,
    ex_r,
    em_s,
    em_r,
    lp_s,
    lp_r,
    cp_s,
    cp_r,
    hd_s,
    hd_r,
    w_s,
    w_r,
    o_s,
    o_r,
    wx_s,
    wx_r,
    wm_s,
    wm_r,
    rs_s,
    rs_r,
    vouch,
):
    s = lax.axis_index("sp")
    t = lax.axis_index("tp")
    d = lax.axis_index("dp")
    h = lax.rem(d, 2)
    mate = d + 1 - 2 * h
    n_dev = n_sp * n_tp
    me = s * n_tp + t
    first_plane = n_sp // 2 - 1
    last_plane = n_sp // 2
    side = s - first_plane
    target = first_plane + h
    is_worker = jnp.logical_and(s >= first_plane, s <= last_plane)
    is_leader = s == target
    is_follower = jnp.logical_and(is_worker, s != target)
    is_sender = s != target
    rows, width = latents.shape
    ctx_rows = context.shape[0]
    length = rows * n_tp
    lat_all = n_sp * length
    total = hid.shape[1]
    depth = hid.shape[2]
    heads = decay_bias.shape[1] // DK
    dv = head_gain.shape[1]
    rank = decay_up.shape[1]
    span_t = width // n_tp

    def remote(src, dst, send, recv, device):
        return pltpu.make_async_remote_copy(
            src_ref=src,
            dst_ref=dst,
            send_sem=send,
            recv_sem=recv,
            device_id=device,
            device_id_type=MESH,
        )

    def tp_peer(k):
        return lax.rem(t + k, n_tp)

    def tp_from(k):
        return lax.rem(t - k + n_tp, n_tp)

    def sp_peer(k):
        return lax.rem(s + k, n_sp)

    def sp_from(k):
        return lax.rem(s - k + n_sp, n_sp)

    def head_cols(size):
        return pl.ds(pl.multiple_of(h * size, DK), size)

    weights = ((key_weight, wk, DK), (value_weight, wv, dv), (query_weight, wq, DK))
    own_weight = [
        pltpu.make_async_copy(source.at[:, head_cols(size)], slots.at[s], loc_sem.at[1 + m])
        for m, (source, slots, size) in enumerate(weights)
    ]
    mod_load = pltpu.make_async_copy(modulator, mod_w, loc_sem.at[0])
    out_load = pltpu.make_async_copy(out_weight, wo, loc_sem.at[4])
    barrier = pltpu.get_barrier_semaphore()

    def signal(semaphore, device):
        pl.semaphore_signal(semaphore, inc=1, device_id=device, device_id_type=MESH)

    above = s + 1 < n_sp
    below = s > 0
    twist = t + 1 - 2 * lax.rem(t, 2)
    cross = lax.rem(t + 2, n_tp)
    signal(barrier, {"tp": twist})
    signal(barrier, {"tp": cross})
    signal(barrier, {"dp": mate})

    @pl.when(above)
    def _():
        signal(barrier, {"sp": s + 1})

    @pl.when(below)
    def _():
        signal(barrier, {"sp": s - 1})

    small = [
        pltpu.make_async_copy(source, where, loc_sem.at[8 + i])
        for i, (source, where) in enumerate(
            (
                (sample_vector_in, sample_vector),
                (context_vector_in, context_vector),
                (latents_in, latents),
                (context_in, context),
                (decay_extra_in, decay_extra),
                (norm_gain_in, norm_gain),
                (decay_down_in, decay_down),
                (decay_up_in, decay_up),
                (decay_bias_in, decay_bias),
                (head_gain_in, head_gain),
            )
        )
    ]
    for copy in small[:5] + own_weight + [mod_load] + small[5:] + [out_load]:
        copy.start()
    for copy in small[2:5] + own_weight:
        copy.wait()
    pl.semaphore_wait(barrier, 3 + jnp.where(above, 1, 0) + jnp.where(below, 1, 0))
    signal(vouch.at[n_sp], {"tp": twist})

    def pass_word(step):
        @pl.when(jnp.logical_and(below, s + step < n_sp))
        def _():
            signal(vouch.at[step], {"sp": s - 1})

        @pl.when(jnp.logical_and(above, s - step >= 0))
        def _():
            signal(vouch.at[0 if step == 1 else n_sp - 1], {"sp": s + 1})

    def hear_word(step):
        @pl.when(s + step + 1 < n_sp)
        def _():
            pl.semaphore_wait(vouch.at[step], 1)

        @pl.when(s - step - 1 >= 0)
        def _():
            pl.semaphore_wait(vouch.at[0 if step == 1 else n_sp - 1], 1)

    pass_word(1)

    def onward(r):
        return s + 1 <= last_plane if r == 0 else s - 1 >= first_plane

    def exists(r, j):
        if r == 0:
            return jnp.logical_and(s <= last_plane, s - j >= 0)
        return jnp.logical_and(s >= first_plane, s + j < n_sp)

    def origin_of(r, j):
        return s - j if r == 0 else s + j

    def ring_copy(m, r, j):
        view = weights[m][1].at[origin_of(r, j)]
        to = s + 1 if r == 0 else s - 1
        return remote(view, view, w_s.at[m, r, j], w_r.at[m, r, j], {"sp": to})

    def ring_arrival(m, r, j):
        view = weights[m][1].at[origin_of(r, j)]
        return remote(view, view, w_s.at[m, r, j - 1], w_r.at[m, r, j - 1], {"sp": s})

    def relay(m, j):
        for r in range(2):

            @pl.when(exists(r, j))
            def _():
                ring_arrival(m, r, j).wait_recv()

                @pl.when(onward(r))
                def _():
                    ring_copy(m, r, j).start()

    def multiply(m, j, acc, count):
        slots = weights[m][1]
        for r in range(2):

            @pl.when(exists(r, j))
            def _():
                origin = origin_of(r, j)
                acc[...] += dot(hid[origin, 0:count], slots[origin])

    def lat_in(b, to):
        view = lat.at[b, t]
        return remote(latents, view, lo_s, lo_r.at[b], {"sp": to})

    def extra_in(b, to):
        return remote(decay_extra, extras.at[b], ex_s, ex_r.at[b], {"sp": to})

    def ctx_cols(owner):
        return pl.ds(pl.multiple_of(owner * span_t, span_t), span_t)

    def ctx_in(b, to):
        return remote(
            context.at[:, ctx_cols(t)],
            ctx.at[b, :, ctx_cols(t)],
            cx_s,
            cx_r.at[b],
            {"sp": to},
        )

    def lat_plane(b, k, owner, to):
        view = lat.at[b, owner]
        return remote(view, view, lp_s.at[b, k], lp_r.at[b, k], {"tp": to})

    def lat_own(k):
        return remote(latents, lat.at[s, t], lp_s.at[s, k], lp_r.at[s, k], {"tp": tp_peer(k)})

    def ctx_plane(b, k, owner, to):
        view = ctx.at[b, :, ctx_cols(owner)]
        return remote(view, view, cp_s.at[b, k], cp_r.at[b, k], {"tp": to})

    def hid_copy(i, at, count):
        view = hid.at[:, pl.ds(pl.multiple_of(at, 16), count)]
        return remote(view, view, hd_s.at[i], hd_r.at[i], {"dp": mate})

    def lat_hid(b):
        return hid_copy(b, b * length, length)

    def ctx_hid(b):
        return hid_copy(n_sp + b, lat_all + b * ctx_rows, ctx_rows)

    def extra_mate():
        return remote(extras, extras, em_s, em_r, {"dp": mate})

    def others():
        towards = 1 - 2 * side
        steps = sorted(range(-first_plane, n_sp // 2 + 1), key=abs)
        return [s + towards * step for step in steps if step]

    adjacent = jnp.logical_or(s == target + 1, s == target - 1)

    def send_rows():
        lat_in(s, target).start()
        extra_in(s, target).start()
        ctx_in(s, target).start()

    def send_weight(m):
        for r in range(2):

            @pl.when(onward(r))
            def _():
                ring_copy(m, r, 0).start()

    pl.when(adjacent)(send_rows)

    @pl.when(is_leader)
    def _():
        for k in (1, 2, 3):

            @pl.when(tp_peer(k) != lax.rem(twist + 2, n_tp))
            def _():
                lat_own(k).start()

    send_weight(0)
    hear_word(1)
    pl.semaphore_wait(vouch.at[n_sp], 1)
    pl.when(jnp.logical_and(is_sender, jnp.logical_not(adjacent)))(send_rows)

    @pl.when(is_leader)
    def _():
        for k in (1, 2, 3):

            @pl.when(tp_peer(k) == lax.rem(twist + 2, n_tp))
            def _():
                lat_own(k).start()

    send_weight(1)
    send_weight(2)

    small[0].wait()
    small[1].wait()
    is_first = lax.broadcasted_iota(jnp.int32, (16, width), 0) == 0
    vectors = jnp.where(is_first, sample_vector[...], context_vector[...])
    conditions = (vectors / (1.0 + jnp.exp(-vectors))).astype(BF16)
    mod_load.wait()
    mods[me] = dot(conditions, mod_w[...])[0:2]

    def mod_tp(k, owner, to):
        view = mods.at[s * n_tp + owner]
        return remote(view, view, mt_s.at[k], mt_r.at[k], {"tp": to})

    def mod_sp(k, owner, to):
        view = mods.at[pl.ds(owner * n_tp, n_tp)]
        return remote(view, view, ms_s.at[k], ms_r.at[owner], {"sp": to})

    low_side = s <= first_plane
    partner = s + 1 - 2 * lax.rem(s, 2)
    over = jnp.where(low_side, last_plane, first_plane)
    beyond = jnp.where(low_side, last_plane, 0)
    mod_direct = [mod_sp(0, s, partner), mod_sp(1, s, over)]
    mod_passed = [mod_sp(2 + i, beyond + i, partner) for i in range(2)]

    for k in range(1, n_tp):
        mod_tp(k, t, tp_peer(k)).start()
    for k in range(1, n_tp):
        mod_tp(k, tp_from(k), t).wait_recv()
    for copy in mod_direct:
        copy.start()
    for copy in small[5:]:
        copy.wait()

    def mod_part(i):
        return jnp.concatenate([mods[j] for j in range(n_dev)], axis=1)[
            :, i * width : (i + 1) * width
        ]

    def mods_arrive():
        for k in range(1, n_sp):
            mod_sp(k, sp_from(k), s).wait_recv()

        @pl.when(is_worker)
        def _():
            for copy in mod_passed:
                copy.start()

    piece = min(32, ctx_rows)

    def put(x, row, at):
        count = x.shape[0]
        x = x.astype(F32)
        x = x * lax.rsqrt(jnp.mean(x * x, axis=-1, keepdims=True) + EPS) * norm_gain[...]
        scale = mod_part(1)[row : row + 1]
        shift = mod_part(0)[row : row + 1]
        x = (x * (1.0 + scale) + shift).astype(BF16)
        at = pl.multiple_of(at, piece)
        for o in range(n_sp):
            hid[o, pl.ds(at, count)] = x[:, o * depth : (o + 1) * depth]

    lead = jnp.where(side == h, d, mate)
    parity = lax.rem(t, 2)
    two = n_tp // 2

    def inside(b):
        return first_plane <= b <= last_plane

    def o_copies(b):
        if inside(b):
            to = {"sp": b, "dp": lead}
            return [remote(o_out.at[b], normed.at[h], o_s.at[b, 0], o_r.at[0, h], to)]
        return [
            remote(
                o_out.at[b, pl.ds(two * rank_of, two)],
                duo.at[group, h],
                o_s.at[b, group],
                o_r.at[group, h],
                {"sp": b, "tp": to, "dp": lead},
            )
            for group, (rank_of, to) in enumerate(((parity, t), (1 - parity, twist)))
        ]

    def o_mate():
        return remote(o_out.at[s], normed.at[h], o_s.at[s, 0], o_r.at[0, h], {"dp": mate})

    def o_arrival(c):
        return remote(normed.at[c], normed.at[c], o_s.at[s, 0], o_r.at[0, c], {"dp": mate})

    def duo_arrival(group, c):
        view = duo.at[group, c]
        return remote(view, view, o_s.at[s, 0], o_r.at[group, c], {"dp": mate})

    half_rows = wo.shape[0] // 2

    def wo_half(where, side_of):
        return where.at[pl.ds(pl.multiple_of(side_of * half_rows, half_rows), half_rows)]

    def wo_cross():
        return remote(wo_half(wo, h), wo_half(wo_twist, h), wx_s, wx_r, {"tp": twist})

    def wo_mate(side_of):
        view = wo_half(wo_twist, side_of)
        return remote(view, view, wm_s, wm_r, {"dp": mate})

    def work():
        blocks = lat_all // BLOCK
        per = length // BLOCK

        @pl.when(is_leader)
        def _():
            for b in others():
                remote(lat.at[b, t], lat.at[b, t], lo_s, lo_r.at[b], {"sp": s}).wait_recv()
                for k in range(1, n_tp):
                    lat_plane(b, k, t, tp_peer(k)).start()
            for b in others():
                view = ctx.at[b, :, ctx_cols(t)]
                remote(view, view, cx_s, cx_r.at[b], {"sp": s}).wait_recv()
                for k in range(1, n_tp):
                    ctx_plane(b, k, t, tp_peer(k)).start()
            lat[s, t] = latents[...]
            mods_arrive()
            for i, b in enumerate([s] + others()):
                for k in range(1, n_tp):
                    lat_plane(b, k, tp_from(k), t).wait_recv()
                for u in range(n_tp):
                    put(lat[b, u], 0, b * length + u * rows)
                lat_hid(b).start()
                if i == 0:
                    relay(0, 1)
                    extras[s] = decay_extra[...]
                    for c in others():
                        remote(
                            extras.at[c], extras.at[c], ex_s, ex_r.at[c], {"sp": s}
                        ).wait_recv()
                    extra_mate().start()
                if i == 2:
                    relay(1, 1)

        @pl.when(is_follower)
        def _():
            relay(0, 1)
            relay(1, 1)
            mods_arrive()
            extra_mate().wait_recv()
            for b in range(n_sp):
                lat_hid(b).wait_recv()

        def lows(lo, hi):
            value = dot_nt(hid[0, lo:hi], decay_down[:, 0:depth])
            for o in range(1, n_sp):
                value = value + dot_nt(
                    hid[o, lo:hi], decay_down[:, o * depth : (o + 1) * depth]
                )
            return value.astype(BF16)

        def log_decays(low, z):
            x = dot(low[:, z * rank : (z + 1) * rank], decay_up[z, :, head_cols(DK)])
            return log_sigmoid(x + decay_bias[z : z + 1, head_cols(DK)]) / SHARP

        low = lows(0, lat_all)
        relay(2, 1)
        decays = [log_decays(low, z) for z in range(2)]
        group = 2 * length
        row_id = lax.broadcasted_iota(jnp.int32, (group, group), 0)
        col_id = lax.broadcasted_iota(jnp.int32, (group, group), 1)
        same = row_id // BLOCK == col_id // BLOCK
        inner = [same & (col_id <= row_id), same & (col_id >= row_id)]

        def within_of(z):
            pieces = []
            for i in range(lat_all // group):
                line = jnp.concatenate(
                    [extras[2 * i + e, z, pl.ds(h, 1), :] for e in range(2)], axis=1
                )
                extra = jnp.sum(jnp.where(inner[z], line, 0.0), axis=1, keepdims=True)
                pieces.append(sums(inner[z], decays[z][i * group : (i + 1) * group]) + extra)
            return jnp.concatenate(pieces, axis=0)

        within = [within_of(z) for z in range(2)]
        totals = [
            [within[0][(b + 1) * BLOCK - 1 : (b + 1) * BLOCK] for b in range(blocks)],
            [within[1][b * BLOCK : b * BLOCK + 1] for b in range(blocks)],
        ]
        none = jnp.zeros_like(totals[0][0])

        def between(z, lo, hi):
            value = none
            for b in range(lo, hi):
                value = value + totals[z][b]
            return value

        def per_block(f):
            return jnp.concatenate([f(b) for b in range(blocks)], axis=0)

        def rows_of(x, b):
            return x[b * BLOCK : (b + 1) * BLOCK]

        def key_span(z, i):
            if z == 0:
                return 0, min(-(-(i + 1) * BLOCK // DK) * DK, lat_all)
            return i * BLOCK // DK * DK, lat_all

        reach = [jnp.exp(within[z]) for z in range(2)]
        lifted_by = [
            jnp.exp(per_block(lambda b: rows_of(within[0], b) + between(0, 0, b))),
            jnp.exp(per_block(lambda b: rows_of(within[1], b) + between(1, b + 1, blocks))),
        ]

        @pl.when(is_leader)
        def _():
            for i in range(ctx_rows // piece):
                put(
                    context[i * piece : (i + 1) * piece],
                    1,
                    lat_all + s * ctx_rows + i * piece,
                )
            ctx_hid(s).start()
            for b in others():
                for k in range(1, n_tp):
                    ctx_plane(b, k, tp_from(k), t).wait_recv()
                for i in range(ctx_rows // piece):
                    put(
                        ctx[b, i * piece : (i + 1) * piece],
                        1,
                        lat_all + b * ctx_rows + i * piece,
                    )
                ctx_hid(b).start()

        @pl.when(is_follower)
        def _():
            for b in range(n_sp):
                ctx_hid(b).wait_recv()

        low_ctx = lows(lat_all, total)
        ctx_decays = [log_decays(low_ctx, z) for z in range(2)]
        ctx_all = total - lat_all
        crow = lax.broadcasted_iota(jnp.int32, (ctx_all, ctx_all), 0)
        ccol = lax.broadcasted_iota(jnp.int32, (ctx_all, ctx_all), 1)
        ctx_weight = [
            jnp.exp(sums(ccol > crow, ctx_decays[0])),
            jnp.exp(sums(ccol < crow, ctx_decays[1])),
        ]

        acc_k[...] = dot(hid[s], wk[s])
        acc_v[...] = dot(hid[s], wv[s])
        acc_q[...] = dot(hid[s, 0:lat_all], wq[s])
        multiply(0, 1, acc_k, total)
        multiply(1, 1, acc_v, total)
        multiply(2, 1, acc_q, lat_all)
        far = range(2, n_sp // 2 + 1)
        for j in far:
            relay(0, j)
            multiply(0, j, acc_k, total)
        keys = acc_k[...].astype(BF16).astype(F32)
        ckeys = keys[lat_all:]
        keys = keys[:lat_all]
        for z in range(2):
            close = (keys * jnp.exp(-within[z])).astype(BF16)
            near = keys * jnp.exp(per_block(lambda b: totals[z][b] - rows_of(within[z], b)))
            for i in range(blocks):
                lo, hi = key_span(z, i)
                for j in range(lo // BLOCK, hi // BLOCK):
                    if (j > i) if z == 0 else (j < i):
                        block = jnp.zeros((BLOCK, DK), BF16)
                    elif i == j:
                        block = rows_of(close, j)
                    else:
                        gap = between(z, min(i, j) + 1, max(i, j))
                        block = (rows_of(near, j) * jnp.exp(gap)).astype(BF16)
                    key_rows[z, i, j * BLOCK : (j + 1) * BLOCK] = block
        for j in far:
            relay(1, j)
            multiply(1, j, acc_v, total)
        values = acc_v[...].astype(BF16)
        cvals = values[lat_all:]
        values = values[:lat_all]
        state = [
            (CTX_LIFT * dot_tn(cvals, (ckeys * ctx_weight[z]).astype(BF16))).astype(BF16)
            for z in range(2)
        ]
        for j in far:
            relay(2, j)
            multiply(2, j, acc_q, lat_all)
        tri_row = lax.broadcasted_iota(jnp.int32, (BLOCK, lat_all), 0)
        tri_col = lax.broadcasted_iota(jnp.int32, (BLOCK, lat_all), 1)

        def attend(b):
            lines = []
            part_of = slice(b * length, (b + 1) * length)
            queries = acc_q[part_of].astype(BF16).astype(F32)
            query_dec = [(queries * reach[z][part_of]).astype(BF16) for z in range(2)]
            lifted = [(queries * lifted_by[z][part_of]).astype(BF16) for z in range(2)]
            for i in range(b * per, (b + 1) * per):
                full = []
                for z in range(2):
                    lo, hi = key_span(z, i)
                    score = dot_nt(rows_of(query_dec[z], i - b * per), key_rows[z, i, lo:hi])
                    ids = tri_row[:, lo:hi] + i * BLOCK
                    cols = tri_col[:, lo:hi]
                    keep = cols <= ids if z == 0 else cols >= ids
                    score = jnp.where(keep, score, 0.0)
                    pads = [jnp.zeros((BLOCK, lo), F32), score, jnp.zeros((BLOCK, lat_all - hi), F32)]
                    full.append(jnp.concatenate([p for p in pads if p.shape[1]], axis=1))
                lines.append((full[0] + full[1]).astype(BF16))
            mixed = dot(jnp.concatenate(lines, axis=0), values)
            for z in range(2):
                mixed = mixed + dot_nt(lifted[z], state[z])
            by = lax.rsqrt(jnp.mean(mixed * mixed, axis=-1, keepdims=True) + EPS)
            return (mixed * by * head_gain[...]).astype(BF16)

        for w in range(2):

            @pl.when(side == w)
            def _():
                here = first_plane + w
                near = here - 1 + 2 * w
                order = sorted((b for b in range(n_sp) if not inside(b)), key=lambda b: b == near)[:1] + [here + 1 - 2 * w, near, here]

                def store(b, value):
                    for u in range(n_tp):
                        at = u if inside(b) else u % 2 * two + u // 2
                        o_out[b, at] = value[u * rows : (u + 1) * rows]

                for b in order:
                    result = attend(b)
                    if b != here:
                        store(b, result)
                        for copy in o_copies(b):
                            copy.start()
                        continue

                    @pl.when(is_leader)
                    def _():
                        for u in range(n_tp):
                            normed[h, u] = result[u * rows : (u + 1) * rows]

                    @pl.when(is_follower)
                    def _():
                        store(b, result)
                        o_mate().start()

    pl.when(is_worker)(work)

    is_outer = jnp.logical_not(is_worker)

    @pl.when(is_outer)
    def _():
        out_load.wait()
        wo_cross().start()
        mods_arrive()
        wo_cross().wait_recv()
        wo_mate(h).start()
        wo_mate(1 - h).wait_recv()
        for group in range(2):
            for c in range(heads):
                duo_arrival(group, c).wait_recv()

    @pl.when(is_leader)
    def _():
        o_arrival(1 - h).wait_recv()

    @pl.when(is_follower)
    def _():
        for c in range(heads):
            o_arrival(c).wait_recv()

    chunks = rs_s.shape[1]
    span = width // chunks

    def rs_copy(index, k, c, to):
        return remote(
            part.at[index, :, pl.ds(c * span, span)],
            rs.at[k, :, pl.ds(c * span, span)],
            rs_s.at[k, c],
            rs_r.at[k, c],
            {"tp": to},
        )

    def write_out(cols, summed):
        gate = jnp.concatenate([mods[j] for j in range(n_dev)], axis=1)[0:1, 2 * width :]
        projected = summed.astype(BF16).astype(F32)
        out[:, cols] = (latents[:, cols].astype(F32) + gate[:, cols] * projected).astype(BF16)

    @pl.when(is_worker)
    def _():
        out_load.wait()
        for c in range(chunks):
            cols = slice(c * span, (c + 1) * span)
            product = 0.0
            for g in range(heads):
                product = product + dot(
                    normed[g].reshape(length, dv), wo[g * dv : (g + 1) * dv, cols]
                )
            product = product.astype(BF16)
            for i in range(n_tp):
                part[i, :, cols] = product[i * rows : (i + 1) * rows]
            for k in range(1, n_tp):
                rs_copy(tp_peer(k), k, c, tp_peer(k)).start()
        for c in range(chunks):
            cols = slice(c * span, (c + 1) * span)
            summed = part[t, :, cols].astype(F32)
            for k in range(1, n_tp):
                rs_copy(tp_peer(k), k, c, tp_peer(k)).wait_recv()
                summed = summed + rs[k, :, cols].astype(F32)
            write_out(cols, summed)
        for c in range(chunks):
            for k in range(1, n_tp):
                rs_copy(tp_peer(k), k, c, tp_peer(k)).wait_send()

    @pl.when(is_outer)
    def _():
        for c in range(chunks):
            cols = slice(c * span, (c + 1) * span)
            product = 0.0
            for group, matrix in enumerate((wo, wo_twist)):
                for g in range(heads):
                    product = product + dot(
                        duo[group, g].reshape(two * rows, dv), matrix[g * dv : (g + 1) * dv, cols]
                    )
            low_half = t < two
            kept[:, cols] = jnp.where(low_half, product[:rows], product[rows:])
            part[0, :, cols] = jnp.where(low_half, product[rows:], product[:rows]).astype(BF16)
            rs_copy(0, 1, c, cross).start()
        for c in range(chunks):
            cols = slice(c * span, (c + 1) * span)
            rs_copy(0, 1, c, cross).wait_recv()
            write_out(cols, kept[:, cols] + rs[1, :, cols].astype(F32))
        for c in range(chunks):
            rs_copy(0, 1, c, cross).wait_send()
        wo_cross().wait_send()
        wo_mate(h).wait_send()

    for k in range(1, n_tp):
        mod_tp(k, t, tp_peer(k)).wait_send()
    for copy in mod_direct:
        copy.wait_send()

    @pl.when(is_worker)
    def _():
        for copy in mod_passed:
            copy.wait_send()

    @pl.when(is_sender)
    def _():
        lat_in(s, target).wait_send()
        extra_in(s, target).wait_send()
        ctx_in(s, target).wait_send()

    @pl.when(is_leader)
    def _():
        extra_mate().wait_send()
        for k in range(1, n_tp):
            lat_own(k).wait_send()
            for b in others():
                lat_plane(b, k, t, tp_peer(k)).wait_send()
                ctx_plane(b, k, t, tp_peer(k)).wait_send()
        for b in range(n_sp):
            lat_hid(b).wait_send()
            ctx_hid(b).wait_send()

    @pl.when(is_follower)
    def _():
        o_mate().wait_send()

    for w in range(2):

        @pl.when(side == w)
        def _():
            for b in range(n_sp):
                if b != first_plane + w:
                    for copy in o_copies(b):
                        copy.wait_send()

    for m in range(3):
        for r in range(2):

            @pl.when(onward(r))
            def _():
                ring_copy(m, r, 0).wait_send()

            for j in range(1, n_sp // 2 + 1):

                @pl.when(jnp.logical_and(exists(r, j), onward(r)))
                def _():
                    ring_copy(m, r, j).wait_send()


def per_device(n_sp, n_tp, *args):
    (latents, sv, context, cv, gain, modulator, wq, wk, wv, down, up, bias, extra, hg, wo) = args
    heads = bias.shape[1] // DK
    if n_sp != 4 or n_tp != 4 or heads != 2:
        return chain_per_device(n_sp, n_tp, *args)
    rows, width = latents.shape
    ctx_rows = context.shape[0]
    n_dev = n_sp * n_tp
    length = rows * n_tp
    lat_all = n_sp * length
    total = n_sp * (length + ctx_rows)
    depth = wq.shape[0]
    dv = hg.shape[0]
    chunks = 2
    vmem = pl.BlockSpec(memory_space=pltpu.VMEM)
    hbm = pl.BlockSpec(memory_space=pl.ANY)
    dma = pltpu.SemaphoreType.DMA
    scratch = [
        pltpu.VMEM(latents.shape, BF16),
        pltpu.VMEM(sv.shape, F32),
        pltpu.VMEM(context.shape, BF16),
        pltpu.VMEM(cv.shape, F32),
        pltpu.VMEM((1, width), F32),
        pltpu.VMEM(down.shape[::-1], BF16),
        pltpu.VMEM(up.shape, BF16),
        pltpu.VMEM(bias.shape, F32),
        pltpu.VMEM((2, heads, length), F32),
        pltpu.VMEM((1, dv), F32),
        pltpu.VMEM(modulator.shape, BF16),
        pltpu.VMEM((n_dev, 2, modulator.shape[1]), F32),
        pltpu.VMEM((n_sp, n_tp, rows, width), BF16),
        pltpu.VMEM((n_sp, ctx_rows, width), BF16),
        pltpu.VMEM((n_sp, 2, heads, length), F32),
        pltpu.VMEM((n_sp, total, depth), BF16),
        pltpu.VMEM((n_sp, depth, DK), BF16),
        pltpu.VMEM((n_sp, depth, dv), BF16),
        pltpu.VMEM((n_sp, depth, DK), BF16),
        pltpu.VMEM(wo.shape, BF16),
        pltpu.VMEM((total, DK), F32),
        pltpu.VMEM((total, dv), F32),
        pltpu.VMEM((lat_all, DK), F32),
        pltpu.VMEM((2, lat_all // BLOCK, lat_all, DK), BF16),
        pltpu.VMEM((n_sp, n_tp, rows, dv), BF16),
        pltpu.VMEM((heads, n_tp, rows, dv), BF16),
        pltpu.VMEM((2, heads, n_tp // 2, rows, dv), BF16),
        pltpu.VMEM(wo.shape, BF16),
        pltpu.VMEM((rows, width), F32),
        pltpu.VMEM((n_tp, rows, width), BF16),
        pltpu.VMEM((n_tp, rows, width), BF16),
        dma((18,)),
        dma((n_tp,)),
        dma((n_tp,)),
        dma((n_sp,)),
        dma((n_sp,)),
        dma,
        dma((n_sp,)),
        dma,
        dma((n_sp,)),
        dma,
        dma((n_sp,)),
        dma,
        dma,
        dma((n_sp, n_tp)),
        dma((n_sp, n_tp)),
        dma((n_sp, n_tp)),
        dma((n_sp, n_tp)),
        dma((2 * n_sp,)),
        dma((2 * n_sp,)),
        dma((3, 2, n_sp)),
        dma((3, 2, n_sp)),
        dma((n_sp, 2)),
        dma((2, heads)),
        dma,
        dma,
        dma,
        dma,
        dma((n_tp, chunks)),
        dma((n_tp, chunks)),
        pltpu.SemaphoreType.REGULAR((n_sp + n_tp,)),
    ]
    return pl.pallas_call(
        functools.partial(kernel, n_sp, n_tp),
        out_shape=jax.ShapeDtypeStruct(latents.shape, BF16),
        in_specs=[hbm] * 15,
        out_specs=vmem,
        scratch_shapes=scratch,
        compiler_params=pltpu.CompilerParams(
            collective_id=0, has_side_effects=True, vmem_limit_bytes=56 * 1024 * 1024
        ),
    )(
        latents,
        sv,
        context,
        cv,
        gain.reshape(1, -1),
        modulator,
        wq,
        wk,
        wv,
        down.T,
        up,
        bias,
        extra.transpose(0, 2, 1),
        hg.reshape(1, -1),
        wo,
    )


def solution(mesh):
    placed = (
        P(("dp", "sp", "tp"), None),
        P("dp", None),
        P(("dp", "sp"), None),
        P(),
        P(),
        P(None, ("sp", "tp")),
        P("sp", "tp"),
        P("sp", "tp"),
        P("sp", "tp"),
        P(),
        P(None, None, "tp"),
        P(None, "tp"),
        P(None, ("dp", "sp"), "tp"),
        P(),
        P("tp", None),
    )
    return jax.shard_map(
        functools.partial(per_device, mesh.shape["sp"], mesh.shape["tp"]),
        mesh=mesh,
        in_specs=placed,
        out_specs=P(("dp", "sp", "tp"), None),
        check_vma=False,
    )
```
